32 devices in a mesh: kv: 4 (over y, x), tp: 8 (over z, core).
Axes of the slice: x: 2, y: 2, z: 4, core: 2. Of those that a mesh axis runs over, the one named last changes fastest.
Arguments:
- tokens: bfloat16 [128, 4096], P(None, ('kv', 'tp')), may hold values from -41 to 41
- lengths: int32 [128], P('kv'), may hold values from 1 to 8192, 262144 in all
- retention_state: float32 [128, 16, 128, 256], P('kv', 'tp'), may hold values from -4 to 4
- mixer_gain: float32 [4096], P('kv'), may hold values from 0.1 to 1.9
- query_weight: bfloat16 [4096, 2048], P('kv', 'tp'), may hold values from -0.09375 to 0.09375
- key_weight: bfloat16 [4096, 2048], P('kv', 'tp'), may hold values from -0.09375 to 0.09375
- value_weight: bfloat16 [4096, 4096], P('kv', 'tp'), may hold values from -0.09375 to 0.09375
- gate_weight: bfloat16 [4096, 4096], P('kv', 'tp'), may hold values from -0.09375 to 0.09375
- output_weight: bfloat16 [4096, 4096], P('tp', 'kv'), may hold values from -0.125 to 0.125
- channel_gain: float32 [4096], P('kv'), may hold values from 0.1 to 1.9
- ffn_gate: bfloat16 [4096, 11264], P('kv', 'tp'), may hold values from -0.09375 to 0.09375
- ffn_up: bfloat16 [4096, 11264], P('kv', 'tp'), may hold values from -0.09375 to 0.09375
- ffn_down: bfloat16 [11264, 4096], P('tp', 'kv'), may hold values from -0.078125 to 0.078125
Outputs:
- layer_output: bfloat16 [128, 4096], P(None, ('kv', 'tp'))
- new_state: float32 [128, 16, 128, 256], P('kv', 'tp')
The draws below stay inside these ranges and needn't reach their ends.
All inputs are finite; a program needn't handle non-finite values. No bound on the sum of `lengths` on one device may be relied on, other than what follows from the above.
Results may differ from the reference program's by a relative error of at most 0.022.
Values may be sent and summed in bfloat16 or wider, within the bound.
A program may use at most 64 MiB of HBM per device.

```python
import math
import jax
import jax.numpy as jnp
import numpy as np
from jax import lax

BATCH = 128
D = 4096
HEADS = 16
QK = 128
VD = 256
FF = 11264
MAXLEN = 8192


def draw_tokens(key, part):
    subkeys = jax.random.split(key, 3)
    positions = jnp.arange(D, dtype=jnp.float32) / (D - 1)
    roughness = jnp.exp(jax.random.uniform(subkeys[0], (D,), minval=-0.3, maxval=0.3))
    column_scale = jnp.exp(jnp.log(0.3) + positions * jnp.log(10.0)) * roughness
    base_values = jnp.clip(jax.random.normal(subkeys[2], (BATCH, D)), -5.0, 5.0)
    row_scale = jnp.exp(jax.random.uniform(subkeys[1], (BATCH, 1), minval=jnp.log(0.5), maxval=jnp.log(2.0)))
    return (base_values * row_scale * column_scale[None, :]).astype(jnp.bfloat16)


def with_spikes(entries, stream_key, source, target, parts, factor):
    def block_of(position):
        return (jnp.arange(entries.shape[position]) // (entries.shape[position] // parts)).reshape((-1,) + (1,) * (entries.ndim - 1 - position))

    near = jax.random.permutation(stream_key, parts)[block_of(target)]
    other_side = (block_of(target) + parts // 2) % parts
    return jnp.where((block_of(source) == near) | (block_of(source) == other_side), factor * entries, entries)


def levels(own_key, extent, cuts, low, largest):
    level, own = 1.0, jax.random.fold_in(own_key, 6)
    for dim, shards_of in cuts:
        steps = jnp.exp(jax.random.uniform(jax.random.fold_in(own, dim), (shards_of,), jnp.float32, low / len(cuts), largest / len(cuts)))
        level = level * jnp.repeat(steps, extent[dim] // shards_of).reshape([-1 if axis == dim else 1 for axis in range(len(extent))])
    return level


def split_up(count, total, bound, skew):
    weights = [(1 << 20) // math.isqrt(grade ** skew) + 1 for grade in range(2, count + 1)]
    spare, holding = total - bound - (count - 1), [1] * (count - 1)
    while spare > 0:
        movable = [i for i in range(count - 1) if holding[i] < bound]
        mass, left = sum([weights[i] for i in movable]), spare
        for i in movable:
            more = min(bound - holding[i], max(1, left * weights[i] // mass), spare)
            holding[i] = holding[i] + more
            spare = spare - more
    return np.array([bound] + holding)


def uneven_parts(rng, number_of, total, limit, skew):
    if number_of == 2:
        one = jax.random.randint(rng, (), max(1, total - limit), min(limit, total - 1) + 1)
        return jnp.stack([one, total - one])
    tallies = jnp.asarray(split_up(number_of, total, limit, skew), jnp.int32)
    couples = (number_of - 1) // 2
    source_of, receiver = tallies[1:1 + 2 * couples:2], tallies[2:2 + 2 * couples:2]
    margin = jnp.minimum(source_of - 1, limit - receiver)
    moved = jax.random.randint(jax.random.fold_in(rng, 1), (couples,), 0, 1 << 20) % (margin + 1)
    tallies = tallies.at[1:1 + 2 * couples:2].set(source_of - moved).at[2:2 + 2 * couples:2].set(receiver + moved)
    return tallies[jax.random.permutation(jax.random.fold_in(rng, 2), number_of)]


def centred(rng, extent, width, bound, cuts=(), kind=jnp.bfloat16):
    values = jax.random.normal(rng, extent, jnp.float32) * width
    if len(cuts) > 0:
        values = levels(rng, extent, cuts, -0.22, 0.18) * values
    return jnp.clip(values, min=-bound, max=bound).astype(kind)


def bell_draw_with(stream_key, shape, spread, limit, cuts, heavy, kind=jnp.bfloat16):
    drawn = spread * jax.random.normal(stream_key, shape, jnp.float32)
    if cuts:
        drawn = drawn * levels(stream_key, shape, cuts, -0.22, 0.18)
    return jnp.clip(with_spikes(drawn, jax.random.fold_in(stream_key, 3), *heavy), -limit, limit).astype(kind)


def setup_inputs(seed: int = 0) -> dict:
    streams_of = jax.random.split(jax.random.key(seed), 14)
    return {
        "tokens": draw_tokens(jax.random.fold_in(streams_of[13], 71), 0),
        "lengths": uneven_parts(streams_of[1], BATCH, BATCH * MAXLEN // 4, MAXLEN, 2).astype(jnp.int32),
        "retention_state": centred(streams_of[2], (BATCH, HEADS, QK, VD), 0.3, 4.0, ((0, 4), (1, 8)), jnp.float32),
        "mixer_gain": jnp.clip(1.0 + 0.18 * jax.random.normal(streams_of[3], (D,), jnp.float32), 0.1, 1.9),
        "query_weight": centred(streams_of[4], (D, HEADS * QK), D ** -0.5, 0.09375, ((0, 4), (1, 8))),
        "key_weight": centred(streams_of[5], (D, HEADS * QK), D ** -0.5, 0.09375, ((0, 4), (1, 8))),
        "value_weight": centred(streams_of[6], (D, HEADS * VD), D ** -0.5, 0.09375, ((0, 4), (1, 8))),
        "gate_weight": centred(streams_of[7], (D, HEADS * VD), D ** -0.5, 0.09375, ((0, 4), (1, 8))),
        "output_weight": bell_draw_with(streams_of[8], (HEADS * VD, D), D ** -0.5, 0.125, ((0, 8), (1, 4)), (0, 1, 8, 2.0)),
        "channel_gain": jnp.clip(1.0 + 0.18 * jax.random.normal(streams_of[9], (D,), jnp.float32), 0.1, 1.9),
        "ffn_gate": centred(streams_of[10], (D, FF), D ** -0.5, 0.09375, ((0, 4), (1, 8))),
        "ffn_up": centred(streams_of[11], (D, FF), D ** -0.5, 0.09375, ((0, 4), (1, 8))),
        "ffn_down": bell_draw_with(streams_of[12], (FF, D), FF ** -0.5, 0.078125, ((0, 8), (1, 4)), (0, 1, 8, 2.0)),
    }


def rotate_heads(vectors, positions):
    half_dim = vectors.shape[-1] // 2
    frequency = 10000.0 ** (-jnp.arange(half_dim, dtype=jnp.float32) / half_dim)
    angles = positions.astype(jnp.float32)[:, None, None] * frequency
    cosine = jnp.cos(angles)
    sine_part = jnp.sin(angles)
    first_half = vectors[..., :half_dim]
    second = vectors[..., half_dim:]
    return jnp.concatenate([first_half * cosine - second * sine_part, first_half * sine_part + second * cosine], axis=-1)

def inverse_rms(values):
    return lax.rsqrt(lax.optimization_barrier(jnp.mean(values * values, axis=-1)) + 1e-06)

def reference(tokens, lengths, retention_state, mixer_gain, query_weight, key_weight, value_weight, gate_weight, output_weight, channel_gain, ffn_gate, ffn_up, ffn_down):
    batch_rows = tokens.shape[0]
    tokens_wide = tokens.astype(jnp.float32)
    scale_one = inverse_rms(tokens_wide)[:, None]
    normed = (tokens_wide * mixer_gain).astype(jnp.bfloat16)
    query_proj = jnp.dot(normed, query_weight, preferred_element_type=jnp.float32) * scale_one
    query_rows = rotate_heads(query_proj.reshape(batch_rows, HEADS, QK), lengths).astype(jnp.bfloat16)
    key_proj = jnp.dot(normed, key_weight, preferred_element_type=jnp.float32) * scale_one
    key_rows = (rotate_heads(key_proj.reshape(batch_rows, HEADS, QK), lengths) * QK ** (-0.5)).astype(jnp.bfloat16)
    value_rows = (jnp.dot(normed, value_weight, preferred_element_type=jnp.float32) * scale_one).astype(jnp.bfloat16)
    value_rows = value_rows.reshape(batch_rows, HEADS, VD)
    gate_rows = jnp.dot(normed, gate_weight, preferred_element_type=jnp.float32) * scale_one
    head_ids = jnp.arange(HEADS, dtype=jnp.float32)
    decay_rate = 1.0 - 2.0 ** (-5.0 - 10.0 * head_ids / (HEADS - 1))
    new_state = decay_rate[None, :, None, None] * retention_state + key_rows.astype(jnp.float32)[..., :, None] * value_rows.astype(jnp.float32)[..., None, :]
    retained = jnp.einsum('bhk,bhkv->bhv', query_rows.astype(jnp.float32), new_state, precision=lax.Precision.HIGHEST)
    normalized = retained * inverse_rms(retained)[..., None]
    merged = (normalized.reshape(batch_rows, HEADS * VD) * jax.nn.silu(gate_rows)).astype(jnp.bfloat16)
    residual = (tokens_wide + jnp.dot(merged, output_weight, preferred_element_type=jnp.float32)).astype(jnp.bfloat16)
    residual_wide = residual.astype(jnp.float32)
    scale_two = inverse_rms(residual_wide)[:, None]
    normed_two = (residual_wide * channel_gain).astype(jnp.bfloat16)
    gate_ff = jnp.dot(normed_two, ffn_gate, preferred_element_type=jnp.float32) * scale_two
    up_ff = jnp.dot(normed_two, ffn_up, preferred_element_type=jnp.float32) * scale_two
    hidden = (jax.nn.silu(gate_ff) * up_ff).astype(jnp.bfloat16)
    layer_output = (residual_wide + jnp.dot(hidden, ffn_down, preferred_element_type=jnp.float32)).astype(jnp.bfloat16)
    return (layer_output, new_state)
```

```python
import functools

import jax
import jax.numpy as jnp
import numpy as np
from jax import lax
from jax.experimental import pallas as pl
from jax.experimental.pallas import tpu as pltpu
from jax.sharding import PartitionSpec as P

D = 4096
HEADS = 16
QK = 128
LANES = 128


def rotate_heads(vectors, positions):
    half_dim = vectors.shape[-1] // 2
    frequency = 10000.0 ** (-jnp.arange(half_dim, dtype=jnp.float32) / half_dim)
    angles = positions.astype(jnp.float32)[:, None, None] * frequency
    cosine = jnp.cos(angles)
    sine_part = jnp.sin(angles)
    first_half = vectors[..., :half_dim]
    second = vectors[..., half_dim:]
    return jnp.concatenate(
        [first_half * cosine - second * sine_part, first_half * sine_part + second * cosine],
        axis=-1,
    )


def gathered_rows(columns):
    return lax.all_gather(columns, "tp", axis=1, tiled=True)


def owned_sums(partial_value, squares):
    raw_sums, totals = (
        lax.psum_scatter(
            partial_value.astype(jnp.bfloat16), "kv", scatter_dimension=0, tiled=True
        ).astype(jnp.float32),
        lax.psum_scatter(
            squares.astype(jnp.bfloat16), "kv", scatter_dimension=0, tiled=True
        ).astype(jnp.float32),
    )
    summed = raw_sums * lax.rsqrt(totals / D + 1e-06)[:, None]
    return summed


def every_sum(partial_value, squares):
    raw_sums, totals = (
        lax.psum(partial_value.astype(jnp.bfloat16), "kv").astype(jnp.float32),
        lax.psum(squares.astype(jnp.bfloat16), "kv").astype(jnp.float32),
    )
    summed = raw_sums * lax.rsqrt(totals / D + 1e-06)[:, None]
    return summed


def on_device(
    tokens,
    lengths,
    retention_state,
    mixer_gain,
    query_weight,
    key_weight,
    value_weight,
    gate_weight,
    output_weight,
    channel_gain,
    ffn_gate,
    ffn_up,
    ffn_down,
):
    feature_block = gathered_rows(tokens).astype(jnp.float32)
    squares = jnp.sum(feature_block * feature_block, axis=1)
    normed = (feature_block * mixer_gain).astype(jnp.bfloat16)
    partial_value = jnp.concatenate(
        [
            jnp.dot(normed, query_weight, preferred_element_type=jnp.float32),
            jnp.dot(normed, key_weight, preferred_element_type=jnp.float32),
            jnp.dot(normed, value_weight, preferred_element_type=jnp.float32),
            jnp.dot(normed, gate_weight, preferred_element_type=jnp.float32),
        ],
        axis=1,
    )
    owned_rows = owned_sums(partial_value, squares)
    local_heads = query_weight.shape[1] // QK
    q_width = query_weight.shape[1]
    v_width = value_weight.shape[1]
    head_width = v_width // local_heads
    seq_rows = owned_rows.shape[0]
    query_rows = rotate_heads(
        owned_rows[:, :q_width].reshape(seq_rows, local_heads, QK), lengths
    ).astype(jnp.bfloat16)
    key_rows = (
        rotate_heads(
            owned_rows[:, q_width : 2 * q_width].reshape(seq_rows, local_heads, QK), lengths
        )
        * QK ** (-0.5)
    ).astype(jnp.bfloat16)
    value_rows = (
        owned_rows[:, 2 * q_width : 2 * q_width + v_width]
        .astype(jnp.bfloat16)
        .reshape(seq_rows, local_heads, head_width)
    )
    gate_rows = owned_rows[:, 2 * q_width + v_width :]
    head_ids = (lax.axis_index("tp") * local_heads + jnp.arange(local_heads)).astype(jnp.float32)
    decay_rate = 1.0 - 2.0 ** (-5.0 - 10.0 * head_ids / (HEADS - 1))
    new_state = (
        decay_rate[None, :, None, None] * retention_state
        + key_rows.astype(jnp.float32)[..., :, None] * value_rows.astype(jnp.float32)[..., None, :]
    )
    retained = jnp.einsum(
        "bhk,bhkv->bhv", query_rows.astype(jnp.float32), new_state, precision=lax.Precision.HIGHEST
    )
    normalized = retained * lax.rsqrt(jnp.mean(retained * retained, axis=-1) + 1e-06)[..., None]
    merged = (normalized.reshape(seq_rows, v_width) * jax.nn.silu(gate_rows)).astype(jnp.bfloat16)
    mixed_part = jnp.dot(
        lax.all_gather(merged, "kv", axis=0, tiled=True),
        output_weight,
        preferred_element_type=jnp.float32,
    )
    mixed_cols = lax.psum_scatter(
        mixed_part.astype(jnp.bfloat16), "tp", scatter_dimension=1, tiled=True
    ).astype(jnp.float32)
    residual = (tokens.astype(jnp.float32) + mixed_cols).astype(jnp.bfloat16)
    block_two = gathered_rows(residual).astype(jnp.float32)
    squares_two = jnp.sum(block_two * block_two, axis=1)
    normed_two = (block_two * channel_gain).astype(jnp.bfloat16)
    partial_two = jnp.concatenate(
        [
            jnp.dot(normed_two, ffn_gate, preferred_element_type=jnp.float32),
            jnp.dot(normed_two, ffn_up, preferred_element_type=jnp.float32),
        ],
        axis=1,
    )
    hidden_units = ffn_gate.shape[1]
    summed = every_sum(partial_two, squares_two)
    hidden = (jax.nn.silu(summed[:, :hidden_units]) * summed[:, hidden_units:]).astype(jnp.bfloat16)
    down_part = jnp.dot(hidden, ffn_down, preferred_element_type=jnp.float32)
    down_sums = lax.psum_scatter(
        down_part.astype(jnp.bfloat16), "tp", scatter_dimension=1, tiled=True
    ).astype(jnp.float32)
    layer_output = (residual.astype(jnp.float32) + down_sums).astype(jnp.bfloat16)
    return (layer_output, new_state)


MESH_ID = pl.DeviceIdType.MESH
VMEM_TOTAL = 67043328
CORES = 2


def greet(groups):
    barrier = pltpu.get_barrier_semaphore()
    for axis, peers in groups:
        for peer in peers:
            pl.semaphore_signal(barrier, inc=1, device_id={axis: peer}, device_id_type=MESH_ID)
    pl.semaphore_wait(barrier, sum(len(peers) for _, peers in groups))


def send_all(axis, count, me, source, target, send_sems, recv_sems):
    copies = []
    for step in range(1, count):
        peer = lax.rem(me + step, count)
        copy = pltpu.make_async_remote_copy(
            src_ref=source(peer),
            dst_ref=target(step),
            send_sem=send_sems.at[step - 1],
            recv_sem=recv_sems.at[step - 1],
            device_id={axis: peer},
            device_id_type=MESH_ID,
        )
        copy.start()
        copies.append(copy)
    return copies


def received(copies):
    for copy in copies:
        copy.wait_recv()


def sent(copies):
    for copy in copies:
        copy.wait_send()


def load_all(pairs, sems):
    copies = [pltpu.make_async_copy(src, dst, sems.at[i]) for i, (src, dst) in enumerate(pairs)]
    for copy in copies:
        copy.start()
    return copies


def silu(value):
    return value / (1.0 + jnp.exp(-value))


def square_block(squares):
    head = squares.astype(jnp.bfloat16).astype(jnp.float32)
    rest = squares - head
    lane = lax.broadcasted_iota(jnp.int32, (squares.shape[0], LANES), 1)
    return jnp.where(lane < LANES // 2, head, rest).astype(jnp.bfloat16)


def square_total(block):
    return block[:, :1] + block[:, LANES // 2 : LANES // 2 + 1]


def wide(ref):
    return jnp.concatenate([ref[j] for j in range(ref.shape[0])], axis=1)


def remote(axis, peer, source, target, send_sem, recv_sem):
    return pltpu.make_async_remote_copy(
        src_ref=source, dst_ref=target, send_sem=send_sem, recv_sem=recv_sem,
        device_id={axis: peer}, device_id_type=MESH_ID,
    )


def gather_tp(slots, source, tp, n_tp, send_sems, recv_sems):
    chips = n_tp // CORES
    chip, core = tp // CORES, lax.rem(tp, CORES)
    partner = chip * CORES + 1 - core
    direct = []
    for step in range(1, chips):
        peer = lax.rem(chip + step, chips) * CORES + core
        direct.append(
            remote("tp", peer, source, slots.at[tp], send_sems.at[step], recv_sems.at[step])
        )
    across = [remote("tp", partner, source, slots.at[tp], send_sems.at[0], recv_sems.at[0])]
    for copy in direct + across:
        copy.start()

    def finish():
        for step in range(1, chips):
            direct[step - 1].wait_recv()
            slot = lax.rem(chip - step + chips, chips) * CORES + core
            i = chips - 1 + step
            copy = remote(
                "tp", partner, slots.at[slot], slots.at[slot], send_sems.at[i], recv_sems.at[i]
            )
            copy.start()
            across.append(copy)
        received(across)
        return direct + across

    return finish


def reduce_tp(lhs, weight, parts, swapped, staged, landed, tp, n_tp, send_sems, recv_sems):
    chips = n_tp // CORES
    chip, core = tp // CORES, lax.rem(tp, CORES)
    partner = chip * CORES + 1 - core
    columns = parts.shape[3]

    def multiply(side):
        starts = [pl.multiple_of((z * CORES + side) * columns, LANES) for z in range(chips)]
        rhs = jnp.concatenate([weight[:, pl.ds(start, columns)] for start in starts], axis=1)
        full = jnp.dot(lhs, rhs, preferred_element_type=jnp.float32).astype(jnp.bfloat16)
        for z in range(chips):
            parts[side, z] = full[:, z * columns : (z + 1) * columns]

    multiply(1 - core)
    swap = remote(
        "tp", partner, parts.at[1 - core], swapped, send_sems.at[0], recv_sems.at[0]
    )
    swap.start()
    multiply(core)
    swap.wait_recv()
    copies = []
    for step in range(1, chips):
        other = lax.rem(chip + step, chips)
        pair = parts[core, other].astype(jnp.float32) + swapped[other].astype(jnp.float32)
        staged[step - 1] = pair.astype(jnp.bfloat16)
        copy = remote(
            "tp", other * CORES + core, staged.at[step - 1], landed.at[step - 1],
            send_sems.at[step], recv_sems.at[step],
        )
        copy.start()
        copies.append(copy)
    total = parts[core, chip].astype(jnp.float32) + swapped[chip].astype(jnp.float32)
    for step in range(1, chips):
        copies[step - 1].wait_recv()
        total += landed[step - 1].astype(jnp.float32)
    return total, copies + [swap]


def total_of(own, landed):
    total = own.astype(jnp.float32)
    for step in range(landed.shape[0]):
        total += landed[step].astype(jnp.float32)
    return total


def layer_kernel(
    n_kv, n_tp, features,
    tokens_hbm, lengths_hbm, freq_hbm, gain_hbm, gain_two_hbm, state_hbm,
    wq_hbm, wk_hbm, wv_hbm, wg_hbm, wo_hbm, fg_hbm, fu_hbm, fd_hbm,
    out, state,
    lengths, freq, gain, gain_two, wq, wk, wv, wg, wo, fg, fu, fd,
    gathered, out_a, out_b, in_a, in_b, qk, value, retained, merged,
    parts_x, swapped_x, staged_x, landed_x, own, gathered_two,
    gate_out, up_out, gate_in, up_in, hidden, parts_d, swapped_d, staged_d, landed_d,
    load_sems, gs, gr, as_, ar, bs, br, ms, mr, xs, xr, cs, cr, es, er, fs, fr, hs, hr, ds_, dr,
):
    kv, tp = lax.axis_index("kv"), lax.axis_index("tp")
    chips = n_tp // CORES
    chip, core = tp // CORES, lax.rem(tp, CORES)
    pairs = [
        (tokens_hbm, gathered.at[tp]), (lengths_hbm, lengths), (freq_hbm, freq), (gain_hbm, gain),
        (wq_hbm, wq), (wk_hbm, wk), (wv_hbm, wv), (wg_hbm, wg), (state_hbm, state),
        (gain_two_hbm, gain_two), (wo_hbm, wo), (fg_hbm, fg), (fu_hbm, fu), (fd_hbm, fd),
    ]
    loads = load_all(pairs, load_sems)
    along = [lax.rem(chip + step, chips) * CORES + core for step in range(1, chips)]
    greet([
        ("tp", along + [chip * CORES + 1 - core]),
        ("kv", [lax.rem(kv + step, n_kv) for step in range(1, n_kv)]),
    ])
    loads[0].wait()
    finish_g = gather_tp(gathered, gathered.at[tp], tp, n_tp, gs, gr)
    for i in (1, 2, 3):
        loads[i].wait()
    rows = out_a.shape[1]
    row = lax.broadcasted_iota(jnp.int32, (rows, rows), 0)
    col = lax.broadcasted_iota(jnp.int32, (rows, rows), 1)
    spread = jnp.where(row == col, lengths[...].astype(jnp.float32), 0.0)
    angles = jnp.sum(spread, axis=1, keepdims=True) * freq[...]
    cosine, sine = jnp.cos(angles), jnp.sin(angles)
    lane = lax.broadcasted_iota(jnp.int32, angles.shape, 1)
    sine = jnp.where(lane < QK // 2, -sine, sine)
    started = finish_g()

    def normalise(slots, gains):
        x = wide(slots).astype(jnp.float32)
        squares = jnp.sum(x * x, axis=1, keepdims=True)
        return (x * gains[...]).astype(jnp.bfloat16), square_block(squares).reshape(n_kv, rows, LANES)

    def project(lhs, weight):
        full = jnp.dot(lhs, weight[...], preferred_element_type=jnp.float32)
        return full.astype(jnp.bfloat16).reshape(n_kv, rows, full.shape[1])

    normed, squares = normalise(gathered, gain)
    q_width, v_width = wq.shape[1], wv.shape[1]
    heads = q_width // QK
    width = v_width // heads
    out_a[:, :, 2 * q_width :] = squares
    loads[4].wait()
    out_a[:, :, :q_width] = project(normed, wq)
    loads[5].wait()
    out_a[:, :, q_width : 2 * q_width] = project(normed, wk)
    first = send_all("kv", n_kv, kv, lambda p: out_a.at[p], lambda s: in_a.at[s - 1], as_, ar)
    loads[6].wait()
    out_b[:, :, :v_width] = project(normed, wv)
    loads[7].wait()
    out_b[:, :, v_width:] = project(normed, wg)
    second = send_all("kv", n_kv, kv, lambda p: out_b.at[p], lambda s: in_b.at[s - 1], bs, br)
    loads[8].wait()
    received(first)
    total = total_of(out_a[kv], in_a)
    scale = lax.rsqrt(square_total(total[:, 2 * q_width :]) / features + 1e-06)
    total = total * scale
    blocks = []
    for base, factor in ((0, 1.0), (q_width, QK ** (-0.5))):
        for head in range(heads):
            part = total[:, base + head * QK : base + (head + 1) * QK]
            turned = (part * cosine + pltpu.roll(part, QK // 2, 1) * sine) * factor
            blocks.append(turned.astype(jnp.bfloat16).astype(jnp.float32))
    qk[...] = jnp.concatenate(blocks, axis=0).T
    block = 4

    def turned_to(start):
        return pltpu.roll(qk[...], lax.rem(LANES - start, LANES), 1)

    def query_step(i, carry):
        start = i * block
        turned = turned_to(start)
        for s in range(block):
            for head in range(heads):
                query = turned[:, head * rows + s : head * rows + s + 1]
                retained[pl.ds(start + s, 1), head * width : (head + 1) * width] = jnp.sum(
                    query * state[start + s, head], axis=0, keepdims=True
                )
        return carry

    lax.fori_loop(0, rows // block, query_step, 0)
    decays = []
    for head in range(heads):
        number = jnp.full((1, width), tp * heads + head, jnp.int32).astype(jnp.float32)
        decays.append(1.0 - jnp.exp2(-5.0 - 10.0 * number / (heads * n_tp - 1)))
    received(second)
    total = total_of(out_b[kv], in_b) * scale
    value[...] = total[:, :v_width].astype(jnp.bfloat16).astype(jnp.float32)
    pieces = []
    for head in range(heads):
        overlap = jnp.sum(blocks[head] * blocks[heads + head], axis=1, keepdims=True)
        span = slice(head * width, (head + 1) * width)
        piece = decays[head] * retained[:, span] + overlap * value[:, span]
        pieces.append(piece * lax.rsqrt(jnp.mean(piece * piece, axis=1, keepdims=True) + 1e-06))
    merged[kv] = (jnp.concatenate(pieces, axis=1) * silu(total[:, v_width:])).astype(jnp.bfloat16)
    copies_m = send_all("kv", n_kv, kv, lambda p: merged.at[kv], lambda s: merged.at[kv], ms, mr)

    def update_step(i, carry):
        start = i * block
        turned = turned_to(start)
        for s in range(block):
            for head in range(heads):
                lane = (heads + head) * rows + s
                outer = turned[:, lane : lane + 1] * value[pl.ds(start + s, 1), head * width : (head + 1) * width]
                state[start + s, head] = decays[head] * state[start + s, head] + outer
        return carry

    lax.fori_loop(0, rows // block, update_step, 0)
    loads[10].wait()
    received(copies_m)
    batch = n_kv * rows
    total, copies_x = reduce_tp(
        merged[...].reshape(batch, v_width), wo, parts_x, swapped_x, staged_x, landed_x, tp, n_tp, xs, xr
    )
    residual = (tokens_of(gathered, tp) + total).astype(jnp.bfloat16)
    own[...] = residual
    gathered_two[tp] = residual
    finish_c = gather_tp(gathered_two, own, tp, n_tp, cs, cr)
    loads[9].wait()
    loads[11].wait()
    copies_c = finish_c()
    normed, squares = normalise(gathered_two, gain_two)
    units = fg.shape[1]
    gate_out[:, :, units:] = squares
    gate_out[:, :, :units] = project(normed, fg)
    copies_e = send_all("kv", n_kv, kv, lambda p: gate_out.at[p], lambda s: gate_in.at[s - 1], es, er)
    loads[12].wait()
    up_out[...] = project(normed, fu)
    copies_f = send_all("kv", n_kv, kv, lambda p: up_out.at[p], lambda s: up_in.at[s - 1], fs, fr)
    received(copies_e)
    total = total_of(gate_out[kv], gate_in)
    scale = lax.rsqrt(square_total(total[:, units:]) / features + 1e-06)
    activated = silu(total[:, :units] * scale)
    received(copies_f)
    hidden[kv] = (activated * (total_of(up_out[kv], up_in) * scale)).astype(jnp.bfloat16)
    copies_h = send_all("kv", n_kv, kv, lambda p: hidden.at[kv], lambda s: hidden.at[kv], hs, hr)
    loads[13].wait()
    received(copies_h)
    total, copies_d = reduce_tp(
        hidden[...].reshape(batch, units), fd, parts_d, swapped_d, staged_d, landed_d, tp, n_tp, ds_, dr
    )
    out[...] = (own[...].astype(jnp.float32) + total).astype(jnp.bfloat16)
    for copies in (started, first, second, copies_m, copies_x, copies_c, copies_e, copies_f, copies_h, copies_d):
        sent(copies)


def finish_kernel(state, out, state_to, out_to, store_sems):
    chunks = store_sems.shape[0] - 1
    size = state.shape[0] // chunks
    targets = [(out, out_to)]
    for i in range(chunks):
        part = pl.ds(i * size, size)
        targets.append((state.at[part], state_to.at[part]))
    for copy in load_all(targets, store_sems):
        copy.wait()


def tokens_of(slots, tp):
    return slots[tp].astype(jnp.float32)


def fused_on_device(n_kv, n_tp, *arrays):
    (
        tokens, lengths, state, mixer_gain, wq, wk, wv, wg, wo, channel_gain, fg, fu, fd,
    ) = arrays
    batch, columns = tokens.shape
    rows = state.shape[0]
    depth, q_width = wq.shape
    v_width, units = wv.shape[1], fg.shape[1]
    bf16, f32 = jnp.bfloat16, jnp.float32
    vmem = pl.BlockSpec(memory_space=pltpu.VMEM)
    hbm = pl.BlockSpec(memory_space=pltpu.HBM)
    dma = pltpu.SemaphoreType.DMA
    tp_sems, kv_sems = [dma((n_tp - 1,))] * 2, [dma((n_kv - 1,))] * 2
    chips = n_tp // CORES
    chip_sems = [dma((chips,))] * 2
    index = np.arange(QK) % (QK // 2)
    freq = jnp.asarray((10000.0 ** (-index / (QK // 2))).astype(np.float32))[None, :]
    a_width, b_width = 2 * q_width + LANES, 2 * v_width
    reduce_scratch = [
        pltpu.VMEM((CORES, chips, batch, columns), bf16),
        pltpu.VMEM((chips, batch, columns), bf16),
        pltpu.VMEM((chips - 1, batch, columns), bf16),
        pltpu.VMEM((chips - 1, batch, columns), bf16),
    ]
    out, new_state = pl.pallas_call(
        functools.partial(layer_kernel, n_kv, n_tp, depth * n_kv),
        out_shape=(
            pltpu.VMEM(tokens.shape, bf16),
            pltpu.VMEM(state.shape, f32),
        ),
        in_specs=[hbm] * 14,
        out_specs=(vmem, vmem),
        scratch_shapes=[
            pltpu.VMEM((1, rows), jnp.int32),
            pltpu.VMEM((1, QK), f32),
            pltpu.VMEM((1, depth), f32),
            pltpu.VMEM((1, depth), f32),
        ]
        + [pltpu.VMEM(w.shape, bf16) for w in (wq, wk, wv, wg, wo, fg, fu, fd)]
        + [
            pltpu.VMEM((n_tp, batch, columns), bf16),
            pltpu.VMEM((n_kv, rows, a_width), bf16),
            pltpu.VMEM((n_kv, rows, b_width), bf16),
            pltpu.VMEM((n_kv - 1, rows, a_width), bf16),
            pltpu.VMEM((n_kv - 1, rows, b_width), bf16),
            pltpu.VMEM((QK, LANES), f32),
            pltpu.VMEM((rows, v_width), f32),
            pltpu.VMEM((rows, v_width), f32),
            pltpu.VMEM((n_kv, rows, v_width), bf16),
        ]
        + reduce_scratch
        + [
            pltpu.VMEM((batch, columns), bf16),
            pltpu.VMEM((n_tp, batch, columns), bf16),
            pltpu.VMEM((n_kv, rows, units + LANES), bf16),
            pltpu.VMEM((n_kv, rows, units), bf16),
            pltpu.VMEM((n_kv - 1, rows, units + LANES), bf16),
            pltpu.VMEM((n_kv - 1, rows, units), bf16),
            pltpu.VMEM((n_kv, rows, units), bf16),
        ]
        + reduce_scratch
        + [dma((14,))]
        + tp_sems + kv_sems + kv_sems + kv_sems + chip_sems + tp_sems + kv_sems + kv_sems + kv_sems + chip_sems,
        compiler_params=pltpu.CompilerParams(
            collective_id=0, has_side_effects=True, vmem_limit_bytes=40000000
        ),
        name="layer",
    )(*[pltpu.with_memory_space_constraint(a, pltpu.HBM) for a in (tokens, lengths[None, :], freq, mixer_gain[None, :], channel_gain[None, :], state, wq, wk, wv, wg, wo, fg, fu, fd)])
    new_state, out = pl.pallas_call(
        finish_kernel,
        out_shape=(
            jax.ShapeDtypeStruct(state.shape, f32),
            jax.ShapeDtypeStruct(tokens.shape, bf16),
        ),
        in_specs=[vmem, vmem],
        out_specs=(hbm, hbm),
        scratch_shapes=[dma((9,))],
        compiler_params=pltpu.CompilerParams(vmem_limit_bytes=20000000),
        name="finish",
    )(new_state, out)
    return out, new_state


def fits(n_kv, n_tp, arrays):
    tokens, state, ffn_gate = arrays[0], arrays[2], arrays[10]
    rows, heads = state.shape[0], state.shape[1]
    return (
        tokens.shape[1] % LANES == 0
        and n_tp % CORES == 0
        and n_tp > CORES
        and n_kv > 1
        and 4 * state.size < VMEM_TOTAL // 4
        and ffn_gate.shape[1] % LANES == 0
        and rows % 16 == 0
        and 2 * heads * rows == LANES
        and state.shape[2] == QK == LANES
        and state.shape[3] % LANES == 0
    )


def per_device(n_kv, n_tp, *arrays):
    if fits(n_kv, n_tp, arrays):
        return fused_on_device(n_kv, n_tp, *arrays)
    return on_device(*arrays)


def solution(mesh):
    in_specs = (
        P(None, ("kv", "tp")),
        P("kv"),
        P("kv", "tp", None, None),
        P("kv"),
        P("kv", "tp"),
        P("kv", "tp"),
        P("kv", "tp"),
        P("kv", "tp"),
        P("tp", "kv"),
        P("kv"),
        P("kv", "tp"),
        P("kv", "tp"),
        P("tp", "kv"),
    )
    out_specs = (P(None, ("kv", "tp")), P("kv", "tp", None, None))
    return jax.shard_map(
        functools.partial(per_device, mesh.shape["kv"], mesh.shape["tp"]),
        mesh=mesh, in_specs=in_specs, out_specs=out_specs, check_vma=False
    )
```

```python
import functools

import jax
import jax.numpy as jnp
import numpy as np
from jax import lax
from jax.experimental import pallas as pl
from jax.experimental.pallas import tpu as pltpu
from jax.sharding import PartitionSpec as P

D = 4096
HEADS = 16
QK = 128
LANES = 128


def rotate_heads(vectors, positions):
    half_dim = vectors.shape[-1] // 2
    frequency = 10000.0 ** (-jnp.arange(half_dim, dtype=jnp.float32) / half_dim)
    angles = positions.astype(jnp.float32)[:, None, None] * frequency
    cosine = jnp.cos(angles)
    sine_part = jnp.sin(angles)
    first_half = vectors[..., :half_dim]
    second = vectors[..., half_dim:]
    return jnp.concatenate(
        [first_half * cosine - second * sine_part, first_half * sine_part + second * cosine],
        axis=-1,
    )


def gathered_rows(columns):
    return lax.all_gather(columns, "tp", axis=1, tiled=True)


def owned_sums(partial_value, squares):
    raw_sums, totals = (
        lax.psum_scatter(
            partial_value.astype(jnp.bfloat16), "kv", scatter_dimension=0, tiled=True
        ).astype(jnp.float32),
        lax.psum_scatter(
            squares.astype(jnp.bfloat16), "kv", scatter_dimension=0, tiled=True
        ).astype(jnp.float32),
    )
    summed = raw_sums * lax.rsqrt(totals / D + 1e-06)[:, None]
    return summed


def every_sum(partial_value, squares):
    raw_sums, totals = (
        lax.psum(partial_value.astype(jnp.bfloat16), "kv").astype(jnp.float32),
        lax.psum(squares.astype(jnp.bfloat16), "kv").astype(jnp.float32),
    )
    summed = raw_sums * lax.rsqrt(totals / D + 1e-06)[:, None]
    return summed


def on_device(
    tokens,
    lengths,
    retention_state,
    mixer_gain,
    query_weight,
    key_weight,
    value_weight,
    gate_weight,
    output_weight,
    channel_gain,
    ffn_gate,
    ffn_up,
    ffn_down,
):
    feature_block = gathered_rows(tokens).astype(jnp.float32)
    squares = jnp.sum(feature_block * feature_block, axis=1)
    normed = (feature_block * mixer_gain).astype(jnp.bfloat16)
    partial_value = jnp.concatenate(
        [
            jnp.dot(normed, query_weight, preferred_element_type=jnp.float32),
            jnp.dot(normed, key_weight, preferred_element_type=jnp.float32),
            jnp.dot(normed, value_weight, preferred_element_type=jnp.float32),
            jnp.dot(normed, gate_weight, preferred_element_type=jnp.float32),
        ],
        axis=1,
    )
    owned_rows = owned_sums(partial_value, squares)
    local_heads = query_weight.shape[1] // QK
    q_width = query_weight.shape[1]
    v_width = value_weight.shape[1]
    head_width = v_width // local_heads
    seq_rows = owned_rows.shape[0]
    query_rows = rotate_heads(
        owned_rows[:, :q_width].reshape(seq_rows, local_heads, QK), lengths
    ).astype(jnp.bfloat16)
    key_rows = (
        rotate_heads(
            owned_rows[:, q_width : 2 * q_width].reshape(seq_rows, local_heads, QK), lengths
        )
        * QK ** (-0.5)
    ).astype(jnp.bfloat16)
    value_rows = (
        owned_rows[:, 2 * q_width : 2 * q_width + v_width]
        .astype(jnp.bfloat16)
        .reshape(seq_rows, local_heads, head_width)
    )
    gate_rows = owned_rows[:, 2 * q_width + v_width :]
    head_ids = (lax.axis_index("tp") * local_heads + jnp.arange(local_heads)).astype(jnp.float32)
    decay_rate = 1.0 - 2.0 ** (-5.0 - 10.0 * head_ids / (HEADS - 1))
    new_state = (
        decay_rate[None, :, None, None] * retention_state
        + key_rows.astype(jnp.float32)[..., :, None] * value_rows.astype(jnp.float32)[..., None, :]
    )
    retained = jnp.einsum(
        "bhk,bhkv->bhv", query_rows.astype(jnp.float32), new_state, precision=lax.Precision.HIGHEST
    )
    normalized = retained * lax.rsqrt(jnp.mean(retained * retained, axis=-1) + 1e-06)[..., None]
    merged = (normalized.reshape(seq_rows, v_width) * jax.nn.silu(gate_rows)).astype(jnp.bfloat16)
    mixed_part = jnp.dot(
        lax.all_gather(merged, "kv", axis=0, tiled=True),
        output_weight,
        preferred_element_type=jnp.float32,
    )
    mixed_cols = lax.psum_scatter(
        mixed_part.astype(jnp.bfloat16), "tp", scatter_dimension=1, tiled=True
    ).astype(jnp.float32)
    residual = (tokens.astype(jnp.float32) + mixed_cols).astype(jnp.bfloat16)
    block_two = gathered_rows(residual).astype(jnp.float32)
    squares_two = jnp.sum(block_two * block_two, axis=1)
    normed_two = (block_two * channel_gain).astype(jnp.bfloat16)
    partial_two = jnp.concatenate(
        [
            jnp.dot(normed_two, ffn_gate, preferred_element_type=jnp.float32),
            jnp.dot(normed_two, ffn_up, preferred_element_type=jnp.float32),
        ],
        axis=1,
    )
    hidden_units = ffn_gate.shape[1]
    summed = every_sum(partial_two, squares_two)
    hidden = (jax.nn.silu(summed[:, :hidden_units]) * summed[:, hidden_units:]).astype(jnp.bfloat16)
    down_part = jnp.dot(hidden, ffn_down, preferred_element_type=jnp.float32)
    down_sums = lax.psum_scatter(
        down_part.astype(jnp.bfloat16), "tp", scatter_dimension=1, tiled=True
    ).astype(jnp.float32)
    layer_output = (residual.astype(jnp.float32) + down_sums).astype(jnp.bfloat16)
    return (layer_output, new_state)


MESH_ID = pl.DeviceIdType.MESH
VMEM_TOTAL = 67043328
CORES = 2
LAYER_VMEM = 50000000
FINISH_VMEM = 20000000


def greet(groups):
    barrier = pltpu.get_barrier_semaphore()
    for axis, peers in groups:
        for peer in peers:
            pl.semaphore_signal(barrier, inc=1, device_id={axis: peer}, device_id_type=MESH_ID)
    pl.semaphore_wait(barrier, sum(len(peers) for _, peers in groups))


def send_all(axis, count, me, source, target, send_sems, recv_sems):
    copies = []
    for step in range(1, count):
        peer = lax.rem(me + step, count)
        copy = pltpu.make_async_remote_copy(
            src_ref=source(peer),
            dst_ref=target(step),
            send_sem=send_sems.at[step - 1],
            recv_sem=recv_sems.at[step - 1],
            device_id={axis: peer},
            device_id_type=MESH_ID,
        )
        copy.start()
        copies.append(copy)
    return copies


def received(copies):
    for copy in copies:
        copy.wait_recv()


def sent(copies):
    for copy in copies:
        copy.wait_send()


def load_all(pairs, sems):
    copies = [pltpu.make_async_copy(src, dst, sems.at[i]) for i, (src, dst) in enumerate(pairs)]
    for copy in copies:
        copy.start()
    return copies


def silu(value):
    return value / (1.0 + jnp.exp(-value))


def square_block(squares):
    head = squares.astype(jnp.bfloat16).astype(jnp.float32)
    rest = squares - head
    lane = lax.broadcasted_iota(jnp.int32, (squares.shape[0], LANES), 1)
    return jnp.where(lane < LANES // 2, head, rest).astype(jnp.bfloat16)


def square_total(block):
    return block[:, :1] + block[:, LANES // 2 : LANES // 2 + 1]


def remote(axis, peer, source, target, send_sem, recv_sem):
    return pltpu.make_async_remote_copy(
        src_ref=source, dst_ref=target, send_sem=send_sem, recv_sem=recv_sem,
        device_id={axis: peer}, device_id_type=MESH_ID,
    )


def start_gather(slots, tp, n_tp, send_sems, recv_sems):
    chips = n_tp // CORES
    chip, core = tp // CORES, lax.rem(tp, CORES)
    partner = chip * CORES + 1 - core
    direct = []
    for step in range(1, chips):
        peer = lax.rem(chip + step, chips) * CORES + core
        direct.append(
            remote("tp", peer, slots.at[tp], slots.at[tp], send_sems.at[step], recv_sems.at[step])
        )
    across = [remote("tp", partner, slots.at[tp], slots.at[tp], send_sems.at[0], recv_sems.at[0])]
    for copy in direct + across:
        copy.start()

    def relay():
        for step in range(1, chips):
            direct[step - 1].wait_recv()
            slot = lax.rem(chip - step + chips, chips) * CORES + core
            i = chips - 1 + step
            copy = remote(
                "tp", partner, slots.at[slot], slots.at[slot], send_sems.at[i], recv_sems.at[i]
            )
            copy.start()
            across.append(copy)

    def finish():
        received(across)
        return direct + across

    return relay, finish


def start_reduce(lhs, weight, parts, swapped, tp, n_tp, send_sems, recv_sems):
    chips = n_tp // CORES
    chip, core = tp // CORES, lax.rem(tp, CORES)
    columns = parts.shape[3]

    def multiply(side):
        starts = [pl.multiple_of((z * CORES + side) * columns, LANES) for z in range(chips)]
        rhs = jnp.concatenate([weight[:, pl.ds(start, columns)] for start in starts], axis=1)
        full = jnp.dot(lhs, rhs, preferred_element_type=jnp.float32).astype(jnp.bfloat16)
        for z in range(chips):
            parts[side, z] = full[:, z * columns : (z + 1) * columns]

    multiply(1 - core)
    swap = remote(
        "tp", chip * CORES + 1 - core, parts.at[1 - core], swapped, send_sems.at[0], recv_sems.at[0]
    )
    swap.start()
    multiply(core)
    return swap


def spread_pairs(swap, parts, swapped, staged, landed, tp, n_tp, send_sems, recv_sems):
    chips = n_tp // CORES
    chip, core = tp // CORES, lax.rem(tp, CORES)
    swap.wait_recv()
    copies = []
    for step in range(1, chips):
        other = lax.rem(chip + step, chips)
        pair = parts[core, other].astype(jnp.float32) + swapped[other].astype(jnp.float32)
        staged[step - 1] = pair.astype(jnp.bfloat16)
        copy = remote(
            "tp", other * CORES + core, staged.at[step - 1], landed.at[step - 1],
            send_sems.at[step], recv_sems.at[step],
        )
        copy.start()
        copies.append(copy)
    return copies


def pairs_total(copies, parts, swapped, landed, tp):
    chip, core = tp // CORES, lax.rem(tp, CORES)
    total = parts[core, chip].astype(jnp.float32) + swapped[chip].astype(jnp.float32)
    for step, copy in enumerate(copies):
        copy.wait_recv()
        total += landed[step].astype(jnp.float32)
    return total


def total_of(own, landed):
    total = own.astype(jnp.float32)
    for step in range(landed.shape[0]):
        total += landed[step].astype(jnp.float32)
    return total


def layer_kernel(
    n_kv, n_tp, features,
    tokens_hbm, lengths_hbm, freq_hbm, gain_hbm, gain_two_hbm, state_hbm,
    wq_hbm, wk_hbm, wv_hbm, wg_hbm, wo_hbm, fg_hbm, fu_hbm, fd_hbm,
    out, state, s, sems,
):
    kv, tp = lax.axis_index("kv"), lax.axis_index("tp")
    chips = n_tp // CORES
    chip, core = tp // CORES, lax.rem(tp, CORES)
    gathered, gathered_two, merged, hidden = s["gathered"], s["gathered_two"], s["merged"], s["hidden"]
    halves, rows = gathered.shape[0], gathered.shape[3]
    batch = n_kv * rows
    names = ("wq", "wk", "wv", "wg", "gain_two", "wo", "fg", "fu", "fd")
    sources = (wq_hbm, wk_hbm, wv_hbm, wg_hbm, gain_two_hbm, wo_hbm, fg_hbm, fu_hbm, fd_hbm)
    pairs = [(tokens_hbm.at[:, h], gathered.at[h, tp]) for h in range(halves)]
    pairs += [(lengths_hbm, s["lengths"]), (freq_hbm, s["freq"]), (gain_hbm, s["gain"])]
    pairs += [(ref, s[name]) for ref, name in zip(sources[:4], names[:4])]
    pairs += [(state_hbm, state)]
    pairs += [(ref, s[name]) for ref, name in zip(sources[4:], names[4:])]
    loads = load_all(pairs, sems["load"])
    order = ["tokens"] * halves + ["lengths", "freq", "gain"] + list(names[:4]) + ["state"] + list(names[4:])

    def ready(*wanted):
        for name, copy in zip(order, loads):
            if name in wanted:
                copy.wait()

    along = [lax.rem(chip + step, chips) * CORES + core for step in range(1, chips)]
    greet([
        ("tp", along + [chip * CORES + 1 - core]),
        ("kv", [lax.rem(kv + step, n_kv) for step in range(1, n_kv)]),
    ])
    open_sends = []

    def pair_of(name, h):
        return sems[name + "_s"].at[h], sems[name + "_r"].at[h]

    def kv_send(name, h, source, target):
        copies = send_all("kv", n_kv, kv, source, target, *pair_of(name, h))
        open_sends.extend(copies)
        return copies

    ready("tokens")
    first_gather = [
        start_gather(gathered.at[h], tp, n_tp, *pair_of("g", h)) for h in range(halves)
    ]
    ready("lengths", "freq", "gain")
    all_rows = halves * rows
    row = lax.broadcasted_iota(jnp.int32, (all_rows, all_rows), 0)
    col = lax.broadcasted_iota(jnp.int32, (all_rows, all_rows), 1)
    spread = jnp.where(row == col, s["lengths"][...].astype(jnp.float32), 0.0)
    angles = jnp.sum(spread, axis=1, keepdims=True) * s["freq"][...]
    cosine, sine = jnp.cos(angles), jnp.sin(angles)
    lane = lax.broadcasted_iota(jnp.int32, angles.shape, 1)
    sine = jnp.where(lane < QK // 2, -sine, sine)

    def normalise(slots, gains):
        x = jnp.concatenate(
            [slots[j].reshape(batch, slots.shape[3]) for j in range(slots.shape[0])], axis=1
        ).astype(jnp.float32)
        squares = jnp.sum(x * x, axis=1, keepdims=True)
        return (x * gains[...]).astype(jnp.bfloat16), square_block(squares).reshape(n_kv, rows, LANES)

    def project(lhs, weight):
        full = jnp.dot(lhs, weight[...], preferred_element_type=jnp.float32)
        return full.astype(jnp.bfloat16).reshape(n_kv, rows, full.shape[1])

    q_width, v_width = s["wq"].shape[1], s["wv"].shape[1]
    units = s["fg"].shape[1]
    heads = q_width // QK
    width = v_width // heads
    out_a, out_b, in_a, in_b = s["out_a"], s["out_b"], s["in_a"], s["in_b"]
    first, second, copies_m = [], [], []

    def project_first(h):
        normed, squares = normalise(gathered.at[h], s["gain"])
        out_a[h, :, :, 2 * q_width :] = squares
        ready_once("wq", "wk", h)
        out_a[h, :, :, :q_width] = project(normed, s["wq"])
        out_a[h, :, :, q_width : 2 * q_width] = project(normed, s["wk"])
        first.append(kv_send("a", h, lambda p: out_a.at[h, p], lambda n: in_a.at[h, n - 1]))
        ready_once("wv", "wg", h)
        out_b[h, :, :, :v_width] = project(normed, s["wv"])
        out_b[h, :, :, v_width:] = project(normed, s["wg"])
        second.append(kv_send("b", h, lambda p: out_b.at[h, p], lambda n: in_b.at[h, n - 1]))

    def ready_once(*args):
        if args[-1] == 0:
            ready(*args[:-1])

    decays = []
    for head in range(heads):
        number = jnp.full((1, width), tp * heads + head, jnp.int32).astype(jnp.float32)
        decays.append(1.0 - jnp.exp2(-5.0 - 10.0 * number / (heads * n_tp - 1)))
    qk, value, retained = s["qk"], s["value"], s["retained"]

    def attend(h):
        base = h * rows
        received(first[h])
        total = total_of(out_a[h, kv], in_a.at[h])
        scale = lax.rsqrt(square_total(total[:, 2 * q_width :]) / features + 1e-06)
        total = total * scale
        cosines, sines = cosine[base : base + rows], sine[base : base + rows]
        blocks = []
        for start, factor in ((0, 1.0), (q_width, QK ** (-0.5))):
            for head in range(heads):
                part = total[:, start + head * QK : start + (head + 1) * QK]
                turned = (part * cosines + pltpu.roll(part, QK // 2, 1) * sines) * factor
                blocks.append(turned.astype(jnp.bfloat16).astype(jnp.float32))
        columns = jnp.concatenate(blocks * (LANES // (len(blocks) * rows)), axis=0).T
        qk[h] = columns
        for i in range(rows):
            for head in range(heads):
                query = columns[:, head * rows + i : head * rows + i + 1]
                retained[base + i : base + i + 1, head * width : (head + 1) * width] = jnp.sum(
                    query * state[base + i, head], axis=0, keepdims=True
                )
        received(second[h])
        total = total_of(out_b[h, kv], in_b.at[h]) * scale
        values = total[:, :v_width].astype(jnp.bfloat16).astype(jnp.float32)
        value[base : base + rows] = values
        pieces = []
        for head in range(heads):
            overlap = jnp.sum(blocks[head] * blocks[heads + head], axis=1, keepdims=True)
            span = slice(head * width, (head + 1) * width)
            piece = decays[head] * retained[base : base + rows, span] + overlap * values[:, span]
            pieces.append(piece * lax.rsqrt(jnp.mean(piece * piece, axis=1, keepdims=True) + 1e-06))
        merged[h, kv] = (jnp.concatenate(pieces, axis=1) * silu(total[:, v_width:])).astype(jnp.bfloat16)
        copies_m.append(kv_send("m", h, lambda p: merged.at[h, kv], lambda n: merged.at[h, kv]))

    block = 8

    def update(h):
        base = h * rows

        def update_step(i, carry):
            start = i * block
            turned = pltpu.roll(qk[h], lax.rem(LANES - start, LANES), 1)
            for n in range(block):
                for head in range(heads):
                    lane = (heads + head) * rows + n
                    at = base + start + n
                    outer = turned[:, lane : lane + 1] * value[pl.ds(at, 1), head * width : (head + 1) * width]
                    state[at, head] = decays[head] * state[at, head] + outer
            return carry

        lax.fori_loop(0, rows // block, update_step, 0)

    def reduce_start(h, lhs, weight, tag):
        return start_reduce(
            lhs, s[weight], s["parts_" + tag].at[h], s["swapped_" + tag].at[h], tp, n_tp, *pair_of(tag, h)
        )

    def reduce_spread(h, swap, tag):
        copies = spread_pairs(
            swap, s["parts_" + tag].at[h], s["swapped_" + tag].at[h], s["staged_" + tag].at[h],
            s["landed_" + tag].at[h], tp, n_tp, *pair_of(tag, h)
        )
        open_sends.extend(copies + [swap])
        return copies

    def reduce_total(h, copies, tag):
        return pairs_total(
            copies, s["parts_" + tag].at[h], s["swapped_" + tag].at[h], s["landed_" + tag].at[h], tp
        )

    gate_out, up_out, gate_in, up_in = s["gate_out"], s["up_out"], s["gate_in"], s["up_in"]
    copies_e, copies_f, copies_h = [], [], []

    def project_second(h):
        normed, squares = normalise(gathered_two.at[h], s["gain_two"])
        gate_out[h, :, :, units:] = squares
        gate_out[h, :, :, :units] = project(normed, s["fg"])
        copies_e.append(kv_send("e", h, lambda p: gate_out.at[h, p], lambda n: gate_in.at[h, n - 1]))
        up_out[h] = project(normed, s["fu"])
        copies_f.append(kv_send("f", h, lambda p: up_out.at[h, p], lambda n: up_in.at[h, n - 1]))

    def activate(h):
        received(copies_e[h])
        total = total_of(gate_out[h, kv], gate_in.at[h])
        scale = lax.rsqrt(square_total(total[:, units:]) / features + 1e-06)
        activated = silu(total[:, :units] * scale)
        received(copies_f[h])
        hidden[h, kv] = (activated * (total_of(up_out[h, kv], up_in.at[h]) * scale)).astype(jnp.bfloat16)
        copies_h.append(kv_send("h", h, lambda p: hidden.at[h, kv], lambda n: hidden.at[h, kv]))

    for relay, _ in first_gather:
        relay()
    for h in range(halves):
        open_sends.extend(first_gather[h][1]())
        project_first(h)
    ready("state")
    for h in range(halves):
        attend(h)
    ready("wo")
    spread_o = []
    for h in range(halves):
        received(copies_m[h])
        swap = reduce_start(h, merged[h].reshape(batch, v_width), "wo", "x")
        spread_o.append(reduce_spread(h, swap, "x"))
        update(h)
    second_gather = []
    for h in range(halves):
        total = reduce_total(h, spread_o[h], "x")
        own = gathered[h, tp].reshape(batch, LANES).astype(jnp.float32)
        gathered_two[h, tp] = (own + total).astype(jnp.bfloat16).reshape(n_kv, rows, LANES)
        second_gather.append(start_gather(gathered_two.at[h], tp, n_tp, *pair_of("c", h)))
    ready("gain_two", "fg", "fu")
    for h in range(halves):
        second_gather[h][0]()
        open_sends.extend(second_gather[h][1]())
        project_second(h)
    for h in range(halves):
        activate(h)
    ready("fd")
    spread_d = []
    for h in range(halves):
        received(copies_h[h])
        swap = reduce_start(h, hidden[h].reshape(batch, units), "fd", "d")
        spread_d.append(reduce_spread(h, swap, "d"))
    for h in range(halves):
        total = reduce_total(h, spread_d[h], "d")
        own = gathered_two[h, tp].reshape(batch, LANES).astype(jnp.float32)
        out[:, h] = (own + total).astype(jnp.bfloat16).reshape(n_kv, rows, LANES)
    sent(open_sends)


def finish_kernel(state, out, state_to, out_to, store_sems):
    chunks = store_sems.shape[0] - 1
    size = state.shape[0] // chunks
    targets = [(out, out_to)]
    for i in range(chunks):
        part = pl.ds(i * size, size)
        targets.append((state.at[part], state_to.at[part]))
    for copy in load_all(targets, store_sems):
        copy.wait()


HALVES = 2


def fused_on_device(n_kv, n_tp, *arrays):
    (
        tokens, lengths, state, mixer_gain, wq, wk, wv, wg, wo, channel_gain, fg, fu, fd,
    ) = arrays
    columns = tokens.shape[1]
    rows = state.shape[0] // HALVES
    batch = n_kv * rows
    depth, q_width = wq.shape
    v_width, units = wv.shape[1], fg.shape[1]
    bf16, f32 = jnp.bfloat16, jnp.float32
    vmem = pl.BlockSpec(memory_space=pltpu.VMEM)
    hbm = pl.BlockSpec(memory_space=pltpu.HBM)
    chips = n_tp // CORES
    index = np.arange(QK) % (QK // 2)
    freq = jnp.asarray((10000.0 ** (-index / (QK // 2))).astype(np.float32))[None, :]
    a_width, b_width = 2 * q_width + LANES, 2 * v_width

    def buffer(*shape, dtype=bf16):
        return pltpu.VMEM((HALVES,) + shape, dtype)

    scratch = {
        "lengths": pltpu.VMEM((1, HALVES * rows), jnp.int32),
        "freq": pltpu.VMEM((1, QK), f32),
        "gain": pltpu.VMEM((1, depth), f32),
        "gain_two": pltpu.VMEM((1, depth), f32),
        "gathered": buffer(n_tp, n_kv, rows, columns),
        "gathered_two": buffer(n_tp, n_kv, rows, columns),
        "out_a": buffer(n_kv, rows, a_width),
        "out_b": buffer(n_kv, rows, b_width),
        "in_a": buffer(n_kv - 1, rows, a_width),
        "in_b": buffer(n_kv - 1, rows, b_width),
        "qk": buffer(QK, LANES, dtype=f32),
        "retained": pltpu.VMEM((HALVES * rows, v_width), f32),
        "value": pltpu.VMEM((HALVES * rows, v_width), f32),
        "merged": buffer(n_kv, rows, v_width),
        "gate_out": buffer(n_kv, rows, units + LANES),
        "up_out": buffer(n_kv, rows, units),
        "gate_in": buffer(n_kv - 1, rows, units + LANES),
        "up_in": buffer(n_kv - 1, rows, units),
        "hidden": buffer(n_kv, rows, units),
    }
    weights = {"wq": wq, "wk": wk, "wv": wv, "wg": wg, "wo": wo, "fg": fg, "fu": fu, "fd": fd}
    scratch.update({name: pltpu.VMEM(w.shape, bf16) for name, w in weights.items()})
    for tag in ("x", "d"):
        scratch["parts_" + tag] = buffer(CORES, chips, batch, columns)
        scratch["swapped_" + tag] = buffer(chips, batch, columns)
        scratch["staged_" + tag] = buffer(chips - 1, batch, columns)
        scratch["landed_" + tag] = buffer(chips - 1, batch, columns)
    counts = {"g": n_tp - 1, "c": n_tp - 1, "x": chips, "d": chips}
    counts.update({tag: n_kv - 1 for tag in ("a", "b", "m", "e", "f", "h")})
    sems = {"load": pltpu.SemaphoreType.DMA((HALVES + 13,))}
    for tag, count in counts.items():
        sems[tag + "_s"] = sems[tag + "_r"] = pltpu.SemaphoreType.DMA((HALVES, count))
    operands = (
        tokens.reshape(n_kv, HALVES, rows, columns), lengths[None, :], freq, mixer_gain[None, :],
        channel_gain[None, :], state, wq, wk, wv, wg, wo, fg, fu, fd,
    )
    out_shape = (n_kv, HALVES, rows, columns)
    out, new_state = pl.pallas_call(
        functools.partial(layer_kernel, n_kv, n_tp, depth * n_kv),
        out_shape=(pltpu.VMEM(out_shape, bf16), pltpu.VMEM(state.shape, f32)),
        in_specs=[hbm] * 14,
        out_specs=(vmem, vmem),
        scratch_shapes=[scratch, sems],
        compiler_params=pltpu.CompilerParams(
            collective_id=0, has_side_effects=True, vmem_limit_bytes=LAYER_VMEM
        ),
        name="layer",
    )(*[pltpu.with_memory_space_constraint(a, pltpu.HBM) for a in operands])
    new_state, out = pl.pallas_call(
        finish_kernel,
        out_shape=(
            jax.ShapeDtypeStruct(state.shape, f32),
            jax.ShapeDtypeStruct(out_shape, bf16),
        ),
        in_specs=[vmem, vmem],
        out_specs=(hbm, hbm),
        scratch_shapes=[pltpu.SemaphoreType.DMA((9,))],
        compiler_params=pltpu.CompilerParams(vmem_limit_bytes=FINISH_VMEM),
        name="finish",
    )(new_state, out)
    return out.reshape(tokens.shape), new_state


def fits(n_kv, n_tp, arrays):
    tokens, state, ffn_gate = arrays[0], arrays[2], arrays[10]
    rows, heads = state.shape[0], state.shape[1]
    return (
        tokens.shape[1] % LANES == 0
        and n_tp % CORES == 0
        and n_tp > CORES
        and n_kv > 1
        and 4 * state.size < VMEM_TOTAL // 4
        and ffn_gate.shape[1] % LANES == 0
        and tokens.shape[1] == LANES
        and tokens.shape[0] == n_kv * rows
        and rows % (16 * HALVES) == 0
        and 2 * heads * rows == LANES
        and state.shape[2] == QK == LANES
        and state.shape[3] % LANES == 0
    )


def per_device(n_kv, n_tp, *arrays):
    if fits(n_kv, n_tp, arrays):
        return fused_on_device(n_kv, n_tp, *arrays)
    return on_device(*arrays)


def solution(mesh):
    in_specs = (
        P(None, ("kv", "tp")),
        P("kv"),
        P("kv", "tp", None, None),
        P("kv"),
        P("kv", "tp"),
        P("kv", "tp"),
        P("kv", "tp"),
        P("kv", "tp"),
        P("tp", "kv"),
        P("kv"),
        P("kv", "tp"),
        P("kv", "tp"),
        P("tp", "kv"),
    )
    out_specs = (P(None, ("kv", "tp")), P("kv", "tp", None, None))
    return jax.shard_map(
        functools.partial(per_device, mesh.shape["kv"], mesh.shape["tp"]),
        mesh=mesh, in_specs=in_specs, out_specs=out_specs, check_vma=False
    )
```

```python
import functools

import jax
import jax.numpy as jnp
import numpy as np
from jax import lax
from jax.experimental import pallas as pl
from jax.experimental.pallas import tpu as pltpu
from jax.sharding import PartitionSpec as P

D = 4096
HEADS = 16
QK = 128
LANES = 128


def rotate_heads(vectors, positions):
    half_dim = vectors.shape[-1] // 2
    frequency = 10000.0 ** (-jnp.arange(half_dim, dtype=jnp.float32) / half_dim)
    angles = positions.astype(jnp.float32)[:, None, None] * frequency
    cosine = jnp.cos(angles)
    sine_part = jnp.sin(angles)
    first_half = vectors[..., :half_dim]
    second = vectors[..., half_dim:]
    return jnp.concatenate(
        [first_half * cosine - second * sine_part, first_half * sine_part + second * cosine],
        axis=-1,
    )


def gathered_rows(columns):
    return lax.all_gather(columns, "tp", axis=1, tiled=True)


def owned_sums(partial_value, squares):
    raw_sums, totals = (
        lax.psum_scatter(
            partial_value.astype(jnp.bfloat16), "kv", scatter_dimension=0, tiled=True
        ).astype(jnp.float32),
        lax.psum_scatter(
            squares.astype(jnp.bfloat16), "kv", scatter_dimension=0, tiled=True
        ).astype(jnp.float32),
    )
    summed = raw_sums * lax.rsqrt(totals / D + 1e-06)[:, None]
    return summed


def every_sum(partial_value, squares):
    raw_sums, totals = (
        lax.psum(partial_value.astype(jnp.bfloat16), "kv").astype(jnp.float32),
        lax.psum(squares.astype(jnp.bfloat16), "kv").astype(jnp.float32),
    )
    summed = raw_sums * lax.rsqrt(totals / D + 1e-06)[:, None]
    return summed


def on_device(
    tokens,
    lengths,
    retention_state,
    mixer_gain,
    query_weight,
    key_weight,
    value_weight,
    gate_weight,
    output_weight,
    channel_gain,
    ffn_gate,
    ffn_up,
    ffn_down,
):
    feature_block = gathered_rows(tokens).astype(jnp.float32)
    squares = jnp.sum(feature_block * feature_block, axis=1)
    normed = (feature_block * mixer_gain).astype(jnp.bfloat16)
    partial_value = jnp.concatenate(
        [
            jnp.dot(normed, query_weight, preferred_element_type=jnp.float32),
            jnp.dot(normed, key_weight, preferred_element_type=jnp.float32),
            jnp.dot(normed, value_weight, preferred_element_type=jnp.float32),
            jnp.dot(normed, gate_weight, preferred_element_type=jnp.float32),
        ],
        axis=1,
    )
    owned_rows = owned_sums(partial_value, squares)
    local_heads = query_weight.shape[1] // QK
    q_width = query_weight.shape[1]
    v_width = value_weight.shape[1]
    head_width = v_width // local_heads
    seq_rows = owned_rows.shape[0]
    query_rows = rotate_heads(
        owned_rows[:, :q_width].reshape(seq_rows, local_heads, QK), lengths
    ).astype(jnp.bfloat16)
    key_rows = (
        rotate_heads(
            owned_rows[:, q_width : 2 * q_width].reshape(seq_rows, local_heads, QK), lengths
        )
        * QK ** (-0.5)
    ).astype(jnp.bfloat16)
    value_rows = (
        owned_rows[:, 2 * q_width : 2 * q_width + v_width]
        .astype(jnp.bfloat16)
        .reshape(seq_rows, local_heads, head_width)
    )
    gate_rows = owned_rows[:, 2 * q_width + v_width :]
    head_ids = (lax.axis_index("tp") * local_heads + jnp.arange(local_heads)).astype(jnp.float32)
    decay_rate = 1.0 - 2.0 ** (-5.0 - 10.0 * head_ids / (HEADS - 1))
    new_state = (
        decay_rate[None, :, None, None] * retention_state
        + key_rows.astype(jnp.float32)[..., :, None] * value_rows.astype(jnp.float32)[..., None, :]
    )
    retained = jnp.einsum(
        "bhk,bhkv->bhv", query_rows.astype(jnp.float32), new_state, precision=lax.Precision.HIGHEST
    )
    normalized = retained * lax.rsqrt(jnp.mean(retained * retained, axis=-1) + 1e-06)[..., None]
    merged = (normalized.reshape(seq_rows, v_width) * jax.nn.silu(gate_rows)).astype(jnp.bfloat16)
    mixed_part = jnp.dot(
        lax.all_gather(merged, "kv", axis=0, tiled=True),
        output_weight,
        preferred_element_type=jnp.float32,
    )
    mixed_cols = lax.psum_scatter(
        mixed_part.astype(jnp.bfloat16), "tp", scatter_dimension=1, tiled=True
    ).astype(jnp.float32)
    residual = (tokens.astype(jnp.float32) + mixed_cols).astype(jnp.bfloat16)
    block_two = gathered_rows(residual).astype(jnp.float32)
    squares_two = jnp.sum(block_two * block_two, axis=1)
    normed_two = (block_two * channel_gain).astype(jnp.bfloat16)
    partial_two = jnp.concatenate(
        [
            jnp.dot(normed_two, ffn_gate, preferred_element_type=jnp.float32),
            jnp.dot(normed_two, ffn_up, preferred_element_type=jnp.float32),
        ],
        axis=1,
    )
    hidden_units = ffn_gate.shape[1]
    summed = every_sum(partial_two, squares_two)
    hidden = (jax.nn.silu(summed[:, :hidden_units]) * summed[:, hidden_units:]).astype(jnp.bfloat16)
    down_part = jnp.dot(hidden, ffn_down, preferred_element_type=jnp.float32)
    down_sums = lax.psum_scatter(
        down_part.astype(jnp.bfloat16), "tp", scatter_dimension=1, tiled=True
    ).astype(jnp.float32)
    layer_output = (residual.astype(jnp.float32) + down_sums).astype(jnp.bfloat16)
    return (layer_output, new_state)


MESH_ID = pl.DeviceIdType.MESH
VMEM_TOTAL = 67043328
CORES = 2
SIDE = 2
LAYER_VMEM = 50000000
FINISH_VMEM = 20000000


def greet(devices):
    barrier = pltpu.get_barrier_semaphore()
    for device in devices:
        pl.semaphore_signal(barrier, inc=1, device_id=device, device_id_type=MESH_ID)
    pl.semaphore_wait(barrier, len(devices))


def kv_peers(kv, n_kv):
    return [n_kv - 1 - kv, kv + 1 - 2 * lax.rem(kv, SIDE), lax.rem(kv + SIDE, n_kv)]


def send_all(devices, source, target, send_sem, recv_sem):
    for k, device in enumerate(devices):
        remote_to(device, source(device["kv"]), target(k), send_sem, recv_sem).start()


def landed(ref, sem):
    pltpu.make_async_copy(ref, ref, sem).wait()


def load_all(pairs, sem):
    for source, target in pairs:
        pltpu.make_async_copy(source, target, sem).start()


def silu(value):
    return value / (1.0 + jnp.exp(-value))


def as_row(column):
    lane = lax.broadcasted_iota(jnp.int32, (column.shape[0], LANES), 1)
    row = lax.broadcasted_iota(jnp.int32, (column.shape[0], LANES), 0)
    return jnp.sum(jnp.where(row == lane, column, 0.0), axis=0, keepdims=True)


def as_column(row_values, first, rows):
    lane = lax.broadcasted_iota(jnp.int32, (rows, LANES), 1)
    row = lax.broadcasted_iota(jnp.int32, (rows, LANES), 0)
    return jnp.sum(jnp.where(row + first == lane, row_values, 0.0), axis=1, keepdims=True)


def remote(axis, peer, source, target, send_sem, recv_sem):
    return remote_to({axis: peer}, source, target, send_sem, recv_sem)


def remote_to(device, source, target, send_sem, recv_sem):
    return pltpu.make_async_remote_copy(
        src_ref=source, dst_ref=target, send_sem=send_sem, recv_sem=recv_sem,
        device_id=device, device_id_type=MESH_ID,
    )


def far_first(chip, chips):
    def ascending(at, k):
        return k + 1 - (at + chips - 1 - k) // chips

    low = 1 - chip // (chips // 2)
    mirrored = chips - 1 - chip
    return [
        low * (chips - 1 - ascending(mirrored, k)) + (1 - low) * ascending(chip, k)
        for k in range(chips - 1)
    ]


def start_gather(slots, tp, n_tp, hub, send_sems, recv_sems):
    chips = n_tp // CORES
    chip, core = tp // CORES, lax.rem(tp, CORES)
    partner = chip * CORES + 1 - core
    order = far_first(chip, chips)

    def block(peer, slot, send):
        return remote("tp", peer, slots.at[slot], slots.at[slot], send_sems.at[send], recv_sems.at[slot])

    for peer in order:
        block(peer * CORES + hub, tp, 0).start()
    block(partner, tp, 0).start()
    relayed = [
        block(partner, source * CORES + side, 1) for source in order[::-1] for side in range(CORES)
    ]

    def take(first, last):
        for copy in relayed[first * CORES : last * CORES]:
            copy.wait_recv()

            @pl.when(core == hub)
            def _():
                copy.start()

    def take_own():
        block(partner, partner, 0).wait_recv()

    def close():
        landed(slots.at[:chips], send_sems.at[0])

        @pl.when(core == hub)
        def _():
            landed(slots.at[: len(relayed)], send_sems.at[1])

    return take, take_own, close


def start_reduce(lhs, weight, parts, swapped, tp, send_sems, recv_sems):
    chip, core = tp // CORES, lax.rem(tp, CORES)
    chips, columns = parts.shape[1], parts.shape[3]

    def multiply(side):
        full = jnp.dot(lhs, weight[side], preferred_element_type=jnp.float32).astype(jnp.bfloat16)
        for z in range(chips):
            parts[side, z] = full[:, z * columns : (z + 1) * columns]

    multiply(core)
    remote(
        "tp", chip * CORES + 1 - core, parts.at[core], swapped, send_sems.at[0], recv_sems.at[0]
    ).start()
    multiply(1 - core)


def spread_pairs(parts, swapped, staged, into, tp, send_sems, recv_sems):
    chips = parts.shape[1]
    chip, core = tp // CORES, lax.rem(tp, CORES)
    landed(swapped, recv_sems.at[0])
    for k, other in enumerate(far_first(chip, chips) + [chip]):
        pair = parts[1 - core, other].astype(jnp.float32) + swapped[other].astype(jnp.float32)
        staged[k] = pair.astype(jnp.bfloat16)
        remote(
            "tp", other * CORES + 1 - core, staged.at[k], into.at[chip], send_sems.at[1], recv_sems.at[1]
        ).start()


def total_of(own, others):
    total = own.astype(jnp.float32)
    for step in range(others.shape[0]):
        total += others[step].astype(jnp.float32)
    return total


def layer_kernel(
    n_kv, n_tp, features,
    tokens_hbm, lengths_hbm, freq_hbm, gain_hbm, gain_two_hbm, state_hbm,
    wq_hbm, wk_hbm, wv_hbm, wg_hbm, wo_hbm, fg_hbm, fu_hbm, fd_hbm,
    out, state, s, sems,
):
    kv, tp = lax.axis_index("kv"), lax.axis_index("tp")
    chips = n_tp // CORES
    chip, core = tp // CORES, lax.rem(tp, CORES)
    gathered, gathered_two, merged, hidden = s["gathered"], s["gathered_two"], s["merged"], s["hidden"]
    halves, rows = gathered.shape[0], gathered.shape[3]
    batch = n_kv * rows
    q_width, v_width = wq_hbm.shape[1], wv_hbm.shape[1]
    units, columns = fg_hbm.shape[1], tokens_hbm.shape[3]

    def sides(ref, target):
        return [
            (
                ref.at[:, (z * CORES + side) * columns : (z * CORES + side + 1) * columns],
                target.at[side, :, z * columns : (z + 1) * columns],
            )
            for side in range(CORES)
            for z in range(chips)
        ]

    groups = {
        "tokens": [(tokens_hbm.at[:, h], gathered.at[h, tp]) for h in range(halves)],
        "lengths": [(lengths_hbm, s["lengths"])],
        "freq": [(freq_hbm, s["freq"])],
        "gain": [(gain_hbm, s["gain"])],
        "wqk": [(wq_hbm, s["wqk"].at[:, :q_width]), (wk_hbm, s["wqk"].at[:, q_width:])],
        "wvg": [(wv_hbm, s["wvg"].at[:, :v_width]), (wg_hbm, s["wvg"].at[:, v_width:])],
        "state": [(state_hbm, state)],
        "wo": sides(wo_hbm, s["wo"]),
        "gain_two": [(gain_two_hbm, s["gain_two"])],
        "fg": [(fg_hbm, s["fg"])],
        "fu": [(fu_hbm, s["fu"])],
        "fd": sides(fd_hbm, s["fd"]),
    }
    wholes = {
        "tokens": gathered.at[:, tp], "wqk": s["wqk"], "wvg": s["wvg"], "state": state, "wo": s["wo"], "fd": s["fd"],
        "lengths": s["lengths"], "freq": s["freq"], "gain": s["gain"],
        "gain_two": s["gain_two"], "fg": s["fg"], "fu": s["fu"],
    }
    pending = {}
    for i, (name, group) in enumerate(groups.items()):
        pending[name] = i
        load_all(group, sems["load"].at[i])

    def ready(*wanted):
        for name in wanted:
            if name in pending:
                landed(wholes[name], sems["load"].at[pending.pop(name)])

    partner = chip * CORES + 1 - core
    peers = [{"kv": peer, "tp": tp} for peer in kv_peers(kv, n_kv)]
    crossed = [{"kv": peer, "tp": partner} for peer in kv_peers(kv, n_kv)]
    along = [{"kv": kv, "tp": other * CORES + 1 - core} for other in far_first(chip, chips)]
    beside = {"kv": kv, "tp": partner}
    aside = [{"kv": kv, "tp": other * CORES + core} for other in far_first(chip, chips)]
    greet(along + aside + [beside] + peers + crossed)
    closing = []

    def pair_of(name, h):
        return sems[name + "_s"].at[h], sems[name + "_r"].at[h]

    def kv_send(name, h, devices, source, target, extent):
        send_sem, recv_sem = sems[name].at[h, 0], sems[name].at[h, 1]
        send_all(devices, source, target, send_sem, recv_sem)
        closing.append((extent, send_sem))
        return lambda: landed(extent, recv_sem)

    def send_squares(name, h, squares):
        s[name][h, n_kv - 1] = squares
        return kv_send(
            name, h, crossed, lambda p: s[name].at[h, n_kv - 1], lambda n: s[name].at[h, n], s[name].at[h, : n_kv - 1]
        )

    def scale_of(name, h, wait):
        wait()
        total = s[name][h, 0]
        for n in range(1, n_kv):
            total += s[name][h, n]
        return lax.rsqrt(as_column(total, kv * rows, rows) / features + 1e-06)

    ready("tokens")
    first_gather = [start_gather(gathered.at[0], tp, n_tp, 0, *pair_of("g", 0))]
    ready("lengths", "freq", "gain")
    all_rows = halves * rows
    row = lax.broadcasted_iota(jnp.int32, (all_rows, all_rows), 0)
    col = lax.broadcasted_iota(jnp.int32, (all_rows, all_rows), 1)
    spread = jnp.where(row == col, s["lengths"][...].astype(jnp.float32), 0.0)
    angles = jnp.sum(spread, axis=1, keepdims=True) * s["freq"][...]
    cosine, sine = jnp.cos(angles), jnp.sin(angles)
    lane = lax.broadcasted_iota(jnp.int32, angles.shape, 1)
    sine = jnp.where(lane < QK // 2, -sine, sine)

    def normalise(slots, gains):
        x = jnp.concatenate(
            [slots[j].reshape(batch, slots.shape[3]) for j in range(slots.shape[0])], axis=1
        ).astype(jnp.float32)
        squares = jnp.sum(x * x, axis=1, keepdims=True)
        return (x * gains[...]).astype(jnp.bfloat16), as_row(squares)

    def project(lhs, weight):
        full = jnp.dot(lhs, weight[...], preferred_element_type=jnp.float32)
        return full.astype(jnp.bfloat16).reshape(n_kv, rows, full.shape[1])

    heads = q_width // QK
    width = v_width // heads
    out_a, out_b, in_a, in_b = s["out_a"], s["out_b"], s["in_a"], s["in_b"]
    first, second, copies_m, copies_q = [], [], [], []

    def project_first(h):
        normed, squares = normalise(gathered.at[h], s["gain"])
        ready("wqk")
        out_a[h] = project(normed, s["wqk"])
        first.append(kv_send("a", h, peers, lambda p: out_a.at[h, p], lambda n: in_a.at[h, n], in_a.at[h]))
        ready("wvg")
        out_b[h] = project(normed, s["wvg"])
        copies_q.append(send_squares("squares", h, squares))
        second.append(kv_send("b", h, peers, lambda p: out_b.at[h, p], lambda n: in_b.at[h, n], in_b.at[h]))

    decays = []
    for head in range(heads):
        number = jnp.full((1, width), tp * heads + head, jnp.int32).astype(jnp.float32)
        decays.append(1.0 - jnp.exp2(-5.0 - 10.0 * number / (heads * n_tp - 1)))
    qk, value, retained = s["qk"], s["value"], s["retained"]

    def attend(h):
        base = h * rows
        first[h]()
        total = total_of(out_a[h, kv], in_a.at[h])
        scale = scale_of("squares", h, copies_q[h])
        total = total * scale
        cosines, sines = cosine[base : base + rows], sine[base : base + rows]
        blocks = []
        for start, factor in ((0, 1.0), (q_width, QK ** (-0.5))):
            for head in range(heads):
                part = total[:, start + head * QK : start + (head + 1) * QK]
                turned = (part * cosines + pltpu.roll(part, QK // 2, 1) * sines) * factor
                blocks.append(turned.astype(jnp.bfloat16).astype(jnp.float32))
        columns = jnp.concatenate(blocks * (LANES // (len(blocks) * rows)), axis=0).T
        qk[h] = columns
        for i in range(rows):
            for head in range(heads):
                query = columns[:, head * rows + i : head * rows + i + 1]
                retained[base + i : base + i + 1, head * width : (head + 1) * width] = jnp.sum(
                    query * state[base + i, head], axis=0, keepdims=True
                )
        second[h]()
        total = total_of(out_b[h, kv], in_b.at[h]) * scale
        values = total[:, :v_width].astype(jnp.bfloat16).astype(jnp.float32)
        value[base : base + rows] = values
        pieces = []
        for head in range(heads):
            overlap = jnp.sum(blocks[head] * blocks[heads + head], axis=1, keepdims=True)
            span = slice(head * width, (head + 1) * width)
            piece = decays[head] * retained[base : base + rows, span] + overlap * values[:, span]
            pieces.append(piece * lax.rsqrt(jnp.mean(piece * piece, axis=1, keepdims=True) + 1e-06))
        merged[h, kv] = (jnp.concatenate(pieces, axis=1) * silu(total[:, v_width:])).astype(jnp.bfloat16)
        copies_m.append(kv_send(
            "m", h, peers, lambda p: merged.at[h, kv], lambda n: merged.at[h, kv], merged.at[h, : n_kv - 1]
        ))

    block = 8

    def update(h):
        base = h * rows

        def update_step(i, carry):
            start = i * block
            turned = pltpu.roll(qk[h], lax.rem(LANES - start, LANES), 1)
            for n in range(block):
                for head in range(heads):
                    lane = (heads + head) * rows + n
                    at = base + start + n
                    outer = turned[:, lane : lane + 1] * value[pl.ds(at, 1), head * width : (head + 1) * width]
                    state[at, head] = decays[head] * state[at, head] + outer
            return carry

        lax.fori_loop(0, rows // block, update_step, 0)

    def reduce_start(h, lhs, weight, tag):
        start_reduce(lhs, s[weight], s["parts_" + tag].at[h], s["swapped_" + tag].at[h], tp, *pair_of(tag, h))

    def reduce_spread(h, tag):
        swapped, staged = s["swapped_" + tag].at[h], s["staged_" + tag].at[h]
        send_sems, recv_sems = pair_of(tag, h)
        spread_pairs(s["parts_" + tag].at[h], swapped, staged, s["landed_" + tag].at[h], tp, send_sems, recv_sems)
        closing.extend([(swapped, send_sems.at[0]), (staged, send_sems.at[1])])

    def reduce_total(h, tag):
        into = s["landed_" + tag].at[h]
        landed(into, pair_of(tag, h)[1].at[1])
        return total_of(into[0], into.at[1:])

    gate_out, up_out, gate_in, up_in = s["gate_out"], s["up_out"], s["gate_in"], s["up_in"]
    copies_e, copies_f, copies_h, copies_u = [], [], [], []
    crossed_all = crossed + [beside]

    def project_second(h):
        normed, squares = normalise(gathered_two.at[h], s["gain_two"])
        gate_out[h] = project(normed, s["fg"])
        copies_e.append(
            kv_send("e", h, crossed_all, lambda p: gate_out.at[h, p], lambda n: gate_in.at[h, n], gate_in.at[h])
        )
        copies_u.append(send_squares("squares_two", h, squares))
        up_out[h] = project(normed, s["fu"])
        copies_f.append(
            kv_send("f", h, crossed_all, lambda p: up_out.at[h, p], lambda n: up_in.at[h, n], up_in.at[h])
        )

    def activate(h):
        copies_e[h]()
        total = total_of(gate_in[h, 0], gate_in.at[h, 1:])
        scale = scale_of("squares_two", h, copies_u[h])
        activated = silu(total * scale)
        copies_f[h]()
        up = total_of(up_in[h, 0], up_in.at[h, 1:]) * scale
        s["hidden_out"][h] = (activated * up).astype(jnp.bfloat16)
        copies_h.append(
            kv_send("h", h, crossed_all, lambda p: s["hidden_out"].at[h], lambda n: hidden.at[h, kv], hidden.at[h])
        )

    first_gather[0][0](0, 1)
    for h in range(1, halves):
        first_gather.append(start_gather(gathered.at[h], tp, n_tp, 0, *pair_of("g", h)))
    first_gather[0][0](1, chips - 1)
    for h in range(halves):
        if h > 0:
            first_gather[h][0](0, chips - 1)
        first_gather[h][1]()
        project_first(h)
    ready("state")
    for h in range(halves):
        attend(h)
    ready("wo")
    for h in range(halves):
        copies_m[h]()
        reduce_start(h, merged[h].reshape(batch, v_width), "wo", "x")
        reduce_spread(h, "x")
        update(h)
    second_gather = []
    for h in range(halves):
        total = reduce_total(h, "x")
        own = gathered[h, tp].reshape(batch, LANES).astype(jnp.float32)
        gathered_two[h, tp] = (own + total).astype(jnp.bfloat16).reshape(n_kv, rows, LANES)
        second_gather.append(start_gather(gathered_two.at[h], tp, n_tp, 1, *pair_of("c", h)))
    ready("gain_two", "fg", "fu")
    for h in range(halves):
        second_gather[h][1]()
        second_gather[h][0](0, chips - 1)
        project_second(h)
    for h in range(halves):
        activate(h)
    ready("fd")
    for h in range(halves):
        copies_h[h]()
        reduce_start(h, hidden[h].reshape(batch, units), "fd", "d")
        reduce_spread(h, "d")
    for h in range(halves):
        total = reduce_total(h, "d")
        own = gathered_two[h, tp].reshape(batch, LANES).astype(jnp.float32)
        out[:, h] = (own + total).astype(jnp.bfloat16).reshape(n_kv, rows, LANES)
    for extent, sem in closing:
        landed(extent, sem)
    for gather in first_gather + second_gather:
        gather[2]()


def finish_kernel(state, out, state_to, out_to, store_sems):
    chunks = store_sems.shape[0] - 1
    size = state.shape[0] // chunks
    targets = [(out, out_to)]
    for i in range(chunks):
        part = pl.ds(i * size, size)
        targets.append((state.at[part], state_to.at[part]))
    copies = [
        pltpu.make_async_copy(source, target, store_sems.at[i]) for i, (source, target) in enumerate(targets)
    ]
    for copy in copies:
        copy.start()
    for copy in copies:
        copy.wait()


HALVES = 2


def fused_on_device(n_kv, n_tp, *arrays):
    (
        tokens, lengths, state, mixer_gain, wq, wk, wv, wg, wo, channel_gain, fg, fu, fd,
    ) = arrays
    columns = tokens.shape[1]
    rows = state.shape[0] // HALVES
    batch = n_kv * rows
    depth, q_width = wq.shape
    v_width, units = wv.shape[1], fg.shape[1]
    bf16, f32 = jnp.bfloat16, jnp.float32
    vmem = pl.BlockSpec(memory_space=pltpu.VMEM)
    hbm = pl.BlockSpec(memory_space=pltpu.HBM)
    chips = n_tp // CORES
    index = np.arange(QK) % (QK // 2)
    freq = jnp.asarray((10000.0 ** (-index / (QK // 2))).astype(np.float32))[None, :]
    a_width, b_width = 2 * q_width, 2 * v_width

    def buffer(*shape, dtype=bf16):
        return pltpu.VMEM((HALVES,) + shape, dtype)

    scratch = {
        "lengths": pltpu.VMEM((1, HALVES * rows), jnp.int32),
        "freq": pltpu.VMEM((1, QK), f32),
        "gain": pltpu.VMEM((1, depth), f32),
        "gain_two": pltpu.VMEM((1, depth), f32),
        "gathered": buffer(n_tp, n_kv, rows, columns),
        "gathered_two": buffer(n_tp, n_kv, rows, columns),
        "out_a": buffer(n_kv, rows, a_width),
        "out_b": buffer(n_kv, rows, b_width),
        "in_a": buffer(n_kv - 1, rows, a_width),
        "in_b": buffer(n_kv - 1, rows, b_width),
        "qk": buffer(QK, LANES, dtype=f32),
        "retained": pltpu.VMEM((HALVES * rows, v_width), f32),
        "value": pltpu.VMEM((HALVES * rows, v_width), f32),
        "merged": buffer(n_kv, rows, v_width),
        "gate_out": buffer(n_kv, rows, units),
        "up_out": buffer(n_kv, rows, units),
        "gate_in": buffer(n_kv, rows, units),
        "up_in": buffer(n_kv, rows, units),
        "hidden_out": buffer(rows, units),
        "hidden": buffer(n_kv, rows, units),
        "squares": buffer(n_kv, 1, LANES, dtype=f32),
        "squares_two": buffer(n_kv, 1, LANES, dtype=f32),
    }
    shapes = {
        "wqk": (depth, 2 * q_width), "wvg": (depth, 2 * v_width), "fg": fg.shape, "fu": fu.shape,
        "wo": (CORES, wo.shape[0], chips * columns), "fd": (CORES, fd.shape[0], chips * columns),
    }
    scratch.update({name: pltpu.VMEM(shape, bf16) for name, shape in shapes.items()})
    for tag in ("x", "d"):
        scratch["parts_" + tag] = buffer(CORES, chips, batch, columns)
        scratch["swapped_" + tag] = buffer(chips, batch, columns)
        scratch["staged_" + tag] = buffer(chips, batch, columns)
        scratch["landed_" + tag] = buffer(chips, batch, columns)
    dma = pltpu.SemaphoreType.DMA
    sems = {"load": dma((12,))}
    for tag in ("g", "c"):
        sems[tag + "_s"], sems[tag + "_r"] = dma((HALVES, 2)), dma((HALVES, n_tp))
    for tag in ("x", "d"):
        sems[tag + "_s"] = sems[tag + "_r"] = dma((HALVES, 2))
    for tag in ("a", "b", "m", "e", "f", "h", "squares", "squares_two"):
        sems[tag] = dma((HALVES, 2))
    operands = (
        tokens.reshape(n_kv, HALVES, rows, columns), lengths[None, :], freq, mixer_gain[None, :],
        channel_gain[None, :], state, wq, wk, wv, wg, wo, fg, fu, fd,
    )
    out_shape = (n_kv, HALVES, rows, columns)
    out, new_state = pl.pallas_call(
        functools.partial(layer_kernel, n_kv, n_tp, depth * n_kv),
        out_shape=(pltpu.VMEM(out_shape, bf16), pltpu.VMEM(state.shape, f32)),
        in_specs=[hbm] * 14,
        out_specs=(vmem, vmem),
        scratch_shapes=[scratch, sems],
        compiler_params=pltpu.CompilerParams(
            collective_id=0, has_side_effects=True, vmem_limit_bytes=LAYER_VMEM
        ),
        name="layer",
    )(*[pltpu.with_memory_space_constraint(a, pltpu.HBM) for a in operands])
    new_state, out = pl.pallas_call(
        finish_kernel,
        out_shape=(
            jax.ShapeDtypeStruct(state.shape, f32),
            jax.ShapeDtypeStruct(out_shape, bf16),
        ),
        in_specs=[vmem, vmem],
        out_specs=(hbm, hbm),
        scratch_shapes=[pltpu.SemaphoreType.DMA((9,))],
        compiler_params=pltpu.CompilerParams(vmem_limit_bytes=FINISH_VMEM),
        name="finish",
    )(new_state, out)
    return out.reshape(tokens.shape), new_state


def fits(n_kv, n_tp, arrays):
    tokens, state, ffn_gate = arrays[0], arrays[2], arrays[10]
    rows, heads = state.shape[0], state.shape[1]
    return (
        tokens.shape[1] % LANES == 0
        and n_tp % CORES == 0
        and n_tp > CORES
        and n_kv == SIDE * SIDE
        and 4 * state.size < VMEM_TOTAL // 4
        and ffn_gate.shape[1] % LANES == 0
        and tokens.shape[1] == LANES
        and tokens.shape[0] == n_kv * rows
        and rows % (16 * HALVES) == 0
        and n_kv * rows // HALVES <= LANES
        and 2 * heads * rows == LANES
        and state.shape[2] == QK == LANES
        and state.shape[3] % LANES == 0
    )


def per_device(n_kv, n_tp, *arrays):
    if fits(n_kv, n_tp, arrays):
        return fused_on_device(n_kv, n_tp, *arrays)
    return on_device(*arrays)


def solution(mesh):
    in_specs = (
        P(None, ("kv", "tp")),
        P("kv"),
        P("kv", "tp", None, None),
        P("kv"),
        P("kv", "tp"),
        P("kv", "tp"),
        P("kv", "tp"),
        P("kv", "tp"),
        P("tp", "kv"),
        P("kv"),
        P("kv", "tp"),
        P("kv", "tp"),
        P("tp", "kv"),
    )
    out_specs = (P(None, ("kv", "tp")), P("kv", "tp", None, None))
    return jax.shard_map(
        functools.partial(per_device, mesh.shape["kv"], mesh.shape["tp"]),
        mesh=mesh, in_specs=in_specs, out_specs=out_specs, check_vma=False
    )
```

```python
import functools

import jax
import jax.numpy as jnp
import numpy as np
from jax import lax
from jax.experimental import pallas as pl
from jax.experimental.pallas import tpu as pltpu
from jax.sharding import PartitionSpec as P

D = 4096
HEADS = 16
QK = 128
LANES = 128


def rotate_heads(vectors, positions):
    half_dim = vectors.shape[-1] // 2
    frequency = 10000.0 ** (-jnp.arange(half_dim, dtype=jnp.float32) / half_dim)
    angles = positions.astype(jnp.float32)[:, None, None] * frequency
    cosine = jnp.cos(angles)
    sine_part = jnp.sin(angles)
    first_half = vectors[..., :half_dim]
    second = vectors[..., half_dim:]
    return jnp.concatenate(
        [first_half * cosine - second * sine_part, first_half * sine_part + second * cosine],
        axis=-1,
    )


def gathered_rows(columns):
    return lax.all_gather(columns, "tp", axis=1, tiled=True)


def owned_sums(partial_value, squares):
    raw_sums, totals = (
        lax.psum_scatter(
            partial_value.astype(jnp.bfloat16), "kv", scatter_dimension=0, tiled=True
        ).astype(jnp.float32),
        lax.psum_scatter(
            squares.astype(jnp.bfloat16), "kv", scatter_dimension=0, tiled=True
        ).astype(jnp.float32),
    )
    summed = raw_sums * lax.rsqrt(totals / D + 1e-06)[:, None]
    return summed


def every_sum(partial_value, squares):
    raw_sums, totals = (
        lax.psum(partial_value.astype(jnp.bfloat16), "kv").astype(jnp.float32),
        lax.psum(squares.astype(jnp.bfloat16), "kv").astype(jnp.float32),
    )
    summed = raw_sums * lax.rsqrt(totals / D + 1e-06)[:, None]
    return summed


def on_device(
    tokens,
    lengths,
    retention_state,
    mixer_gain,
    query_weight,
    key_weight,
    value_weight,
    gate_weight,
    output_weight,
    channel_gain,
    ffn_gate,
    ffn_up,
    ffn_down,
):
    feature_block = gathered_rows(tokens).astype(jnp.float32)
    squares = jnp.sum(feature_block * feature_block, axis=1)
    normed = (feature_block * mixer_gain).astype(jnp.bfloat16)
    partial_value = jnp.concatenate(
        [
            jnp.dot(normed, query_weight, preferred_element_type=jnp.float32),
            jnp.dot(normed, key_weight, preferred_element_type=jnp.float32),
            jnp.dot(normed, value_weight, preferred_element_type=jnp.float32),
            jnp.dot(normed, gate_weight, preferred_element_type=jnp.float32),
        ],
        axis=1,
    )
    owned_rows = owned_sums(partial_value, squares)
    local_heads = query_weight.shape[1] // QK
    q_width = query_weight.shape[1]
    v_width = value_weight.shape[1]
    head_width = v_width // local_heads
    seq_rows = owned_rows.shape[0]
    query_rows = rotate_heads(
        owned_rows[:, :q_width].reshape(seq_rows, local_heads, QK), lengths
    ).astype(jnp.bfloat16)
    key_rows = (
        rotate_heads(
            owned_rows[:, q_width : 2 * q_width].reshape(seq_rows, local_heads, QK), lengths
        )
        * QK ** (-0.5)
    ).astype(jnp.bfloat16)
    value_rows = (
        owned_rows[:, 2 * q_width : 2 * q_width + v_width]
        .astype(jnp.bfloat16)
        .reshape(seq_rows, local_heads, head_width)
    )
    gate_rows = owned_rows[:, 2 * q_width + v_width :]
    head_ids = (lax.axis_index("tp") * local_heads + jnp.arange(local_heads)).astype(jnp.float32)
    decay_rate = 1.0 - 2.0 ** (-5.0 - 10.0 * head_ids / (HEADS - 1))
    new_state = (
        decay_rate[None, :, None, None] * retention_state
        + key_rows.astype(jnp.float32)[..., :, None] * value_rows.astype(jnp.float32)[..., None, :]
    )
    retained = jnp.einsum(
        "bhk,bhkv->bhv", query_rows.astype(jnp.float32), new_state, precision=lax.Precision.HIGHEST
    )
    normalized = retained * lax.rsqrt(jnp.mean(retained * retained, axis=-1) + 1e-06)[..., None]
    merged = (normalized.reshape(seq_rows, v_width) * jax.nn.silu(gate_rows)).astype(jnp.bfloat16)
    mixed_part = jnp.dot(
        lax.all_gather(merged, "kv", axis=0, tiled=True),
        output_weight,
        preferred_element_type=jnp.float32,
    )
    mixed_cols = lax.psum_scatter(
        mixed_part.astype(jnp.bfloat16), "tp", scatter_dimension=1, tiled=True
    ).astype(jnp.float32)
    residual = (tokens.astype(jnp.float32) + mixed_cols).astype(jnp.bfloat16)
    block_two = gathered_rows(residual).astype(jnp.float32)
    squares_two = jnp.sum(block_two * block_two, axis=1)
    normed_two = (block_two * channel_gain).astype(jnp.bfloat16)
    partial_two = jnp.concatenate(
        [
            jnp.dot(normed_two, ffn_gate, preferred_element_type=jnp.float32),
            jnp.dot(normed_two, ffn_up, preferred_element_type=jnp.float32),
        ],
        axis=1,
    )
    hidden_units = ffn_gate.shape[1]
    summed = every_sum(partial_two, squares_two)
    hidden = (jax.nn.silu(summed[:, :hidden_units]) * summed[:, hidden_units:]).astype(jnp.bfloat16)
    down_part = jnp.dot(hidden, ffn_down, preferred_element_type=jnp.float32)
    down_sums = lax.psum_scatter(
        down_part.astype(jnp.bfloat16), "tp", scatter_dimension=1, tiled=True
    ).astype(jnp.float32)
    layer_output = (residual.astype(jnp.float32) + down_sums).astype(jnp.bfloat16)
    return (layer_output, new_state)


MESH_ID = pl.DeviceIdType.MESH
VMEM_TOTAL = 67043328
CORES = 2
SIDE = 2
LAYER_VMEM = 50000000
FINISH_VMEM = 20000000


def greet(devices):
    barrier = pltpu.get_barrier_semaphore()
    for device in devices:
        pl.semaphore_signal(barrier, inc=1, device_id=device, device_id_type=MESH_ID)
    pl.semaphore_wait(barrier, len(devices))


def kv_peers(kv, n_kv):
    return [n_kv - 1 - kv, kv + 1 - 2 * lax.rem(kv, SIDE), lax.rem(kv + SIDE, n_kv)]


def send_all(devices, source, target, send_sem, recv_sem):
    for k, device in enumerate(devices):
        remote_to(device, source(device["kv"]), target(k), send_sem, recv_sem).start()


def landed(ref, sem):
    pltpu.make_async_copy(ref, ref, sem).wait()


def load_all(pairs, sem):
    for source, target in pairs:
        pltpu.make_async_copy(source, target, sem).start()


def silu(value):
    return value / (1.0 + jnp.exp(-value))


def as_row(column):
    lane = lax.broadcasted_iota(jnp.int32, (column.shape[0], LANES), 1)
    row = lax.broadcasted_iota(jnp.int32, (column.shape[0], LANES), 0)
    return jnp.sum(jnp.where(row == lane, column, 0.0), axis=0, keepdims=True)


def as_column(row_values, first, rows):
    lane = lax.broadcasted_iota(jnp.int32, (rows, LANES), 1)
    row = lax.broadcasted_iota(jnp.int32, (rows, LANES), 0)
    return jnp.sum(jnp.where(row + first == lane, row_values, 0.0), axis=1, keepdims=True)


def remote(axis, peer, source, target, send_sem, recv_sem):
    return remote_to({axis: peer}, source, target, send_sem, recv_sem)


def remote_to(device, source, target, send_sem, recv_sem):
    return pltpu.make_async_remote_copy(
        src_ref=source, dst_ref=target, send_sem=send_sem, recv_sem=recv_sem,
        device_id=device, device_id_type=MESH_ID,
    )


def far_first(chip, chips):
    def ascending(at, k):
        return k + 1 - (at + chips - 1 - k) // chips

    low = 1 - chip // (chips // 2)
    mirrored = chips - 1 - chip
    return [
        low * (chips - 1 - ascending(mirrored, k)) + (1 - low) * ascending(chip, k)
        for k in range(chips - 1)
    ]


def start_gather(slots, tp, n_tp, hub, send_sems, recv_sems):
    chips = n_tp // CORES
    chip, core = tp // CORES, lax.rem(tp, CORES)
    partner = chip * CORES + 1 - core
    order = far_first(chip, chips)

    def block(peer, slot, send):
        return remote("tp", peer, slots.at[slot], slots.at[slot], send_sems.at[send], recv_sems.at[slot])

    for peer in order:
        block(peer * CORES + hub, tp, 0).start()
    block(partner, tp, 0).start()
    relayed = [
        block(partner, source * CORES + side, 1) for source in order[::-1] for side in range(CORES)
    ]

    def take(first, last):
        for copy in relayed[first * CORES : last * CORES]:
            copy.wait_recv()

            @pl.when(core == hub)
            def _():
                copy.start()

    def take_own():
        block(partner, partner, 0).wait_recv()

    def close():
        landed(slots.at[:chips], send_sems.at[0])

        @pl.when(core == hub)
        def _():
            landed(slots.at[: len(relayed)], send_sems.at[1])

    return take, take_own, close


def start_reduce(lhs, weight, parts, swapped, tp, send_sems, recv_sems):
    chip, core = tp // CORES, lax.rem(tp, CORES)
    chips, columns = parts.shape[1], parts.shape[3]

    def multiply(side):
        full = jnp.dot(lhs, weight[side], preferred_element_type=jnp.float32).astype(jnp.bfloat16)
        for z in range(chips):
            parts[side, z] = full[:, z * columns : (z + 1) * columns]

    multiply(core)
    remote(
        "tp", chip * CORES + 1 - core, parts.at[core], swapped, send_sems.at[0], recv_sems.at[0]
    ).start()
    multiply(1 - core)


def spread_pairs(parts, swapped, staged, into, tp, send_sems, recv_sems):
    chips = parts.shape[1]
    chip, core = tp // CORES, lax.rem(tp, CORES)
    landed(swapped, recv_sems.at[0])
    for k, other in enumerate(far_first(chip, chips) + [chip]):
        pair = parts[1 - core, other].astype(jnp.float32) + swapped[other].astype(jnp.float32)
        staged[k] = pair.astype(jnp.bfloat16)
        remote(
            "tp", other * CORES + 1 - core, staged.at[k], into.at[chip], send_sems.at[1], recv_sems.at[1]
        ).start()


def total_of(own, others):
    total = own.astype(jnp.float32)
    for step in range(others.shape[0]):
        total += others[step].astype(jnp.float32)
    return total


def layer_kernel(
    n_kv, n_tp, features,
    tokens_hbm, lengths_hbm, freq_hbm, gain_hbm, gain_two_hbm, state_hbm,
    wq_hbm, wk_hbm, wv_hbm, wg_hbm, wo_hbm, fg_hbm, fu_hbm, fd_hbm,
    out, state, s, sems,
):
    kv, tp = lax.axis_index("kv"), lax.axis_index("tp")
    chips = n_tp // CORES
    chip, core = tp // CORES, lax.rem(tp, CORES)
    gathered, gathered_two, merged, hidden = s["gathered"], s["gathered_two"], s["merged"], s["hidden"]
    halves, rows = gathered.shape[0], gathered.shape[3]
    batch = n_kv * rows
    q_width, v_width = wq_hbm.shape[1], wv_hbm.shape[1]
    units, columns = fg_hbm.shape[1], tokens_hbm.shape[3]

    def sides(ref, target):
        return [
            (
                ref.at[:, (z * CORES + side) * columns : (z * CORES + side + 1) * columns],
                target.at[side, :, z * columns : (z + 1) * columns],
            )
            for side in range(CORES)
            for z in range(chips)
        ]

    groups = {
        "tokens": [(tokens_hbm.at[:, h], gathered.at[h, tp]) for h in range(halves)],
        "lengths": [(lengths_hbm, s["lengths"])],
        "freq": [(freq_hbm, s["freq"])],
        "gain": [(gain_hbm, s["gain"])],
        "wqk": [(wq_hbm, s["wqk"].at[:, :q_width]), (wk_hbm, s["wqk"].at[:, q_width:])],
        "wvg": [(wv_hbm, s["wvg"].at[:, :v_width]), (wg_hbm, s["wvg"].at[:, v_width:])],
        "state": [(state_hbm, state)],
        "wo": sides(wo_hbm, s["wo"]),
        "gain_two": [(gain_two_hbm, s["gain_two"])],
        "fg": [(fg_hbm, s["fg"])],
        "fu": [(fu_hbm, s["fu"])],
        "fd": sides(fd_hbm, s["fd"]),
    }
    wholes = {
        "tokens": gathered.at[:, tp], "wqk": s["wqk"], "wvg": s["wvg"], "state": state, "wo": s["wo"], "fd": s["fd"],
        "lengths": s["lengths"], "freq": s["freq"], "gain": s["gain"],
        "gain_two": s["gain_two"], "fg": s["fg"], "fu": s["fu"],
    }
    pending = {}
    for i, (name, group) in enumerate(groups.items()):
        pending[name] = i
        load_all(group, sems["load"].at[i])

    def ready(*wanted):
        for name in wanted:
            if name in pending:
                landed(wholes[name], sems["load"].at[pending.pop(name)])

    partner = chip * CORES + 1 - core
    peers = [{"kv": peer, "tp": tp} for peer in kv_peers(kv, n_kv)]
    crossed = [{"kv": peer, "tp": partner} for peer in kv_peers(kv, n_kv)]
    along = [{"kv": kv, "tp": other * CORES + 1 - core} for other in far_first(chip, chips)]
    beside = {"kv": kv, "tp": partner}
    aside = [{"kv": kv, "tp": other * CORES + core} for other in far_first(chip, chips)]
    greet(along + aside + [beside] + peers + crossed)
    closing = []

    def close_sends():
        for extent, sem in closing:
            landed(extent, sem)
        closing.clear()

    def pair_of(name, h):
        return sems[name + "_s"].at[h], sems[name + "_r"].at[h]

    def kv_send(name, h, devices, source, target, extent):
        send_sem, recv_sem = sems[SHARED.get(name, name)].at[h, 0], sems[SHARED.get(name, name)].at[h, 1]
        send_all(devices, source, target, send_sem, recv_sem)
        closing.append((extent, send_sem))
        return lambda: landed(extent, recv_sem)

    def send_squares(name, h, devices):
        return kv_send(
            name, h, devices, lambda p: s[name].at[h, n_kv - 1], lambda n: s[name].at[h, n], s[name].at[h, : n_kv - 1]
        )

    def scale_of(name, h, wait):
        wait()
        total = s[name][h, 0]
        for n in range(1, n_kv):
            total += s[name][h, n]
        return lax.rsqrt(as_column(total, kv * rows, rows) / features + 1e-06)

    ready("tokens")
    first_gather = [start_gather(gathered.at[0], tp, n_tp, 0, *pair_of("g", 0))]
    ready("lengths", "freq", "gain")
    all_rows = halves * rows
    row = lax.broadcasted_iota(jnp.int32, (all_rows, all_rows), 0)
    col = lax.broadcasted_iota(jnp.int32, (all_rows, all_rows), 1)
    spread = jnp.where(row == col, s["lengths"][...].astype(jnp.float32), 0.0)
    angles = jnp.sum(spread, axis=1, keepdims=True) * s["freq"][...]
    cosine, sine = jnp.cos(angles), jnp.sin(angles)
    lane = lax.broadcasted_iota(jnp.int32, angles.shape, 1)
    sine = jnp.where(lane < QK // 2, -sine, sine)

    def normalise(slots, gains):
        x = jnp.concatenate(
            [slots[j].reshape(batch, slots.shape[3]) for j in range(slots.shape[0])], axis=1
        ).astype(jnp.float32)
        squares = jnp.sum(x * x, axis=1, keepdims=True)
        return (x * gains[...]).astype(jnp.bfloat16), as_row(squares)

    def project(lhs, weight):
        full = jnp.dot(lhs, weight[...], preferred_element_type=jnp.float32)
        return full.astype(jnp.bfloat16).reshape(n_kv, rows, full.shape[1])

    heads = q_width // QK
    width = v_width // heads
    out_a, out_b, in_a, in_b = s["out_a"], s["out_b"], s["in_a"], s["in_b"]
    first, second, copies_m, copies_q = [], [], [], []

    def project_first(h):
        normed, s["squares"][h, n_kv - 1] = normalise(gathered.at[h], s["gain"])
        ready("wqk")
        out_a[h] = project(normed, s["wqk"])
        copies_q.append(send_squares("squares", h, peers))
        first.append(kv_send("a", h, peers, lambda p: out_a.at[h, p], lambda n: in_a.at[h, n], in_a.at[h]))
        ready("wvg")
        out_b[h] = project(normed, s["wvg"])
        second.append(kv_send("b", h, peers, lambda p: out_b.at[h, p], lambda n: in_b.at[h, n], in_b.at[h]))

    decays = []
    for head in range(heads):
        number = jnp.full((1, width), tp * heads + head, jnp.int32).astype(jnp.float32)
        decays.append(1.0 - jnp.exp2(-5.0 - 10.0 * number / (heads * n_tp - 1)))
    qk, value, retained = s["qk"], s["value"], s["retained"]

    def attend(h):
        base = h * rows
        first[h]()
        total = total_of(out_a[h, kv], in_a.at[h])
        scale = scale_of("squares", h, copies_q[h])
        total = total * scale
        cosines, sines = cosine[base : base + rows], sine[base : base + rows]
        blocks = []
        for start, factor in ((0, 1.0), (q_width, QK ** (-0.5))):
            for head in range(heads):
                part = total[:, start + head * QK : start + (head + 1) * QK]
                turned = (part * cosines + pltpu.roll(part, QK // 2, 1) * sines) * factor
                blocks.append(turned.astype(jnp.bfloat16).astype(jnp.float32))
        columns = jnp.concatenate(blocks * (LANES // (len(blocks) * rows)), axis=0).T
        qk[h] = columns
        for i in range(rows):
            for head in range(heads):
                query = columns[:, head * rows + i : head * rows + i + 1]
                retained[base + i : base + i + 1, head * width : (head + 1) * width] = jnp.sum(
                    query * state[base + i, head], axis=0, keepdims=True
                )
        second[h]()
        total = total_of(out_b[h, kv], in_b.at[h]) * scale
        values = total[:, :v_width].astype(jnp.bfloat16).astype(jnp.float32)
        value[base : base + rows] = values
        pieces = []
        for head in range(heads):
            overlap = jnp.sum(blocks[head] * blocks[heads + head], axis=1, keepdims=True)
            span = slice(head * width, (head + 1) * width)
            piece = decays[head] * retained[base : base + rows, span] + overlap * values[:, span]
            pieces.append(piece * lax.rsqrt(jnp.mean(piece * piece, axis=1, keepdims=True) + 1e-06))
        merged[h, kv] = (jnp.concatenate(pieces, axis=1) * silu(total[:, v_width:])).astype(jnp.bfloat16)
        copies_m.append(kv_send(
            "m", h, peers, lambda p: merged.at[h, kv], lambda n: merged.at[h, kv], merged.at[h, : n_kv - 1]
        ))

    block = 8

    def update(h):
        base = h * rows

        def update_step(i, carry):
            start = i * block
            turned = pltpu.roll(qk[h], lax.rem(LANES - start, LANES), 1)
            for n in range(block):
                for head in range(heads):
                    lane = (heads + head) * rows + n
                    at = base + start + n
                    outer = turned[:, lane : lane + 1] * value[pl.ds(at, 1), head * width : (head + 1) * width]
                    state[at, head] = decays[head] * state[at, head] + outer
            return carry

        lax.fori_loop(0, rows // block, update_step, 0)

    def reduce_start(h, lhs, weight, tag):
        start_reduce(lhs, s[weight], s["parts_" + tag].at[h], s["swapped_" + tag].at[h], tp, *pair_of("x", h))

    def reduce_spread(h, tag):
        swapped, staged = s["swapped_" + tag].at[h], s["staged_" + tag].at[h]
        send_sems, recv_sems = pair_of("x", h)
        spread_pairs(s["parts_" + tag].at[h], swapped, staged, s["landed_" + tag].at[h], tp, send_sems, recv_sems)
        closing.extend([(swapped, send_sems.at[0]), (staged, send_sems.at[1])])

    def reduce_total(h, tag):
        into = s["landed_" + tag].at[h]
        landed(into, pair_of("x", h)[1].at[1])
        return total_of(into[0], into.at[1:])

    gate_out, up_out, gate_in, up_in = s["gate_out"], s["up_out"], s["gate_in"], s["up_in"]
    copies_e, copies_f, copies_h, copies_u = [], [], [], []
    crossed_all = crossed + [beside]
    first_units = (units // LANES + 1) // 2 * LANES

    def project_second(h):
        normed, s["squares_two"][h, n_kv - 1] = normalise(gathered_two.at[h], s["gain_two"])
        for span in (slice(0, first_units), slice(first_units, units)):
            gate_out[h, :, :, span] = project(normed, s["fg"].at[:, span])
            if span.start == 0:
                copies_u.append(send_squares("squares_two", h, crossed))
            send_all(
                crossed_all, lambda p: gate_out.at[h, p, :, span], lambda n: gate_in.at[h, n, :, span],
                sems["a"].at[h, 0], sems["a"].at[h, 1],
            )
        closing.append((gate_in.at[h], sems["a"].at[h, 0]))
        copies_e.append(lambda: landed(gate_in.at[h], sems["a"].at[h, 1]))
        up_out[h] = project(normed, s["fu"])
        copies_f.append(
            kv_send("f", h, crossed_all, lambda p: up_out.at[h, p], lambda n: up_in.at[h, n], up_in.at[h])
        )

    def activate(h):
        copies_e[h]()
        total = total_of(gate_in[h, 0], gate_in.at[h, 1:])
        scale = scale_of("squares_two", h, copies_u[h])
        activated = silu(total * scale)
        copies_f[h]()
        up = total_of(up_in[h, 0], up_in.at[h, 1:]) * scale
        s["hidden_out"][h] = (activated * up).astype(jnp.bfloat16)
        copies_h.append(
            kv_send("h", h, crossed_all, lambda p: s["hidden_out"].at[h], lambda n: hidden.at[h, kv], hidden.at[h])
        )

    first_gather[0][0](0, 1)
    for h in range(1, halves):
        first_gather.append(start_gather(gathered.at[h], tp, n_tp, 0, *pair_of("g", h)))
    first_gather[0][0](1, chips - 1)
    for h in range(halves):
        if h > 0:
            first_gather[h][0](0, chips - 1)
        first_gather[h][1]()
        project_first(h)
    ready("state")
    for h in range(halves):
        attend(h)
    ready("wo")
    for h in range(halves):
        copies_m[h]()
        reduce_start(h, merged[h].reshape(batch, v_width), "wo", "x")
        reduce_spread(h, "x")
        if h + 1 < halves:
            update(h)
    for gather in first_gather:
        gather[2]()
    second_gather = []
    for h in range(halves):
        total = reduce_total(h, "x")
        own = gathered[h, tp].reshape(batch, LANES).astype(jnp.float32)
        gathered_two[h, tp] = (own + total).astype(jnp.bfloat16).reshape(n_kv, rows, LANES)
        second_gather.append(start_gather(gathered_two.at[h], tp, n_tp, 1, *pair_of("g", h)))
        if h == 0:
            update(halves - 1)
    ready("gain_two", "fg", "fu")
    close_sends()
    for h in range(halves):
        second_gather[h][1]()
        second_gather[h][0](0, chips - 1)
        project_second(h)
    for h in range(halves):
        activate(h)
    ready("fd")
    for h in range(halves):
        copies_h[h]()
        reduce_start(h, hidden[h].reshape(batch, units), "fd", "d")
        reduce_spread(h, "d")
    for h in range(halves):
        total = reduce_total(h, "d")
        own = gathered_two[h, tp].reshape(batch, LANES).astype(jnp.float32)
        out[:, h] = (own + total).astype(jnp.bfloat16).reshape(n_kv, rows, LANES)
    close_sends()
    for gather in second_gather:
        gather[2]()


def finish_kernel(state, out, state_to, out_to, store_sems):
    chunks = store_sems.shape[0] - 1
    size = state.shape[0] // chunks
    targets = [(out, out_to)]
    for i in range(chunks):
        part = pl.ds(i * size, size)
        targets.append((state.at[part], state_to.at[part]))
    copies = [
        pltpu.make_async_copy(source, target, store_sems.at[i]) for i, (source, target) in enumerate(targets)
    ]
    for copy in copies:
        copy.start()
    for copy in copies:
        copy.wait()


HALVES = 2
SHARED = {"f": "b", "h": "m", "squares_two": "squares"}


def fused_on_device(n_kv, n_tp, *arrays):
    (
        tokens, lengths, state, mixer_gain, wq, wk, wv, wg, wo, channel_gain, fg, fu, fd,
    ) = arrays
    columns = tokens.shape[1]
    rows = state.shape[0] // HALVES
    batch = n_kv * rows
    depth, q_width = wq.shape
    v_width, units = wv.shape[1], fg.shape[1]
    bf16, f32 = jnp.bfloat16, jnp.float32
    vmem = pl.BlockSpec(memory_space=pltpu.VMEM)
    hbm = pl.BlockSpec(memory_space=pltpu.HBM)
    chips = n_tp // CORES
    index = np.arange(QK) % (QK // 2)
    freq = jnp.asarray((10000.0 ** (-index / (QK // 2))).astype(np.float32))[None, :]
    a_width, b_width = 2 * q_width, 2 * v_width

    def buffer(*shape, dtype=bf16):
        return pltpu.VMEM((HALVES,) + shape, dtype)

    scratch = {
        "lengths": pltpu.VMEM((1, HALVES * rows), jnp.int32),
        "freq": pltpu.VMEM((1, QK), f32),
        "gain": pltpu.VMEM((1, depth), f32),
        "gain_two": pltpu.VMEM((1, depth), f32),
        "gathered": buffer(n_tp, n_kv, rows, columns),
        "gathered_two": buffer(n_tp, n_kv, rows, columns),
        "out_a": buffer(n_kv, rows, a_width),
        "out_b": buffer(n_kv, rows, b_width),
        "in_a": buffer(n_kv - 1, rows, a_width),
        "in_b": buffer(n_kv - 1, rows, b_width),
        "qk": buffer(QK, LANES, dtype=f32),
        "retained": pltpu.VMEM((HALVES * rows, v_width), f32),
        "value": pltpu.VMEM((HALVES * rows, v_width), f32),
        "merged": buffer(n_kv, rows, v_width),
        "gate_out": buffer(n_kv, rows, units),
        "up_out": buffer(n_kv, rows, units),
        "gate_in": buffer(n_kv, rows, units),
        "up_in": buffer(n_kv, rows, units),
        "hidden_out": buffer(rows, units),
        "hidden": buffer(n_kv, rows, units),
        "squares": buffer(n_kv, 1, LANES, dtype=f32),
        "squares_two": buffer(n_kv, 1, LANES, dtype=f32),
    }
    shapes = {
        "wqk": (depth, 2 * q_width), "wvg": (depth, 2 * v_width), "fg": fg.shape, "fu": fu.shape,
        "wo": (CORES, wo.shape[0], chips * columns), "fd": (CORES, fd.shape[0], chips * columns),
    }
    scratch.update({name: pltpu.VMEM(shape, bf16) for name, shape in shapes.items()})
    for tag in ("x", "d"):
        scratch["parts_" + tag] = buffer(CORES, chips, batch, columns)
        scratch["swapped_" + tag] = buffer(chips, batch, columns)
        scratch["staged_" + tag] = buffer(chips, batch, columns)
        scratch["landed_" + tag] = buffer(chips, batch, columns)
    dma = pltpu.SemaphoreType.DMA
    sems = {"load": dma((12,))}
    sems["g_s"], sems["g_r"] = dma((HALVES, 2)), dma((HALVES, n_tp))
    for tag in ("x_s", "x_r", "a", "b", "m", "squares"):
        sems[tag] = dma((HALVES, 2))
    operands = (
        tokens.reshape(n_kv, HALVES, rows, columns), lengths[None, :], freq, mixer_gain[None, :],
        channel_gain[None, :], state, wq, wk, wv, wg, wo, fg, fu, fd,
    )
    out_shape = (n_kv, HALVES, rows, columns)
    out, new_state = pl.pallas_call(
        functools.partial(layer_kernel, n_kv, n_tp, depth * n_kv),
        out_shape=(pltpu.VMEM(out_shape, bf16), pltpu.VMEM(state.shape, f32)),
        in_specs=[hbm] * 14,
        out_specs=(vmem, vmem),
        scratch_shapes=[scratch, sems],
        compiler_params=pltpu.CompilerParams(
            collective_id=0, has_side_effects=True, vmem_limit_bytes=LAYER_VMEM
        ),
        name="layer",
    )(*[pltpu.with_memory_space_constraint(a, pltpu.HBM) for a in operands])
    new_state, out = pl.pallas_call(
        finish_kernel,
        out_shape=(
            jax.ShapeDtypeStruct(state.shape, f32),
            jax.ShapeDtypeStruct(out_shape, bf16),
        ),
        in_specs=[vmem, vmem],
        out_specs=(hbm, hbm),
        scratch_shapes=[pltpu.SemaphoreType.DMA((9,))],
        compiler_params=pltpu.CompilerParams(vmem_limit_bytes=FINISH_VMEM),
        name="finish",
    )(new_state, out)
    return out.reshape(tokens.shape), new_state


def fits(n_kv, n_tp, arrays):
    tokens, state, ffn_gate = arrays[0], arrays[2], arrays[10]
    rows, heads = state.shape[0], state.shape[1]
    return (
        tokens.shape[1] % LANES == 0
        and n_tp % CORES == 0
        and n_tp > CORES
        and n_kv == SIDE * SIDE
        and 4 * state.size < VMEM_TOTAL // 4
        and ffn_gate.shape[1] % LANES == 0
        and tokens.shape[1] == LANES
        and tokens.shape[0] == n_kv * rows
        and rows % (16 * HALVES) == 0
        and n_kv * rows // HALVES <= LANES
        and 2 * heads * rows == LANES
        and state.shape[2] == QK == LANES
        and state.shape[3] % LANES == 0
    )


def per_device(n_kv, n_tp, *arrays):
    if fits(n_kv, n_tp, arrays):
        return fused_on_device(n_kv, n_tp, *arrays)
    return on_device(*arrays)


def solution(mesh):
    in_specs = (
        P(None, ("kv", "tp")),
        P("kv"),
        P("kv", "tp", None, None),
        P("kv"),
        P("kv", "tp"),
        P("kv", "tp"),
        P("kv", "tp"),
        P("kv", "tp"),
        P("tp", "kv"),
        P("kv"),
        P("kv", "tp"),
        P("kv", "tp"),
        P("tp", "kv"),
    )
    out_specs = (P(None, ("kv", "tp")), P("kv", "tp", None, None))
    return jax.shard_map(
        functools.partial(per_device, mesh.shape["kv"], mesh.shape["tp"]),
        mesh=mesh, in_specs=in_specs, out_specs=out_specs, check_vma=False
    )
```

```python
import functools

import jax
import jax.numpy as jnp
import numpy as np
from jax import lax
from jax.experimental import pallas as pl
from jax.experimental.pallas import tpu as pltpu
from jax.sharding import PartitionSpec as P

D = 4096
HEADS = 16
QK = 128
LANES = 128


def rotate_heads(vectors, positions):
    half_dim = vectors.shape[-1] // 2
    frequency = 10000.0 ** (-jnp.arange(half_dim, dtype=jnp.float32) / half_dim)
    angles = positions.astype(jnp.float32)[:, None, None] * frequency
    cosine = jnp.cos(angles)
    sine_part = jnp.sin(angles)
    first_half = vectors[..., :half_dim]
    second = vectors[..., half_dim:]
    return jnp.concatenate(
        [first_half * cosine - second * sine_part, first_half * sine_part + second * cosine],
        axis=-1,
    )


def gathered_rows(columns):
    return lax.all_gather(columns, "tp", axis=1, tiled=True)


def owned_sums(partial_value, squares):
    raw_sums, totals = (
        lax.psum_scatter(
            partial_value.astype(jnp.bfloat16), "kv", scatter_dimension=0, tiled=True
        ).astype(jnp.float32),
        lax.psum_scatter(
            squares.astype(jnp.bfloat16), "kv", scatter_dimension=0, tiled=True
        ).astype(jnp.float32),
    )
    summed = raw_sums * lax.rsqrt(totals / D + 1e-06)[:, None]
    return summed


def every_sum(partial_value, squares):
    raw_sums, totals = (
        lax.psum(partial_value.astype(jnp.bfloat16), "kv").astype(jnp.float32),
        lax.psum(squares.astype(jnp.bfloat16), "kv").astype(jnp.float32),
    )
    summed = raw_sums * lax.rsqrt(totals / D + 1e-06)[:, None]
    return summed


def on_device(
    tokens,
    lengths,
    retention_state,
    mixer_gain,
    query_weight,
    key_weight,
    value_weight,
    gate_weight,
    output_weight,
    channel_gain,
    ffn_gate,
    ffn_up,
    ffn_down,
):
    feature_block = gathered_rows(tokens).astype(jnp.float32)
    squares = jnp.sum(feature_block * feature_block, axis=1)
    normed = (feature_block * mixer_gain).astype(jnp.bfloat16)
    partial_value = jnp.concatenate(
        [
            jnp.dot(normed, query_weight, preferred_element_type=jnp.float32),
            jnp.dot(normed, key_weight, preferred_element_type=jnp.float32),
            jnp.dot(normed, value_weight, preferred_element_type=jnp.float32),
            jnp.dot(normed, gate_weight, preferred_element_type=jnp.float32),
        ],
        axis=1,
    )
    owned_rows = owned_sums(partial_value, squares)
    local_heads = query_weight.shape[1] // QK
    q_width = query_weight.shape[1]
    v_width = value_weight.shape[1]
    head_width = v_width // local_heads
    seq_rows = owned_rows.shape[0]
    query_rows = rotate_heads(
        owned_rows[:, :q_width].reshape(seq_rows, local_heads, QK), lengths
    ).astype(jnp.bfloat16)
    key_rows = (
        rotate_heads(
            owned_rows[:, q_width : 2 * q_width].reshape(seq_rows, local_heads, QK), lengths
        )
        * QK ** (-0.5)
    ).astype(jnp.bfloat16)
    value_rows = (
        owned_rows[:, 2 * q_width : 2 * q_width + v_width]
        .astype(jnp.bfloat16)
        .reshape(seq_rows, local_heads, head_width)
    )
    gate_rows = owned_rows[:, 2 * q_width + v_width :]
    head_ids = (lax.axis_index("tp") * local_heads + jnp.arange(local_heads)).astype(jnp.float32)
    decay_rate = 1.0 - 2.0 ** (-5.0 - 10.0 * head_ids / (HEADS - 1))
    new_state = (
        decay_rate[None, :, None, None] * retention_state
        + key_rows.astype(jnp.float32)[..., :, None] * value_rows.astype(jnp.float32)[..., None, :]
    )
    retained = jnp.einsum(
        "bhk,bhkv->bhv", query_rows.astype(jnp.float32), new_state, precision=lax.Precision.HIGHEST
    )
    normalized = retained * lax.rsqrt(jnp.mean(retained * retained, axis=-1) + 1e-06)[..., None]
    merged = (normalized.reshape(seq_rows, v_width) * jax.nn.silu(gate_rows)).astype(jnp.bfloat16)
    mixed_part = jnp.dot(
        lax.all_gather(merged, "kv", axis=0, tiled=True),
        output_weight,
        preferred_element_type=jnp.float32,
    )
    mixed_cols = lax.psum_scatter(
        mixed_part.astype(jnp.bfloat16), "tp", scatter_dimension=1, tiled=True
    ).astype(jnp.float32)
    residual = (tokens.astype(jnp.float32) + mixed_cols).astype(jnp.bfloat16)
    block_two = gathered_rows(residual).astype(jnp.float32)
    squares_two = jnp.sum(block_two * block_two, axis=1)
    normed_two = (block_two * channel_gain).astype(jnp.bfloat16)
    partial_two = jnp.concatenate(
        [
            jnp.dot(normed_two, ffn_gate, preferred_element_type=jnp.float32),
            jnp.dot(normed_two, ffn_up, preferred_element_type=jnp.float32),
        ],
        axis=1,
    )
    hidden_units = ffn_gate.shape[1]
    summed = every_sum(partial_two, squares_two)
    hidden = (jax.nn.silu(summed[:, :hidden_units]) * summed[:, hidden_units:]).astype(jnp.bfloat16)
    down_part = jnp.dot(hidden, ffn_down, preferred_element_type=jnp.float32)
    down_sums = lax.psum_scatter(
        down_part.astype(jnp.bfloat16), "tp", scatter_dimension=1, tiled=True
    ).astype(jnp.float32)
    layer_output = (residual.astype(jnp.float32) + down_sums).astype(jnp.bfloat16)
    return (layer_output, new_state)


MESH_ID = pl.DeviceIdType.MESH
VMEM_TOTAL = 67043328
CORES = 2
SIDE = 2
LAYER_VMEM = 50000000
FINISH_VMEM = 20000000


def greet(devices):
    barrier = pltpu.get_barrier_semaphore()
    for device in devices:
        pl.semaphore_signal(barrier, inc=1, device_id=device, device_id_type=MESH_ID)
    pl.semaphore_wait(barrier, len(devices))


def kv_peers(kv, n_kv):
    return [n_kv - 1 - kv, kv + 1 - 2 * lax.rem(kv, SIDE), lax.rem(kv + SIDE, n_kv)]


def send_all(devices, source, target, send_sem, recv_sem):
    for k, device in enumerate(devices):
        remote_to(device, source(device["kv"]), target(k), send_sem, recv_sem).start()


def landed(ref, sem):
    pltpu.make_async_copy(ref, ref, sem).wait()


def load_all(pairs, sem):
    for source, target in pairs:
        pltpu.make_async_copy(source, target, sem).start()


def silu(value):
    return value / (1.0 + jnp.exp(-value))


def as_row(column):
    lane = lax.broadcasted_iota(jnp.int32, (column.shape[0], LANES), 1)
    row = lax.broadcasted_iota(jnp.int32, (column.shape[0], LANES), 0)
    return jnp.sum(jnp.where(row == lane, column, 0.0), axis=0, keepdims=True)


def as_column(row_values, first, rows):
    lane = lax.broadcasted_iota(jnp.int32, (rows, LANES), 1)
    row = lax.broadcasted_iota(jnp.int32, (rows, LANES), 0)
    return jnp.sum(jnp.where(row + first == lane, row_values, 0.0), axis=1, keepdims=True)


def remote(axis, peer, source, target, send_sem, recv_sem):
    return remote_to({axis: peer}, source, target, send_sem, recv_sem)


def remote_to(device, source, target, send_sem, recv_sem):
    return pltpu.make_async_remote_copy(
        src_ref=source, dst_ref=target, send_sem=send_sem, recv_sem=recv_sem,
        device_id=device, device_id_type=MESH_ID,
    )


def far_first(chip, chips):
    def ascending(at, k):
        return k + 1 - (at + chips - 1 - k) // chips

    low = 1 - chip // (chips // 2)
    mirrored = chips - 1 - chip
    return [
        low * (chips - 1 - ascending(mirrored, k)) + (1 - low) * ascending(chip, k)
        for k in range(chips - 1)
    ]


def start_gather(slots, tp, n_tp, hub, send_sems, recv_sems):
    chips = n_tp // CORES
    chip, core = tp // CORES, lax.rem(tp, CORES)
    partner = chip * CORES + 1 - core
    order = far_first(chip, chips)

    def block(peer, slot, send):
        return remote("tp", peer, slots.at[slot], slots.at[slot], send_sems.at[send], recv_sems.at[slot])

    for peer in order:
        block(peer * CORES + hub, tp, 0).start()
    block(partner, tp, 0).start()
    relayed = [
        block(partner, source * CORES + side, 1) for source in order[::-1] for side in range(CORES)
    ]

    def take(first, last):
        for copy in relayed[first * CORES : last * CORES]:
            copy.wait_recv()

            @pl.when(core == hub)
            def _():
                copy.start()

    def take_own():
        block(partner, partner, 0).wait_recv()

    def close():
        landed(slots.at[:chips], send_sems.at[0])

        @pl.when(core == hub)
        def _():
            landed(slots.at[: len(relayed)], send_sems.at[1])

    return take, take_own, close, order[::-1]


def start_reduce(lhs, weight, parts, swapped, tp, send_sems, recv_sems):
    chip, core = tp // CORES, lax.rem(tp, CORES)
    chips, columns = parts.shape[1], parts.shape[3]

    def multiply(side):
        full = jnp.dot(lhs, weight[side], preferred_element_type=jnp.float32).astype(jnp.bfloat16)
        for z in range(chips):
            parts[side, z] = full[:, z * columns : (z + 1) * columns]

    multiply(core)
    remote(
        "tp", chip * CORES + 1 - core, parts.at[core], swapped, send_sems.at[0], recv_sems.at[0]
    ).start()
    multiply(1 - core)


def spread_pairs(parts, swapped, staged, into, tp, send_sems, recv_sems):
    chips = parts.shape[1]
    chip, core = tp // CORES, lax.rem(tp, CORES)
    landed(swapped, recv_sems.at[0])
    for k, other in enumerate(far_first(chip, chips) + [chip]):
        pair = parts[1 - core, other].astype(jnp.float32) + swapped[other].astype(jnp.float32)
        staged[k] = pair.astype(jnp.bfloat16)
        remote(
            "tp", other * CORES + 1 - core, staged.at[k], into.at[chip], send_sems.at[1], recv_sems.at[1]
        ).start()


def total_of(own, others):
    total = own.astype(jnp.float32)
    for step in range(others.shape[0]):
        total += others[step].astype(jnp.float32)
    return total


def layer_kernel(
    n_kv, n_tp, features,
    tokens_hbm, lengths_hbm, freq_hbm, gain_hbm, gain_two_hbm, state_hbm,
    wq_hbm, wk_hbm, wv_hbm, wg_hbm, wo_hbm, fg_hbm, fu_hbm, fd_hbm,
    out, state, s, sems,
):
    kv, tp = lax.axis_index("kv"), lax.axis_index("tp")
    chips = n_tp // CORES
    chip, core = tp // CORES, lax.rem(tp, CORES)
    gathered, gathered_two, merged, hidden = s["gathered"], s["gathered_two"], s["merged"], s["hidden"]
    halves, rows = gathered.shape[0], gathered.shape[3]
    batch = n_kv * rows
    q_width, v_width = wq_hbm.shape[1], wv_hbm.shape[1]
    units, columns = fg_hbm.shape[1], tokens_hbm.shape[3]

    def sides(ref, target):
        return [
            (
                ref.at[:, (z * CORES + side) * columns : (z * CORES + side + 1) * columns],
                target.at[side, :, z * columns : (z + 1) * columns],
            )
            for side in range(CORES)
            for z in range(chips)
        ]

    groups = {
        "tokens": [(tokens_hbm.at[:, h], gathered.at[h, tp]) for h in range(halves)],
        "lengths": [(lengths_hbm, s["lengths"])],
        "freq": [(freq_hbm, s["freq"])],
        "gain": [(gain_hbm, s["gain"])],
        "wqk": [(wq_hbm, s["wqk"].at[:, :q_width]), (wk_hbm, s["wqk"].at[:, q_width:])],
        "wvg": [(wv_hbm, s["wvg"].at[:, :v_width]), (wg_hbm, s["wvg"].at[:, v_width:])],
        "state": [(state_hbm, state)],
        "wo": sides(wo_hbm, s["wo"]),
        "gain_two": [(gain_two_hbm, s["gain_two"])],
        "fg": [(fg_hbm, s["fg"])],
        "fu": [(fu_hbm, s["fu"])],
        "fd": sides(fd_hbm, s["fd"]),
    }
    wholes = {
        "tokens": gathered.at[:, tp], "wqk": s["wqk"], "wvg": s["wvg"], "state": state, "wo": s["wo"], "fd": s["fd"],
        "lengths": s["lengths"], "freq": s["freq"], "gain": s["gain"],
        "gain_two": s["gain_two"], "fg": s["fg"], "fu": s["fu"],
    }
    pending = {}
    for i, (name, group) in enumerate(groups.items()):
        pending[name] = i
        load_all(group, sems["load"].at[i])

    def ready(*wanted):
        for name in wanted:
            if name in pending:
                landed(wholes[name], sems["load"].at[pending.pop(name)])

    partner = chip * CORES + 1 - core
    peers = [{"kv": peer, "tp": tp} for peer in kv_peers(kv, n_kv)]
    crossed = [{"kv": peer, "tp": partner} for peer in kv_peers(kv, n_kv)]
    along = [{"kv": kv, "tp": other * CORES + 1 - core} for other in far_first(chip, chips)]
    beside = {"kv": kv, "tp": partner}
    crossed_all = crossed + [beside]
    aside = [{"kv": kv, "tp": other * CORES + core} for other in far_first(chip, chips)]
    greet(along + aside + [beside] + peers + crossed)
    closing = []

    def close_sends():
        for extent, sem in closing:
            landed(extent, sem)
        closing.clear()

    def pair_of(name, h):
        return sems[name + "_s"].at[h], sems[name + "_r"].at[h]

    def kv_send(name, h, devices, source, target, extent):
        send_sem, recv_sem = sems[SHARED.get(name, name)].at[h, 0], sems[SHARED.get(name, name)].at[h, 1]
        send_all(devices, source, target, send_sem, recv_sem)
        closing.append((extent, send_sem))
        return lambda: landed(extent, recv_sem)

    def send_squares(name, h, devices):
        return kv_send(
            name, h, devices, lambda p: s[name].at[h, n_kv - 1], lambda n: s[name].at[h, n], s[name].at[h, : n_kv - 1]
        )

    def scale_of(name, h, wait):
        wait()
        total = s[name][h, 0]
        for n in range(1, n_kv):
            total += s[name][h, n]
        return lax.rsqrt(as_column(total, kv * rows, rows) / features + 1e-06)

    ready("tokens")
    first_gather = [start_gather(gathered.at[0], tp, n_tp, 0, *pair_of("g", 0))]
    ready("lengths", "freq", "gain")
    all_rows = halves * rows
    row = lax.broadcasted_iota(jnp.int32, (all_rows, all_rows), 0)
    col = lax.broadcasted_iota(jnp.int32, (all_rows, all_rows), 1)
    spread = jnp.where(row == col, s["lengths"][...].astype(jnp.float32), 0.0)
    angles = jnp.sum(spread, axis=1, keepdims=True) * s["freq"][...]
    cosine, sine = jnp.cos(angles), jnp.sin(angles)
    lane = lax.broadcasted_iota(jnp.int32, angles.shape, 1)
    sine = jnp.where(lane < QK // 2, -sine, sine)

    def gathered_product(gather, slots, gains, weight, between=None):
        take, take_own, _, near = gather
        span = CORES * columns

        def chunk(source):
            at = pl.multiple_of(source * span, span)
            x = jnp.concatenate(
                [slots[source * CORES + side].reshape(batch, columns) for side in range(CORES)], axis=1
            ).astype(jnp.float32)
            part = (x * gains[:, pl.ds(at, span)]).astype(jnp.bfloat16)
            s["normed"][:, pl.ds(at, span)] = part
            product = jnp.dot(part, weight[pl.ds(at, span), :], preferred_element_type=jnp.float32)
            return product, jnp.sum(x * x, axis=1, keepdims=True)

        take_own()
        if between is not None:
            between()
        product, squares = chunk(chip)
        for k, source in enumerate(near):
            take(k, k + 1)
            more, more_squares = chunk(source)
            product += more
            squares += more_squares
        return product.astype(jnp.bfloat16).reshape(n_kv, rows, product.shape[1]), as_row(squares)

    def project(weight):
        full = jnp.dot(s["normed"][...], weight[...], preferred_element_type=jnp.float32)
        return full.astype(jnp.bfloat16).reshape(n_kv, rows, full.shape[1])

    heads = q_width // QK
    width = v_width // heads
    out_a, out_b, in_a, in_b = s["out_a"], s["out_b"], s["in_a"], s["in_b"]
    first, second, copies_m, copies_q = [], [], [], []

    def start_next_gather(h):
        if h < halves:
            first_gather.append(start_gather(gathered.at[h], tp, n_tp, 0, *pair_of("g", h)))

    def project_first(h):
        out_a[h], s["squares"][h, n_kv - 1] = gathered_product(
            first_gather[h], gathered.at[h], s["gain"], s["wqk"], lambda: start_next_gather(h + 1)
        )
        first.append(kv_send("a", h, peers, lambda p: out_a.at[h, p], lambda n: in_a.at[h, n], in_a.at[h]))
        copies_q.append(send_squares("squares", h, peers))
        ready("wvg")
        out_b[h] = project(s["wvg"])
        second.append(kv_send("b", h, peers, lambda p: out_b.at[h, p], lambda n: in_b.at[h, n], in_b.at[h]))

    decays = []
    for head in range(heads):
        number = jnp.full((1, width), tp * heads + head, jnp.int32).astype(jnp.float32)
        decays.append(1.0 - jnp.exp2(-5.0 - 10.0 * number / (heads * n_tp - 1)))
    qk, value, retained = s["qk"], s["value"], s["retained"]

    def attend(h):
        base = h * rows
        first[h]()
        total = total_of(out_a[h, kv], in_a.at[h])
        scale = scale_of("squares", h, copies_q[h])
        total = total * scale
        cosines, sines = cosine[base : base + rows], sine[base : base + rows]
        blocks = []
        for start, factor in ((0, 1.0), (q_width, QK ** (-0.5))):
            for head in range(heads):
                part = total[:, start + head * QK : start + (head + 1) * QK]
                turned = (part * cosines + pltpu.roll(part, QK // 2, 1) * sines) * factor
                blocks.append(turned.astype(jnp.bfloat16).astype(jnp.float32))
        columns = jnp.concatenate(blocks * (LANES // (len(blocks) * rows)), axis=0).T
        qk[h] = columns
        for i in range(rows):
            for head in range(heads):
                query = columns[:, head * rows + i : head * rows + i + 1]
                retained[base + i : base + i + 1, head * width : (head + 1) * width] = jnp.sum(
                    query * state[base + i, head], axis=0, keepdims=True
                )
        second[h]()
        total = total_of(out_b[h, kv], in_b.at[h]) * scale
        values = total[:, :v_width].astype(jnp.bfloat16).astype(jnp.float32)
        value[base : base + rows] = values
        pieces = []
        for head in range(heads):
            overlap = jnp.sum(blocks[head] * blocks[heads + head], axis=1, keepdims=True)
            span = slice(head * width, (head + 1) * width)
            piece = decays[head] * retained[base : base + rows, span] + overlap * values[:, span]
            pieces.append(piece * lax.rsqrt(jnp.mean(piece * piece, axis=1, keepdims=True) + 1e-06))
        s["merged_out"][h] = (jnp.concatenate(pieces, axis=1) * silu(total[:, v_width:])).astype(jnp.bfloat16)
        copies_m.append(
            kv_send("m", h, crossed_all, lambda p: s["merged_out"].at[h], lambda n: merged.at[h, kv], merged.at[h])
        )

    block = 8

    def update(h):
        base = h * rows

        def update_step(i, carry):
            start = i * block
            turned = pltpu.roll(qk[h], lax.rem(LANES - start, LANES), 1)
            for n in range(block):
                for head in range(heads):
                    lane = (heads + head) * rows + n
                    at = base + start + n
                    outer = turned[:, lane : lane + 1] * value[pl.ds(at, 1), head * width : (head + 1) * width]
                    state[at, head] = decays[head] * state[at, head] + outer
            return carry

        lax.fori_loop(0, rows // block, update_step, 0)

    def reduce_start(h, lhs, weight, tag):
        start_reduce(lhs, s[weight], s["parts_" + tag].at[h], s["swapped_" + tag].at[h], tp, *pair_of("x", h))

    def reduce_spread(h, tag):
        swapped, staged = s["swapped_" + tag].at[h], s["staged_" + tag].at[h]
        send_sems, recv_sems = pair_of("x", h)
        spread_pairs(s["parts_" + tag].at[h], swapped, staged, s["landed_" + tag].at[h], tp, send_sems, recv_sems)
        closing.extend([(swapped, send_sems.at[0]), (staged, send_sems.at[1])])

    def reduce_total(h, tag):
        into = s["landed_" + tag].at[h]
        landed(into, pair_of("x", h)[1].at[1])
        return total_of(into[0], into.at[1:])

    gate_out, up_out, gate_in, up_in = s["gate_out"], s["up_out"], s["gate_in"], s["up_in"]
    copies_e, copies_f, copies_h, copies_u = [], [], [], []
    first_units = (units // LANES + 1) // 2 * LANES

    def project_second(h):
        for span in (slice(0, first_units), slice(first_units, units)):
            if span.start == 0:
                gate_out[h, :, :, span], s["squares_two"][h, n_kv - 1] = gathered_product(
                    second_gather[h], gathered_two.at[h], s["gain_two"], s["fg"].at[:, span]
                )
            else:
                gate_out[h, :, :, span] = project(s["fg"].at[:, span])
            send_all(
                crossed_all, lambda p: gate_out.at[h, p, :, span], lambda n: gate_in.at[h, n, :, span],
                sems["a"].at[h, 0], sems["a"].at[h, 1],
            )
            if span.start == 0:
                copies_u.append(send_squares("squares_two", h, crossed))
        closing.append((gate_in.at[h], sems["a"].at[h, 0]))
        copies_e.append(lambda: landed(gate_in.at[h], sems["a"].at[h, 1]))
        up_out[h] = project(s["fu"])
        copies_f.append(
            kv_send("f", h, crossed_all, lambda p: up_out.at[h, p], lambda n: up_in.at[h, n], up_in.at[h])
        )

    def activate(h):
        copies_e[h]()
        total = total_of(gate_in[h, 0], gate_in.at[h, 1:])
        scale = scale_of("squares_two", h, copies_u[h])
        activated = silu(total * scale)
        copies_f[h]()
        up = total_of(up_in[h, 0], up_in.at[h, 1:]) * scale
        s["hidden_out"][h] = (activated * up).astype(jnp.bfloat16)
        copies_h.append(
            kv_send("h", h, crossed_all, lambda p: s["hidden_out"].at[h], lambda n: hidden.at[h, kv], hidden.at[h])
        )

    second_gather = []
    ready("wqk")
    project_first(0)
    ready("wo")
    remote_to(beside, s["wo"], s["wo_far"], sems["wo"].at[0], sems["wo"].at[1]).start()
    for h in range(1, halves):
        project_first(h)
    ready("state")
    for h in range(halves):
        attend(h)
    landed(s["wo_far"], sems["wo"].at[1])
    for h in range(halves):
        copies_m[h]()
        reduce_start(h, merged[h].reshape(batch, v_width), "wo_far", "x")
        reduce_spread(h, "x")
        if h + 1 < halves:
            update(h)
    for gather in first_gather:
        gather[2]()
    for h in range(halves):
        total = reduce_total(h, "x")
        own = gathered[h, tp].reshape(batch, LANES).astype(jnp.float32)
        gathered_two[h, tp] = (own + total).astype(jnp.bfloat16).reshape(n_kv, rows, LANES)
        second_gather.append(start_gather(gathered_two.at[h], tp, n_tp, 1, *pair_of("g", h)))
        if h == 0:
            update(halves - 1)
    ready("gain_two", "fg", "fu")
    landed(s["wo_far"], sems["wo"].at[0])
    close_sends()
    for h in range(halves):
        project_second(h)
    for h in range(halves):
        activate(h)
    ready("fd")
    for h in range(halves):
        copies_h[h]()
        reduce_start(h, hidden[h].reshape(batch, units), "fd", "d")
        reduce_spread(h, "d")
    for h in range(halves):
        total = reduce_total(h, "d")
        own = gathered_two[h, tp].reshape(batch, LANES).astype(jnp.float32)
        out[:, h] = (own + total).astype(jnp.bfloat16).reshape(n_kv, rows, LANES)
    close_sends()
    for gather in second_gather:
        gather[2]()


def finish_kernel(state, out, state_to, out_to, store_sems):
    chunks = store_sems.shape[0] - 1
    size = state.shape[0] // chunks
    targets = [(out, out_to)]
    for i in range(chunks):
        part = pl.ds(i * size, size)
        targets.append((state.at[part], state_to.at[part]))
    copies = [
        pltpu.make_async_copy(source, target, store_sems.at[i]) for i, (source, target) in enumerate(targets)
    ]
    for copy in copies:
        copy.start()
    for copy in copies:
        copy.wait()


HALVES = 2
SHARED = {"f": "b", "h": "m", "squares_two": "squares"}


def fused_on_device(n_kv, n_tp, *arrays):
    (
        tokens, lengths, state, mixer_gain, wq, wk, wv, wg, wo, channel_gain, fg, fu, fd,
    ) = arrays
    columns = tokens.shape[1]
    rows = state.shape[0] // HALVES
    batch = n_kv * rows
    depth, q_width = wq.shape
    v_width, units = wv.shape[1], fg.shape[1]
    bf16, f32 = jnp.bfloat16, jnp.float32
    vmem = pl.BlockSpec(memory_space=pltpu.VMEM)
    hbm = pl.BlockSpec(memory_space=pltpu.HBM)
    chips = n_tp // CORES
    index = np.arange(QK) % (QK // 2)
    freq = jnp.asarray((10000.0 ** (-index / (QK // 2))).astype(np.float32))[None, :]
    a_width, b_width = 2 * q_width, 2 * v_width

    def buffer(*shape, dtype=bf16):
        return pltpu.VMEM((HALVES,) + shape, dtype)

    scratch = {
        "lengths": pltpu.VMEM((1, HALVES * rows), jnp.int32),
        "freq": pltpu.VMEM((1, QK), f32),
        "gain": pltpu.VMEM((1, depth), f32),
        "gain_two": pltpu.VMEM((1, depth), f32),
        "gathered": buffer(n_tp, n_kv, rows, columns),
        "gathered_two": buffer(n_tp, n_kv, rows, columns),
        "out_a": buffer(n_kv, rows, a_width),
        "out_b": buffer(n_kv, rows, b_width),
        "in_a": buffer(n_kv - 1, rows, a_width),
        "in_b": buffer(n_kv - 1, rows, b_width),
        "qk": buffer(QK, LANES, dtype=f32),
        "retained": pltpu.VMEM((HALVES * rows, v_width), f32),
        "value": pltpu.VMEM((HALVES * rows, v_width), f32),
        "merged": buffer(n_kv, rows, v_width),
        "merged_out": buffer(rows, v_width),
        "normed": pltpu.VMEM((batch, depth), bf16),
        "gate_out": buffer(n_kv, rows, units),
        "up_out": buffer(n_kv, rows, units),
        "gate_in": buffer(n_kv, rows, units),
        "up_in": buffer(n_kv, rows, units),
        "hidden_out": buffer(rows, units),
        "hidden": buffer(n_kv, rows, units),
        "squares": buffer(n_kv, 1, LANES, dtype=f32),
        "squares_two": buffer(n_kv, 1, LANES, dtype=f32),
    }
    shapes = {
        "wqk": (depth, 2 * q_width), "wvg": (depth, 2 * v_width), "fg": fg.shape, "fu": fu.shape,
        "wo": (CORES, wo.shape[0], chips * columns),
        "wo_far": (CORES, wo.shape[0], chips * columns),
        "fd": (CORES, fd.shape[0], chips * columns),
    }
    scratch.update({name: pltpu.VMEM(shape, bf16) for name, shape in shapes.items()})
    for tag in ("x", "d"):
        scratch["parts_" + tag] = buffer(CORES, chips, batch, columns)
        scratch["swapped_" + tag] = buffer(chips, batch, columns)
        scratch["staged_" + tag] = buffer(chips, batch, columns)
        scratch["landed_" + tag] = buffer(chips, batch, columns)
    dma = pltpu.SemaphoreType.DMA
    sems = {"load": dma((12,)), "wo": dma((2,))}
    sems["g_s"], sems["g_r"] = dma((HALVES, 2)), dma((HALVES, n_tp))
    for tag in ("x_s", "x_r", "a", "b", "m", "squares"):
        sems[tag] = dma((HALVES, 2))
    operands = (
        tokens.reshape(n_kv, HALVES, rows, columns), lengths[None, :], freq, mixer_gain[None, :],
        channel_gain[None, :], state, wq, wk, wv, wg, wo, fg, fu, fd,
    )
    out_shape = (n_kv, HALVES, rows, columns)
    out, new_state = pl.pallas_call(
        functools.partial(layer_kernel, n_kv, n_tp, depth * n_kv),
        out_shape=(pltpu.VMEM(out_shape, bf16), pltpu.VMEM(state.shape, f32)),
        in_specs=[hbm] * 14,
        out_specs=(vmem, vmem),
        scratch_shapes=[scratch, sems],
        compiler_params=pltpu.CompilerParams(
            collective_id=0, has_side_effects=True, vmem_limit_bytes=LAYER_VMEM
        ),
        name="layer",
    )(*[pltpu.with_memory_space_constraint(a, pltpu.HBM) for a in operands])
    new_state, out = pl.pallas_call(
        finish_kernel,
        out_shape=(
            jax.ShapeDtypeStruct(state.shape, f32),
            jax.ShapeDtypeStruct(out_shape, bf16),
        ),
        in_specs=[vmem, vmem],
        out_specs=(hbm, hbm),
        scratch_shapes=[pltpu.SemaphoreType.DMA((9,))],
        compiler_params=pltpu.CompilerParams(vmem_limit_bytes=FINISH_VMEM),
        name="finish",
    )(new_state, out)
    return out.reshape(tokens.shape), new_state


def fits(n_kv, n_tp, arrays):
    tokens, state, ffn_gate = arrays[0], arrays[2], arrays[10]
    rows, heads = state.shape[0], state.shape[1]
    return (
        tokens.shape[1] % LANES == 0
        and n_tp % CORES == 0
        and n_tp > CORES
        and n_kv == SIDE * SIDE
        and 4 * state.size < VMEM_TOTAL // 4
        and ffn_gate.shape[1] % LANES == 0
        and tokens.shape[1] == LANES
        and tokens.shape[0] == n_kv * rows
        and rows % (16 * HALVES) == 0
        and n_kv * rows // HALVES <= LANES
        and 2 * heads * rows == LANES
        and state.shape[2] == QK == LANES
        and state.shape[3] % LANES == 0
    )


def per_device(n_kv, n_tp, *arrays):
    if fits(n_kv, n_tp, arrays):
        return fused_on_device(n_kv, n_tp, *arrays)
    return on_device(*arrays)


def solution(mesh):
    in_specs = (
        P(None, ("kv", "tp")),
        P("kv"),
        P("kv", "tp", None, None),
        P("kv"),
        P("kv", "tp"),
        P("kv", "tp"),
        P("kv", "tp"),
        P("kv", "tp"),
        P("tp", "kv"),
        P("kv"),
        P("kv", "tp"),
        P("kv", "tp"),
        P("tp", "kv"),
    )
    out_specs = (P(None, ("kv", "tp")), P("kv", "tp", None, None))
    return jax.shard_map(
        functools.partial(per_device, mesh.shape["kv"], mesh.shape["tp"]),
        mesh=mesh, in_specs=in_specs, out_specs=out_specs, check_vma=False
    )
```

```python
import functools

import jax
import jax.numpy as jnp
import numpy as np
from jax import lax
from jax.experimental import pallas as pl
from jax.experimental.pallas import tpu as pltpu
from jax.sharding import PartitionSpec as P

D = 4096
HEADS = 16
QK = 128
LANES = 128


def rotate_heads(vectors, positions):
    half_dim = vectors.shape[-1] // 2
    frequency = 10000.0 ** (-jnp.arange(half_dim, dtype=jnp.float32) / half_dim)
    angles = positions.astype(jnp.float32)[:, None, None] * frequency
    cosine = jnp.cos(angles)
    sine_part = jnp.sin(angles)
    first_half = vectors[..., :half_dim]
    second = vectors[..., half_dim:]
    return jnp.concatenate(
        [first_half * cosine - second * sine_part, first_half * sine_part + second * cosine],
        axis=-1,
    )


def gathered_rows(columns):
    return lax.all_gather(columns, "tp", axis=1, tiled=True)


def owned_sums(partial_value, squares):
    raw_sums, totals = (
        lax.psum_scatter(
            partial_value.astype(jnp.bfloat16), "kv", scatter_dimension=0, tiled=True
        ).astype(jnp.float32),
        lax.psum_scatter(
            squares.astype(jnp.bfloat16), "kv", scatter_dimension=0, tiled=True
        ).astype(jnp.float32),
    )
    summed = raw_sums * lax.rsqrt(totals / D + 1e-06)[:, None]
    return summed


def every_sum(partial_value, squares):
    raw_sums, totals = (
        lax.psum(partial_value.astype(jnp.bfloat16), "kv").astype(jnp.float32),
        lax.psum(squares.astype(jnp.bfloat16), "kv").astype(jnp.float32),
    )
    summed = raw_sums * lax.rsqrt(totals / D + 1e-06)[:, None]
    return summed


def on_device(
    tokens,
    lengths,
    retention_state,
    mixer_gain,
    query_weight,
    key_weight,
    value_weight,
    gate_weight,
    output_weight,
    channel_gain,
    ffn_gate,
    ffn_up,
    ffn_down,
):
    feature_block = gathered_rows(tokens).astype(jnp.float32)
    squares = jnp.sum(feature_block * feature_block, axis=1)
    normed = (feature_block * mixer_gain).astype(jnp.bfloat16)
    partial_value = jnp.concatenate(
        [
            jnp.dot(normed, query_weight, preferred_element_type=jnp.float32),
            jnp.dot(normed, key_weight, preferred_element_type=jnp.float32),
            jnp.dot(normed, value_weight, preferred_element_type=jnp.float32),
            jnp.dot(normed, gate_weight, preferred_element_type=jnp.float32),
        ],
        axis=1,
    )
    owned_rows = owned_sums(partial_value, squares)
    local_heads = query_weight.shape[1] // QK
    q_width = query_weight.shape[1]
    v_width = value_weight.shape[1]
    head_width = v_width // local_heads
    seq_rows = owned_rows.shape[0]
    query_rows = rotate_heads(
        owned_rows[:, :q_width].reshape(seq_rows, local_heads, QK), lengths
    ).astype(jnp.bfloat16)
    key_rows = (
        rotate_heads(
            owned_rows[:, q_width : 2 * q_width].reshape(seq_rows, local_heads, QK), lengths
        )
        * QK ** (-0.5)
    ).astype(jnp.bfloat16)
    value_rows = (
        owned_rows[:, 2 * q_width : 2 * q_width + v_width]
        .astype(jnp.bfloat16)
        .reshape(seq_rows, local_heads, head_width)
    )
    gate_rows = owned_rows[:, 2 * q_width + v_width :]
    head_ids = (lax.axis_index("tp") * local_heads + jnp.arange(local_heads)).astype(jnp.float32)
    decay_rate = 1.0 - 2.0 ** (-5.0 - 10.0 * head_ids / (HEADS - 1))
    new_state = (
        decay_rate[None, :, None, None] * retention_state
        + key_rows.astype(jnp.float32)[..., :, None] * value_rows.astype(jnp.float32)[..., None, :]
    )
    retained = jnp.einsum(
        "bhk,bhkv->bhv", query_rows.astype(jnp.float32), new_state, precision=lax.Precision.HIGHEST
    )
    normalized = retained * lax.rsqrt(jnp.mean(retained * retained, axis=-1) + 1e-06)[..., None]
    merged = (normalized.reshape(seq_rows, v_width) * jax.nn.silu(gate_rows)).astype(jnp.bfloat16)
    mixed_part = jnp.dot(
        lax.all_gather(merged, "kv", axis=0, tiled=True),
        output_weight,
        preferred_element_type=jnp.float32,
    )
    mixed_cols = lax.psum_scatter(
        mixed_part.astype(jnp.bfloat16), "tp", scatter_dimension=1, tiled=True
    ).astype(jnp.float32)
    residual = (tokens.astype(jnp.float32) + mixed_cols).astype(jnp.bfloat16)
    block_two = gathered_rows(residual).astype(jnp.float32)
    squares_two = jnp.sum(block_two * block_two, axis=1)
    normed_two = (block_two * channel_gain).astype(jnp.bfloat16)
    partial_two = jnp.concatenate(
        [
            jnp.dot(normed_two, ffn_gate, preferred_element_type=jnp.float32),
            jnp.dot(normed_two, ffn_up, preferred_element_type=jnp.float32),
        ],
        axis=1,
    )
    hidden_units = ffn_gate.shape[1]
    summed = every_sum(partial_two, squares_two)
    hidden = (jax.nn.silu(summed[:, :hidden_units]) * summed[:, hidden_units:]).astype(jnp.bfloat16)
    down_part = jnp.dot(hidden, ffn_down, preferred_element_type=jnp.float32)
    down_sums = lax.psum_scatter(
        down_part.astype(jnp.bfloat16), "tp", scatter_dimension=1, tiled=True
    ).astype(jnp.float32)
    layer_output = (residual.astype(jnp.float32) + down_sums).astype(jnp.bfloat16)
    return (layer_output, new_state)


MESH_ID = pl.DeviceIdType.MESH
VMEM_TOTAL = 67043328
CORES = 2
SIDE = 2
LAYER_VMEM = 50000000
FINISH_VMEM = 20000000


def greet(devices):
    barrier = pltpu.get_barrier_semaphore()
    for device in devices:
        pl.semaphore_signal(barrier, inc=1, device_id=device, device_id_type=MESH_ID)
    pl.semaphore_wait(barrier, len(devices))


def kv_peers(kv, n_kv):
    return [n_kv - 1 - kv, kv + 1 - 2 * lax.rem(kv, SIDE), lax.rem(kv + SIDE, n_kv)]


def send_all(devices, source, target, send_sem, recv_sem):
    for k, device in enumerate(devices):
        remote_to(device, source(device["kv"]), target(k), send_sem, recv_sem).start()


def landed(ref, sem):
    pltpu.make_async_copy(ref, ref, sem).wait()


def load_all(pairs, sem):
    for source, target in pairs:
        pltpu.make_async_copy(source, target, sem).start()


def silu(value):
    return value / (1.0 + jnp.exp(-value))


def as_row(column):
    lane = lax.broadcasted_iota(jnp.int32, (column.shape[0], LANES), 1)
    row = lax.broadcasted_iota(jnp.int32, (column.shape[0], LANES), 0)
    return jnp.sum(jnp.where(row == lane, column, 0.0), axis=0, keepdims=True)


def as_column(row_values, first, rows):
    lane = lax.broadcasted_iota(jnp.int32, (rows, LANES), 1)
    row = lax.broadcasted_iota(jnp.int32, (rows, LANES), 0)
    return jnp.sum(jnp.where(row + first == lane, row_values, 0.0), axis=1, keepdims=True)


def remote(axis, peer, source, target, send_sem, recv_sem):
    return remote_to({axis: peer}, source, target, send_sem, recv_sem)


def remote_to(device, source, target, send_sem, recv_sem):
    return pltpu.make_async_remote_copy(
        src_ref=source, dst_ref=target, send_sem=send_sem, recv_sem=recv_sem,
        device_id=device, device_id_type=MESH_ID,
    )


def far_first(chip, chips):
    def ascending(at, k):
        return k + 1 - (at + chips - 1 - k) // chips

    low = 1 - chip // (chips // 2)
    mirrored = chips - 1 - chip
    return [
        low * (chips - 1 - ascending(mirrored, k)) + (1 - low) * ascending(chip, k)
        for k in range(chips - 1)
    ]


def start_gather(slots, tp, n_tp, hub, send_sems, recv_sems):
    chips = n_tp // CORES
    chip, core = tp // CORES, lax.rem(tp, CORES)
    partner = chip * CORES + 1 - core
    order = far_first(chip, chips)

    def block(peer, slot, send):
        return remote("tp", peer, slots.at[slot], slots.at[slot], send_sems.at[send], recv_sems.at[slot])

    for peer in order:
        block(peer * CORES + hub, tp, 0).start()
    block(partner, tp, 0).start()
    relayed = [
        block(partner, source * CORES + side, 1) for source in order[::-1] for side in range(CORES)
    ]

    def take(first, last):
        for copy in relayed[first * CORES : last * CORES]:
            copy.wait_recv()

            @pl.when(core == hub)
            def _():
                copy.start()

    def take_own():
        block(partner, partner, 0).wait_recv()

    def close():
        landed(slots.at[:chips], send_sems.at[0])

        @pl.when(core == hub)
        def _():
            landed(slots.at[: len(relayed)], send_sems.at[1])

    return take, take_own, close, order[::-1]


def start_reduce(lhs, weight, parts, swapped, tp, send_sems, recv_sems):
    chip, core = tp // CORES, lax.rem(tp, CORES)
    chips, columns = parts.shape[1], parts.shape[3]

    def multiply(side):
        full = jnp.dot(lhs, weight[side], preferred_element_type=jnp.float32).astype(jnp.bfloat16)
        for z in range(chips):
            parts[side, z] = full[:, z * columns : (z + 1) * columns]

    multiply(core)
    remote(
        "tp", chip * CORES + 1 - core, parts.at[core], swapped, send_sems.at[0], recv_sems.at[0]
    ).start()
    multiply(1 - core)


def spread_pairs(parts, swapped, staged, into, tp, send_sems, recv_sems):
    chips = parts.shape[1]
    chip, core = tp // CORES, lax.rem(tp, CORES)
    landed(swapped, recv_sems.at[0])
    for k, other in enumerate(far_first(chip, chips) + [chip]):
        pair = parts[1 - core, other].astype(jnp.float32) + swapped[other].astype(jnp.float32)
        staged[k] = pair.astype(jnp.bfloat16)
        remote(
            "tp", other * CORES + 1 - core, staged.at[k], into.at[chip], send_sems.at[1], recv_sems.at[1]
        ).start()


def total_of(own, others):
    total = own.astype(jnp.float32)
    for step in range(others.shape[0]):
        total += others[step].astype(jnp.float32)
    return total


def layer_kernel(
    n_kv, n_tp, features,
    tokens_hbm, lengths_hbm, freq_hbm, gain_hbm, gain_two_hbm, state_hbm,
    wq_hbm, wk_hbm, wv_hbm, wg_hbm, wo_hbm, fg_hbm, fu_hbm, fd_hbm,
    out, state, s, sems,
):
    kv, tp = lax.axis_index("kv"), lax.axis_index("tp")
    chips = n_tp // CORES
    chip, core = tp // CORES, lax.rem(tp, CORES)
    gathered, gathered_two, merged, hidden = s["gathered"], s["gathered_two"], s["merged"], s["hidden"]
    halves, rows = gathered.shape[0], gathered.shape[3]
    batch = n_kv * rows
    q_width, v_width = wq_hbm.shape[1], wv_hbm.shape[1]
    units, columns = fg_hbm.shape[1], tokens_hbm.shape[3]

    def sides(ref, target):
        return [
            (
                ref.at[:, (z * CORES + side) * columns : (z * CORES + side + 1) * columns],
                target.at[side, :, z * columns : (z + 1) * columns],
            )
            for side in range(CORES)
            for z in range(chips)
        ]

    groups = {
        "tokens": [(tokens_hbm.at[:, h], gathered.at[h, tp]) for h in range(halves)],
        "lengths": [(lengths_hbm, s["lengths"])],
        "freq": [(freq_hbm, s["freq"])],
        "gain": [(gain_hbm, s["gain"])],
        "wp": [
            (wq_hbm, s["wp"].at[:, :q_width]),
            (wk_hbm, s["wp"].at[:, q_width : 2 * q_width]),
            (wv_hbm, s["wp"].at[:, 2 * q_width : 2 * q_width + v_width]),
            (wg_hbm, s["wp"].at[:, 2 * q_width + v_width :]),
        ],
        "state": [(state_hbm, state)],
        "wo": sides(wo_hbm, s["wo"]),
        "gain_two": [(gain_two_hbm, s["gain_two"])],
        "fg": [(fg_hbm, s["fg"])],
        "fu": [(fu_hbm, s["fu"])],
        "fd": sides(fd_hbm, s["fd"]),
    }
    wholes = {
        "tokens": gathered.at[:, tp], "wp": s["wp"], "state": state, "wo": s["wo"], "fd": s["fd"],
        "lengths": s["lengths"], "freq": s["freq"], "gain": s["gain"],
        "gain_two": s["gain_two"], "fg": s["fg"], "fu": s["fu"],
    }
    pending = {}
    for i, (name, group) in enumerate(groups.items()):
        pending[name] = i
        load_all(group, sems["load"].at[i])

    def ready(*wanted):
        for name in wanted:
            if name in pending:
                landed(wholes[name], sems["load"].at[pending.pop(name)])

    partner = chip * CORES + 1 - core
    peers = [{"kv": peer, "tp": tp} for peer in kv_peers(kv, n_kv)]
    crossed = [{"kv": peer, "tp": partner} for peer in kv_peers(kv, n_kv)]
    along = [{"kv": kv, "tp": other * CORES + 1 - core} for other in far_first(chip, chips)]
    beside = {"kv": kv, "tp": partner}
    crossed_all = crossed + [beside]
    aside = [{"kv": kv, "tp": other * CORES + core} for other in far_first(chip, chips)]
    greet(along + aside + [beside] + peers + crossed)
    closing = []

    def close_sends():
        for extent, sem in closing:
            landed(extent, sem)
        closing.clear()

    def pair_of(name, h):
        return sems[name + "_s"].at[h], sems[name + "_r"].at[h]

    def kv_send(name, h, devices, source, target, extent):
        send_sem, recv_sem = sems[SHARED.get(name, name)].at[h, 0], sems[SHARED.get(name, name)].at[h, 1]
        send_all(devices, source, target, send_sem, recv_sem)
        closing.append((extent, send_sem))
        return lambda: landed(extent, recv_sem)

    def send_squares(name, h, devices):
        return kv_send(
            name, h, devices, lambda p: s[name].at[h, n_kv - 1], lambda n: s[name].at[h, n], s[name].at[h, : n_kv - 1]
        )

    def scale_of(name, h, wait):
        wait()
        total = s[name][h, 0]
        for n in range(1, n_kv):
            total += s[name][h, n]
        return lax.rsqrt(as_column(total, kv * rows, rows) / features + 1e-06)

    ready("tokens")
    first_gather = [start_gather(gathered.at[0], tp, n_tp, 0, *pair_of("g", 0))]
    ready("lengths", "freq", "gain")
    def gathered_product(gather, slots, gains, weight, between=None):
        take, take_own, _, near = gather
        span = CORES * columns

        def chunk(source):
            at = pl.multiple_of(source * span, span)
            x = jnp.concatenate(
                [slots[source * CORES + side].reshape(batch, columns) for side in range(CORES)], axis=1
            ).astype(jnp.float32)
            part = (x * gains[:, pl.ds(at, span)]).astype(jnp.bfloat16)
            s["normed"][:, pl.ds(at, span)] = part
            product = jnp.dot(part, weight[pl.ds(at, span), :], preferred_element_type=jnp.float32)
            return product, jnp.sum(x * x, axis=1, keepdims=True)

        take_own()
        product, squares = chunk(chip)
        if between is not None:
            between()
        for k, source in enumerate(near):
            take(k, k + 1)
            more, more_squares = chunk(source)
            product += more
            squares += more_squares
        return product.astype(jnp.bfloat16).reshape(n_kv, rows, product.shape[1]), as_row(squares)

    def project(weight):
        full = jnp.dot(s["normed"][...], weight[...], preferred_element_type=jnp.float32)
        return full.astype(jnp.bfloat16).reshape(n_kv, rows, full.shape[1])

    heads = q_width // QK
    width = v_width // heads
    out_a, out_b, in_a, in_b = s["out_a"], s["out_b"], s["in_a"], s["in_b"]
    first, second, copies_m, copies_q = [], [], [], []

    angles_of = []

    def find_angles():
        all_rows = halves * rows
        row = lax.broadcasted_iota(jnp.int32, (all_rows, all_rows), 0)
        col = lax.broadcasted_iota(jnp.int32, (all_rows, all_rows), 1)
        spread = jnp.where(row == col, s["lengths"][...].astype(jnp.float32), 0.0)
        angles = jnp.sum(spread, axis=1, keepdims=True) * s["freq"][...]
        cosine, sine = jnp.cos(angles), jnp.sin(angles)
        lane = lax.broadcasted_iota(jnp.int32, angles.shape, 1)
        sine = jnp.where(lane < QK // 2, -sine, sine)
        angles_of.extend([cosine, sine])

    def start_next_gather(h):
        if h == 1:
            find_angles()
        if h < halves:
            first_gather.append(start_gather(gathered.at[h], tp, n_tp, 0, *pair_of("g", h)))

    def project_first(h):
        product, s["squares"][h, n_kv - 1] = gathered_product(
            first_gather[h], gathered.at[h], s["gain"], s["wp"], lambda: start_next_gather(h + 1)
        )
        out_a[h] = product[:, :, : 2 * q_width]
        out_b[h] = product[:, :, 2 * q_width :]
        first.append(kv_send("a", h, peers, lambda p: out_a.at[h, p], lambda n: in_a.at[h, n], in_a.at[h]))
        copies_q.append(send_squares("squares", h, peers))
        second.append(kv_send("b", h, peers, lambda p: out_b.at[h, p], lambda n: in_b.at[h, n], in_b.at[h]))

    decays = []
    for head in range(heads):
        number = jnp.full((1, width), tp * heads + head, jnp.int32).astype(jnp.float32)
        decays.append(1.0 - jnp.exp2(-5.0 - 10.0 * number / (heads * n_tp - 1)))
    qk, value, retained = s["qk"], s["value"], s["retained"]

    def attend(h):
        base = h * rows
        first[h]()
        total = total_of(out_a[h, kv], in_a.at[h])
        scale = scale_of("squares", h, copies_q[h])
        total = total * scale
        cosines, sines = [table[base : base + rows] for table in angles_of]
        blocks = []
        for start, factor in ((0, 1.0), (q_width, QK ** (-0.5))):
            for head in range(heads):
                part = total[:, start + head * QK : start + (head + 1) * QK]
                turned = (part * cosines + pltpu.roll(part, QK // 2, 1) * sines) * factor
                blocks.append(turned.astype(jnp.bfloat16).astype(jnp.float32))
        columns = jnp.concatenate(blocks * (LANES // (len(blocks) * rows)), axis=0).T
        qk[h] = columns
        for i in range(rows):
            for head in range(heads):
                query = columns[:, head * rows + i : head * rows + i + 1]
                retained[base + i : base + i + 1, head * width : (head + 1) * width] = jnp.sum(
                    query * state[base + i, head], axis=0, keepdims=True
                )
        second[h]()
        total = total_of(out_b[h, kv], in_b.at[h]) * scale
        values = total[:, :v_width].astype(jnp.bfloat16).astype(jnp.float32)
        value[base : base + rows] = values
        pieces = []
        for head in range(heads):
            overlap = jnp.sum(blocks[head] * blocks[heads + head], axis=1, keepdims=True)
            span = slice(head * width, (head + 1) * width)
            piece = decays[head] * retained[base : base + rows, span] + overlap * values[:, span]
            pieces.append(piece * lax.rsqrt(jnp.mean(piece * piece, axis=1, keepdims=True) + 1e-06))
        s["merged_out"][h] = (jnp.concatenate(pieces, axis=1) * silu(total[:, v_width:])).astype(jnp.bfloat16)
        copies_m.append(
            kv_send("m", h, crossed_all, lambda p: s["merged_out"].at[h], lambda n: merged.at[h, kv], merged.at[h])
        )

    block = 8

    def update(h):
        base = h * rows

        def update_step(i, carry):
            start = i * block
            turned = pltpu.roll(qk[h], lax.rem(LANES - start, LANES), 1)
            for n in range(block):
                for head in range(heads):
                    lane = (heads + head) * rows + n
                    at = base + start + n
                    outer = turned[:, lane : lane + 1] * value[pl.ds(at, 1), head * width : (head + 1) * width]
                    state[at, head] = decays[head] * state[at, head] + outer
            return carry

        lax.fori_loop(0, rows // block, update_step, 0)

    def reduce_start(h, lhs, weight, tag):
        start_reduce(lhs, s[weight], s["parts_" + tag].at[h], s["swapped_" + tag].at[h], tp, *pair_of("x", h))

    def reduce_spread(h, tag):
        swapped, staged = s["swapped_" + tag].at[h], s["staged_" + tag].at[h]
        send_sems, recv_sems = pair_of("x", h)
        spread_pairs(s["parts_" + tag].at[h], swapped, staged, s["landed_" + tag].at[h], tp, send_sems, recv_sems)
        closing.extend([(swapped, send_sems.at[0]), (staged, send_sems.at[1])])

    def reduce_total(h, tag):
        into = s["landed_" + tag].at[h]
        landed(into, pair_of("x", h)[1].at[1])
        return total_of(into[0], into.at[1:])

    gate_out, up_out, gate_in, up_in = s["gate_out"], s["up_out"], s["gate_in"], s["up_in"]
    copies_e, copies_f, copies_h, copies_u = [], [], [], []
    first_units = (units // LANES + 1) // 2 * LANES

    def project_second(h):
        for span in (slice(0, first_units), slice(first_units, units)):
            if span.start == 0:
                gate_out[h, :, :, span], s["squares_two"][h, n_kv - 1] = gathered_product(
                    second_gather[h], gathered_two.at[h], s["gain_two"], s["fg"].at[:, span]
                )
            else:
                gate_out[h, :, :, span] = project(s["fg"].at[:, span])
            send_all(
                crossed_all, lambda p: gate_out.at[h, p, :, span], lambda n: gate_in.at[h, n, :, span],
                sems["a"].at[h, 0], sems["a"].at[h, 1],
            )
            if span.start == 0:
                copies_u.append(send_squares("squares_two", h, crossed))
        closing.append((gate_in.at[h], sems["a"].at[h, 0]))
        copies_e.append(lambda: landed(gate_in.at[h], sems["a"].at[h, 1]))
        up_out[h] = project(s["fu"])
        copies_f.append(
            kv_send("f", h, crossed_all, lambda p: up_out.at[h, p], lambda n: up_in.at[h, n], up_in.at[h])
        )

    def activate(h):
        copies_e[h]()
        total = total_of(gate_in[h, 0], gate_in.at[h, 1:])
        scale = scale_of("squares_two", h, copies_u[h])
        activated = silu(total * scale)
        copies_f[h]()
        up = total_of(up_in[h, 0], up_in.at[h, 1:]) * scale
        s["hidden_out"][h] = (activated * up).astype(jnp.bfloat16)
        copies_h.append(
            kv_send("h", h, crossed_all, lambda p: s["hidden_out"].at[h], lambda n: hidden.at[h, kv], hidden.at[h])
        )

    second_gather = []
    ready("wp")
    project_first(0)
    ready("wo")
    remote_to(beside, s["wo"], s["wo_far"], sems["wo"].at[0], sems["wo"].at[1]).start()
    for h in range(1, halves):
        project_first(h)
    ready("state")
    for h in range(halves):
        attend(h)
    landed(s["wo_far"], sems["wo"].at[1])
    for h in range(halves):
        copies_m[h]()
        reduce_start(h, merged[h].reshape(batch, v_width), "wo_far", "x")
        reduce_spread(h, "x")
        if h + 1 < halves:
            update(h)
    for gather in first_gather:
        gather[2]()
    for h in range(halves):
        total = reduce_total(h, "x")
        own = gathered[h, tp].reshape(batch, LANES).astype(jnp.float32)
        gathered_two[h, tp] = (own + total).astype(jnp.bfloat16).reshape(n_kv, rows, LANES)
        second_gather.append(start_gather(gathered_two.at[h], tp, n_tp, 1, *pair_of("g", h)))
        if h == 0:
            update(halves - 1)
    ready("gain_two", "fg", "fu")
    landed(s["wo_far"], sems["wo"].at[0])
    close_sends()
    for h in range(halves):
        project_second(h)
    for h in range(halves):
        activate(h)
    ready("fd")
    for h in range(halves):
        copies_h[h]()
        reduce_start(h, hidden[h].reshape(batch, units), "fd", "d")
        reduce_spread(h, "d")
    for h in range(halves):
        total = reduce_total(h, "d")
        own = gathered_two[h, tp].reshape(batch, LANES).astype(jnp.float32)
        out[:, h] = (own + total).astype(jnp.bfloat16).reshape(n_kv, rows, LANES)
    close_sends()
    for gather in second_gather:
        gather[2]()


def finish_kernel(chunks, state, out, state_to, out_to, sems):
    size = state.shape[0] // chunks
    for i in range(chunks):
        part = pl.ds(i * size, size)
        pltpu.make_async_copy(state.at[part], state_to.at[part], sems.at[0]).start()
    pltpu.make_async_copy(out, out_to, sems.at[1]).start()
    pltpu.make_async_copy(state, state_to, sems.at[0]).wait()
    pltpu.make_async_copy(out, out_to, sems.at[1]).wait()


HALVES = 2
FINISH_CHUNKS = 8
SHARED = {"f": "b", "h": "m", "squares_two": "squares"}


def fused_on_device(n_kv, n_tp, *arrays):
    (
        tokens, lengths, state, mixer_gain, wq, wk, wv, wg, wo, channel_gain, fg, fu, fd,
    ) = arrays
    columns = tokens.shape[1]
    rows = state.shape[0] // HALVES
    batch = n_kv * rows
    depth, q_width = wq.shape
    v_width, units = wv.shape[1], fg.shape[1]
    bf16, f32 = jnp.bfloat16, jnp.float32
    vmem = pl.BlockSpec(memory_space=pltpu.VMEM)
    hbm = pl.BlockSpec(memory_space=pltpu.HBM)
    chips = n_tp // CORES
    index = np.arange(QK) % (QK // 2)
    freq = jnp.asarray((10000.0 ** (-index / (QK // 2))).astype(np.float32))[None, :]
    a_width, b_width = 2 * q_width, 2 * v_width

    def buffer(*shape, dtype=bf16):
        return pltpu.VMEM((HALVES,) + shape, dtype)

    scratch = {
        "lengths": pltpu.VMEM((1, HALVES * rows), jnp.int32),
        "freq": pltpu.VMEM((1, QK), f32),
        "gain": pltpu.VMEM((1, depth), f32),
        "gain_two": pltpu.VMEM((1, depth), f32),
        "gathered": buffer(n_tp, n_kv, rows, columns),
        "gathered_two": buffer(n_tp, n_kv, rows, columns),
        "out_a": buffer(n_kv, rows, a_width),
        "out_b": buffer(n_kv, rows, b_width),
        "in_a": buffer(n_kv - 1, rows, a_width),
        "in_b": buffer(n_kv - 1, rows, b_width),
        "qk": buffer(QK, LANES, dtype=f32),
        "retained": pltpu.VMEM((HALVES * rows, v_width), f32),
        "value": pltpu.VMEM((HALVES * rows, v_width), f32),
        "merged": buffer(n_kv, rows, v_width),
        "merged_out": buffer(rows, v_width),
        "normed": pltpu.VMEM((batch, depth), bf16),
        "gate_out": buffer(n_kv, rows, units),
        "up_out": buffer(n_kv, rows, units),
        "gate_in": buffer(n_kv, rows, units),
        "up_in": buffer(n_kv, rows, units),
        "hidden_out": buffer(rows, units),
        "hidden": buffer(n_kv, rows, units),
        "squares": buffer(n_kv, 1, LANES, dtype=f32),
        "squares_two": buffer(n_kv, 1, LANES, dtype=f32),
    }
    shapes = {
        "wp": (depth, 2 * q_width + 2 * v_width), "fg": fg.shape, "fu": fu.shape,
        "wo": (CORES, wo.shape[0], chips * columns),
        "wo_far": (CORES, wo.shape[0], chips * columns),
        "fd": (CORES, fd.shape[0], chips * columns),
    }
    scratch.update({name: pltpu.VMEM(shape, bf16) for name, shape in shapes.items()})
    for tag in ("x", "d"):
        scratch["parts_" + tag] = buffer(CORES, chips, batch, columns)
        scratch["swapped_" + tag] = buffer(chips, batch, columns)
        scratch["staged_" + tag] = buffer(chips, batch, columns)
        scratch["landed_" + tag] = buffer(chips, batch, columns)
    dma = pltpu.SemaphoreType.DMA
    sems = {"load": dma((11,)), "wo": dma((2,))}
    sems["g_s"], sems["g_r"] = dma((HALVES, 2)), dma((HALVES, n_tp))
    for tag in ("x_s", "x_r", "a", "b", "m", "squares"):
        sems[tag] = dma((HALVES, 2))
    operands = (
        tokens.reshape(n_kv, HALVES, rows, columns), lengths[None, :], freq, mixer_gain[None, :],
        channel_gain[None, :], state, wq, wk, wv, wg, wo, fg, fu, fd,
    )
    out_shape = (n_kv, HALVES, rows, columns)
    out, new_state = pl.pallas_call(
        functools.partial(layer_kernel, n_kv, n_tp, depth * n_kv),
        out_shape=(pltpu.VMEM(out_shape, bf16), pltpu.VMEM(state.shape, f32)),
        in_specs=[hbm] * 14,
        out_specs=(vmem, vmem),
        scratch_shapes=[scratch, sems],
        compiler_params=pltpu.CompilerParams(
            collective_id=0, has_side_effects=True, vmem_limit_bytes=LAYER_VMEM
        ),
        name="layer",
    )(*[pltpu.with_memory_space_constraint(a, pltpu.HBM) for a in operands])
    new_state, out = pl.pallas_call(
        functools.partial(finish_kernel, FINISH_CHUNKS),
        out_shape=(
            jax.ShapeDtypeStruct(state.shape, f32),
            jax.ShapeDtypeStruct(out_shape, bf16),
        ),
        in_specs=[vmem, vmem],
        out_specs=(hbm, hbm),
        scratch_shapes=[dma((2,))],
        compiler_params=pltpu.CompilerParams(vmem_limit_bytes=FINISH_VMEM),
        name="finish",
    )(new_state, out)
    return out.reshape(tokens.shape), new_state


def fits(n_kv, n_tp, arrays):
    tokens, state, ffn_gate = arrays[0], arrays[2], arrays[10]
    rows, heads = state.shape[0], state.shape[1]
    return (
        tokens.shape[1] % LANES == 0
        and n_tp % CORES == 0
        and n_tp > CORES
        and n_kv == SIDE * SIDE
        and 4 * state.size < VMEM_TOTAL // 4
        and ffn_gate.shape[1] % LANES == 0
        and tokens.shape[1] == LANES
        and tokens.shape[0] == n_kv * rows
        and rows % (16 * HALVES) == 0
        and n_kv * rows // HALVES <= LANES
        and 2 * heads * rows == LANES
        and state.shape[2] == QK == LANES
        and state.shape[3] % LANES == 0
    )


def per_device(n_kv, n_tp, *arrays):
    if fits(n_kv, n_tp, arrays):
        return fused_on_device(n_kv, n_tp, *arrays)
    return on_device(*arrays)


def solution(mesh):
    in_specs = (
        P(None, ("kv", "tp")),
        P("kv"),
        P("kv", "tp", None, None),
        P("kv"),
        P("kv", "tp"),
        P("kv", "tp"),
        P("kv", "tp"),
        P("kv", "tp"),
        P("tp", "kv"),
        P("kv"),
        P("kv", "tp"),
        P("kv", "tp"),
        P("tp", "kv"),
    )
    out_specs = (P(None, ("kv", "tp")), P("kv", "tp", None, None))
    return jax.shard_map(
        functools.partial(per_device, mesh.shape["kv"], mesh.shape["tp"]),
        mesh=mesh, in_specs=in_specs, out_specs=out_specs, check_vma=False
    )
```

```python
import functools

import jax
import jax.numpy as jnp
import numpy as np
from jax import lax
from jax.experimental import pallas as pl
from jax.experimental.pallas import tpu as pltpu
from jax.sharding import PartitionSpec as P

D = 4096
HEADS = 16
QK = 128
LANES = 128


def rotate_heads(vectors, positions):
    half_dim = vectors.shape[-1] // 2
    frequency = 10000.0 ** (-jnp.arange(half_dim, dtype=jnp.float32) / half_dim)
    angles = positions.astype(jnp.float32)[:, None, None] * frequency
    cosine = jnp.cos(angles)
    sine_part = jnp.sin(angles)
    first_half = vectors[..., :half_dim]
    second = vectors[..., half_dim:]
    return jnp.concatenate(
        [first_half * cosine - second * sine_part, first_half * sine_part + second * cosine],
        axis=-1,
    )


def gathered_rows(columns):
    return lax.all_gather(columns, "tp", axis=1, tiled=True)


def owned_sums(partial_value, squares):
    raw_sums, totals = (
        lax.psum_scatter(
            partial_value.astype(jnp.bfloat16), "kv", scatter_dimension=0, tiled=True
        ).astype(jnp.float32),
        lax.psum_scatter(
            squares.astype(jnp.bfloat16), "kv", scatter_dimension=0, tiled=True
        ).astype(jnp.float32),
    )
    summed = raw_sums * lax.rsqrt(totals / D + 1e-06)[:, None]
    return summed


def every_sum(partial_value, squares):
    raw_sums, totals = (
        lax.psum(partial_value.astype(jnp.bfloat16), "kv").astype(jnp.float32),
        lax.psum(squares.astype(jnp.bfloat16), "kv").astype(jnp.float32),
    )
    summed = raw_sums * lax.rsqrt(totals / D + 1e-06)[:, None]
    return summed


def on_device(
    tokens,
    lengths,
    retention_state,
    mixer_gain,
    query_weight,
    key_weight,
    value_weight,
    gate_weight,
    output_weight,
    channel_gain,
    ffn_gate,
    ffn_up,
    ffn_down,
):
    feature_block = gathered_rows(tokens).astype(jnp.float32)
    squares = jnp.sum(feature_block * feature_block, axis=1)
    normed = (feature_block * mixer_gain).astype(jnp.bfloat16)
    partial_value = jnp.concatenate(
        [
            jnp.dot(normed, query_weight, preferred_element_type=jnp.float32),
            jnp.dot(normed, key_weight, preferred_element_type=jnp.float32),
            jnp.dot(normed, value_weight, preferred_element_type=jnp.float32),
            jnp.dot(normed, gate_weight, preferred_element_type=jnp.float32),
        ],
        axis=1,
    )
    owned_rows = owned_sums(partial_value, squares)
    local_heads = query_weight.shape[1] // QK
    q_width = query_weight.shape[1]
    v_width = value_weight.shape[1]
    head_width = v_width // local_heads
    seq_rows = owned_rows.shape[0]
    query_rows = rotate_heads(
        owned_rows[:, :q_width].reshape(seq_rows, local_heads, QK), lengths
    ).astype(jnp.bfloat16)
    key_rows = (
        rotate_heads(
            owned_rows[:, q_width : 2 * q_width].reshape(seq_rows, local_heads, QK), lengths
        )
        * QK ** (-0.5)
    ).astype(jnp.bfloat16)
    value_rows = (
        owned_rows[:, 2 * q_width : 2 * q_width + v_width]
        .astype(jnp.bfloat16)
        .reshape(seq_rows, local_heads, head_width)
    )
    gate_rows = owned_rows[:, 2 * q_width + v_width :]
    head_ids = (lax.axis_index("tp") * local_heads + jnp.arange(local_heads)).astype(jnp.float32)
    decay_rate = 1.0 - 2.0 ** (-5.0 - 10.0 * head_ids / (HEADS - 1))
    new_state = (
        decay_rate[None, :, None, None] * retention_state
        + key_rows.astype(jnp.float32)[..., :, None] * value_rows.astype(jnp.float32)[..., None, :]
    )
    retained = jnp.einsum(
        "bhk,bhkv->bhv", query_rows.astype(jnp.float32), new_state, precision=lax.Precision.HIGHEST
    )
    normalized = retained * lax.rsqrt(jnp.mean(retained * retained, axis=-1) + 1e-06)[..., None]
    merged = (normalized.reshape(seq_rows, v_width) * jax.nn.silu(gate_rows)).astype(jnp.bfloat16)
    mixed_part = jnp.dot(
        lax.all_gather(merged, "kv", axis=0, tiled=True),
        output_weight,
        preferred_element_type=jnp.float32,
    )
    mixed_cols = lax.psum_scatter(
        mixed_part.astype(jnp.bfloat16), "tp", scatter_dimension=1, tiled=True
    ).astype(jnp.float32)
    residual = (tokens.astype(jnp.float32) + mixed_cols).astype(jnp.bfloat16)
    block_two = gathered_rows(residual).astype(jnp.float32)
    squares_two = jnp.sum(block_two * block_two, axis=1)
    normed_two = (block_two * channel_gain).astype(jnp.bfloat16)
    partial_two = jnp.concatenate(
        [
            jnp.dot(normed_two, ffn_gate, preferred_element_type=jnp.float32),
            jnp.dot(normed_two, ffn_up, preferred_element_type=jnp.float32),
        ],
        axis=1,
    )
    hidden_units = ffn_gate.shape[1]
    summed = every_sum(partial_two, squares_two)
    hidden = (jax.nn.silu(summed[:, :hidden_units]) * summed[:, hidden_units:]).astype(jnp.bfloat16)
    down_part = jnp.dot(hidden, ffn_down, preferred_element_type=jnp.float32)
    down_sums = lax.psum_scatter(
        down_part.astype(jnp.bfloat16), "tp", scatter_dimension=1, tiled=True
    ).astype(jnp.float32)
    layer_output = (residual.astype(jnp.float32) + down_sums).astype(jnp.bfloat16)
    return (layer_output, new_state)


MESH_ID = pl.DeviceIdType.MESH
VMEM_TOTAL = 67043328
CORES = 2
SIDE = 2
LAYER_VMEM = 50000000
FINISH_VMEM = 20000000


def greet(devices):
    barrier = pltpu.get_barrier_semaphore()
    for device in devices:
        pl.semaphore_signal(barrier, inc=1, device_id=device, device_id_type=MESH_ID)
    pl.semaphore_wait(barrier, len(devices))


def kv_peers(kv, n_kv):
    return [n_kv - 1 - kv, kv + 1 - 2 * lax.rem(kv, SIDE), lax.rem(kv + SIDE, n_kv)]


def send_all(devices, source, target, send_sem, recv_sem):
    for k, device in enumerate(devices):
        remote_to(device, source(device["kv"]), target(k), send_sem, recv_sem).start()


def landed(ref, sem):
    pltpu.make_async_copy(ref, ref, sem).wait()


def load_all(pairs, sem):
    for source, target in pairs:
        pltpu.make_async_copy(source, target, sem).start()


def silu(value):
    return value / (1.0 + jnp.exp(-value))


def as_row(column):
    lane = lax.broadcasted_iota(jnp.int32, (column.shape[0], LANES), 1)
    row = lax.broadcasted_iota(jnp.int32, (column.shape[0], LANES), 0)
    return jnp.sum(jnp.where(row == lane, column, 0.0), axis=0, keepdims=True)


def as_column(row_values, first, rows):
    lane = lax.broadcasted_iota(jnp.int32, (rows, LANES), 1)
    row = lax.broadcasted_iota(jnp.int32, (rows, LANES), 0)
    return jnp.sum(jnp.where(row + first == lane, row_values, 0.0), axis=1, keepdims=True)


def remote(axis, peer, source, target, send_sem, recv_sem):
    return remote_to({axis: peer}, source, target, send_sem, recv_sem)


def remote_to(device, source, target, send_sem, recv_sem):
    return pltpu.make_async_remote_copy(
        src_ref=source, dst_ref=target, send_sem=send_sem, recv_sem=recv_sem,
        device_id=device, device_id_type=MESH_ID,
    )


def far_first(chip, chips):
    def ascending(at, k):
        return k + 1 - (at + chips - 1 - k) // chips

    low = 1 - chip // (chips // 2)
    mirrored = chips - 1 - chip
    return [
        low * (chips - 1 - ascending(mirrored, k)) + (1 - low) * ascending(chip, k)
        for k in range(chips - 1)
    ]


def start_gather(slots, tp, n_tp, hub, send_sems, recv_sems):
    chips = n_tp // CORES
    chip, core = tp // CORES, lax.rem(tp, CORES)
    partner = chip * CORES + 1 - core
    order = far_first(chip, chips)

    def block(peer, slot, send):
        return remote("tp", peer, slots.at[slot], slots.at[slot], send_sems.at[send], recv_sems.at[slot])

    for peer in order:
        block(peer * CORES + hub, tp, 0).start()
    block(partner, tp, 0).start()
    relayed = [
        block(partner, source * CORES + side, 1) for source in order[::-1] for side in range(CORES)
    ]

    def take(first, last):
        for copy in relayed[first * CORES : last * CORES]:
            copy.wait_recv()

            @pl.when(core == hub)
            def _():
                copy.start()

    def take_own():
        block(partner, partner, 0).wait_recv()

    def close():
        landed(slots.at[:chips], send_sems.at[0])

        @pl.when(core == hub)
        def _():
            landed(slots.at[: len(relayed)], send_sems.at[1])

    return take, take_own, close, order[::-1]


def start_reduce(lhs, weight, parts, swapped, tp, send_sems, recv_sems):
    chip, core = tp // CORES, lax.rem(tp, CORES)
    chips, columns = parts.shape[1], parts.shape[3]

    def multiply(side):
        full = jnp.dot(lhs, weight[side], preferred_element_type=jnp.float32).astype(jnp.bfloat16)
        for z in range(chips):
            parts[side, z] = full[:, z * columns : (z + 1) * columns]

    multiply(core)
    remote(
        "tp", chip * CORES + 1 - core, parts.at[core], swapped, send_sems.at[0], recv_sems.at[0]
    ).start()
    multiply(1 - core)


def spread_pairs(parts, swapped, staged, into, tp, send_sems, recv_sems):
    chips = parts.shape[1]
    chip, core = tp // CORES, lax.rem(tp, CORES)
    landed(swapped, recv_sems.at[0])
    for k, other in enumerate(far_first(chip, chips) + [chip]):
        pair = parts[1 - core, other].astype(jnp.float32) + swapped[other].astype(jnp.float32)
        staged[k] = pair.astype(jnp.bfloat16)
        remote(
            "tp", other * CORES + 1 - core, staged.at[k], into.at[chip], send_sems.at[1], recv_sems.at[1]
        ).start()


def total_of(own, others):
    total = own.astype(jnp.float32)
    for step in range(others.shape[0]):
        total += others[step].astype(jnp.float32)
    return total


def layer_kernel(
    n_kv, n_tp, features,
    tokens_hbm, lengths_hbm, freq_hbm, gain_hbm, gain_two_hbm, state_hbm,
    wq_hbm, wk_hbm, wv_hbm, wg_hbm, wo_hbm, fg_hbm, fu_hbm, fd_hbm,
    out, state, s, sems,
):
    kv, tp = lax.axis_index("kv"), lax.axis_index("tp")
    chips = n_tp // CORES
    chip, core = tp // CORES, lax.rem(tp, CORES)
    gathered, gathered_two, merged, hidden = s["gathered"], s["gathered_two"], s["merged"], s["hidden"]
    halves, rows = gathered.shape[0], gathered.shape[3]
    batch = n_kv * rows
    q_width, v_width = wq_hbm.shape[1], wv_hbm.shape[1]
    units, columns = fg_hbm.shape[1], tokens_hbm.shape[3]

    def sides(ref, target):
        return [
            (
                ref.at[:, (z * CORES + side) * columns : (z * CORES + side + 1) * columns],
                target.at[side, :, z * columns : (z + 1) * columns],
            )
            for side in range(CORES)
            for z in range(chips)
        ]

    groups = {
        "tokens": [(tokens_hbm.at[:, h], gathered.at[h, tp]) for h in range(halves)],
        "lengths": [(lengths_hbm, s["lengths"])],
        "freq": [(freq_hbm, s["freq"])],
        "gain": [(gain_hbm, s["gain"])],
        "wp": [
            (wq_hbm, s["wp"].at[:, :q_width]),
            (wk_hbm, s["wp"].at[:, q_width : 2 * q_width]),
            (wv_hbm, s["wp"].at[:, 2 * q_width : 2 * q_width + v_width]),
            (wg_hbm, s["wp"].at[:, 2 * q_width + v_width :]),
        ],
        "state": [(state_hbm, state)],
        "wo": sides(wo_hbm, s["wo"]),
        "gain_two": [(gain_two_hbm, s["gain_two"])],
        "fg": [(fg_hbm, s["fg"])],
        "fu": [(fu_hbm, s["fu"])],
        "fd": sides(fd_hbm, s["fd"]),
    }
    wholes = {
        "tokens": gathered.at[:, tp], "wp": s["wp"], "state": state, "wo": s["wo"], "fd": s["fd"],
        "lengths": s["lengths"], "freq": s["freq"], "gain": s["gain"],
        "gain_two": s["gain_two"], "fg": s["fg"], "fu": s["fu"],
    }
    pending = {}
    for i, (name, group) in enumerate(groups.items()):
        pending[name] = i
        load_all(group, sems["load"].at[i])

    def ready(*wanted):
        for name in wanted:
            if name in pending:
                landed(wholes[name], sems["load"].at[pending.pop(name)])

    partner = chip * CORES + 1 - core
    peers = [{"kv": peer, "tp": tp} for peer in kv_peers(kv, n_kv)]
    crossed = [{"kv": peer, "tp": partner} for peer in kv_peers(kv, n_kv)]
    along = [{"kv": kv, "tp": other * CORES + 1 - core} for other in far_first(chip, chips)]
    beside = {"kv": kv, "tp": partner}
    crossed_all = crossed + [beside]
    aside = [{"kv": kv, "tp": other * CORES + core} for other in far_first(chip, chips)]
    greet(along + aside + [beside] + peers + crossed)
    closing = []

    def close_sends():
        for extent, sem in closing:
            landed(extent, sem)
        closing.clear()

    def pair_of(name, h):
        return sems[name + "_s"].at[h], sems[name + "_r"].at[h]

    def kv_send(name, h, devices, source, target, extent):
        send_sem, recv_sem = sems[SHARED.get(name, name)].at[h, 0], sems[SHARED.get(name, name)].at[h, 1]
        send_all(devices, source, target, send_sem, recv_sem)
        closing.append((extent, send_sem))
        return lambda: landed(extent, recv_sem)

    def send_squares(name, h, devices):
        return kv_send(
            name, h, devices, lambda p: s[name].at[h, n_kv - 1], lambda n: s[name].at[h, n], s[name].at[h, : n_kv - 1]
        )

    def scale_of(name, h, wait):
        wait()
        total = s[name][h, 0]
        for n in range(1, n_kv):
            total += s[name][h, n]
        return lax.rsqrt(as_column(total, kv * rows, rows) / features + 1e-06)

    ready("tokens")
    first_gather = [start_gather(gathered.at[0], tp, n_tp, 0, *pair_of("g", 0))]
    ready("lengths", "freq", "gain")
    def gathered_product(gather, slots, gains, weight, between=None):
        take, take_own, _, near = gather
        span = CORES * columns

        def chunk(source):
            at = pl.multiple_of(source * span, span)
            x = jnp.concatenate(
                [slots[source * CORES + side].reshape(batch, columns) for side in range(CORES)], axis=1
            ).astype(jnp.float32)
            part = (x * gains[:, pl.ds(at, span)]).astype(jnp.bfloat16)
            s["normed"][:, pl.ds(at, span)] = part
            product = jnp.dot(part, weight[pl.ds(at, span), :], preferred_element_type=jnp.float32)
            return product, jnp.sum(x * x, axis=1, keepdims=True)

        take_own()
        product, squares = chunk(chip)
        if between is not None:
            between()
        for k, source in enumerate(near):
            take(k, k + 1)
            more, more_squares = chunk(source)
            product += more
            squares += more_squares
        return product.astype(jnp.bfloat16).reshape(n_kv, rows, product.shape[1]), as_row(squares)

    def project(weight):
        full = jnp.dot(s["normed"][...], weight[...], preferred_element_type=jnp.float32)
        return full.astype(jnp.bfloat16).reshape(n_kv, rows, full.shape[1])

    heads = q_width // QK
    width = v_width // heads
    out_a, out_b, in_a, in_b = s["out_a"], s["out_b"], s["in_a"], s["in_b"]
    first, second, copies_m, copies_q = [], [], [], []

    angles_of = []

    def find_angles():
        all_rows = halves * rows
        row = lax.broadcasted_iota(jnp.int32, (all_rows, all_rows), 0)
        col = lax.broadcasted_iota(jnp.int32, (all_rows, all_rows), 1)
        spread = jnp.where(row == col, s["lengths"][...].astype(jnp.float32), 0.0)
        angles = jnp.sum(spread, axis=1, keepdims=True) * s["freq"][...]
        cosine, sine = jnp.cos(angles), jnp.sin(angles)
        lane = lax.broadcasted_iota(jnp.int32, angles.shape, 1)
        sine = jnp.where(lane < QK // 2, -sine, sine)
        angles_of.extend([cosine, sine])

    def start_next_gather(h):
        if h == 1:
            find_angles()
        if h < halves:
            first_gather.append(start_gather(gathered.at[h], tp, n_tp, 0, *pair_of("g", h)))

    def project_first(h):
        product, s["squares"][h, n_kv - 1] = gathered_product(
            first_gather[h], gathered.at[h], s["gain"], s["wp"], lambda: start_next_gather(h + 1)
        )
        out_a[h] = product[:, :, : 2 * q_width]
        out_b[h] = product[:, :, 2 * q_width :]
        first.append(kv_send("a", h, peers, lambda p: out_a.at[h, p], lambda n: in_a.at[h, n], in_a.at[h]))
        copies_q.append(send_squares("squares", h, peers))
        second.append(kv_send("b", h, peers, lambda p: out_b.at[h, p], lambda n: in_b.at[h, n], in_b.at[h]))

    decays = []
    for head in range(heads):
        number = jnp.full((1, width), tp * heads + head, jnp.int32).astype(jnp.float32)
        decays.append(1.0 - jnp.exp2(-5.0 - 10.0 * number / (heads * n_tp - 1)))
    qk, value, retained = s["qk"], s["value"], s["retained"]

    def attend(h):
        base = h * rows
        first[h]()
        total = total_of(out_a[h, kv], in_a.at[h])
        scale = scale_of("squares", h, copies_q[h])
        total = total * scale
        cosines, sines = [table[base : base + rows] for table in angles_of]
        blocks = []
        for start, factor in ((0, 1.0), (q_width, QK ** (-0.5))):
            for head in range(heads):
                part = total[:, start + head * QK : start + (head + 1) * QK]
                turned = (part * cosines + pltpu.roll(part, QK // 2, 1) * sines) * factor
                blocks.append(turned.astype(jnp.bfloat16).astype(jnp.float32))
        columns = jnp.concatenate(blocks * (LANES // (len(blocks) * rows)), axis=0).T
        qk[h] = columns
        for i in range(rows):
            for head in range(heads):
                query = columns[:, head * rows + i : head * rows + i + 1]
                retained[base + i : base + i + 1, head * width : (head + 1) * width] = jnp.sum(
                    query * state[base + i, head], axis=0, keepdims=True
                )
        second[h]()
        total = total_of(out_b[h, kv], in_b.at[h]) * scale
        values = total[:, :v_width].astype(jnp.bfloat16).astype(jnp.float32)
        value[base : base + rows] = values
        pieces = []
        for head in range(heads):
            overlap = jnp.sum(blocks[head] * blocks[heads + head], axis=1, keepdims=True)
            span = slice(head * width, (head + 1) * width)
            piece = decays[head] * retained[base : base + rows, span] + overlap * values[:, span]
            pieces.append(piece * lax.rsqrt(jnp.mean(piece * piece, axis=1, keepdims=True) + 1e-06))
        s["merged_out"][h] = (jnp.concatenate(pieces, axis=1) * silu(total[:, v_width:])).astype(jnp.bfloat16)
        copies_m.append(
            kv_send("m", h, crossed_all, lambda p: s["merged_out"].at[h], lambda n: merged.at[h, kv], merged.at[h])
        )

    block = 8

    def update(h):
        base = h * rows

        def update_step(i, carry):
            start = i * block
            turned = pltpu.roll(qk[h], lax.rem(LANES - start, LANES), 1)
            for n in range(block):
                for head in range(heads):
                    lane = (heads + head) * rows + n
                    at = base + start + n
                    outer = turned[:, lane : lane + 1] * value[pl.ds(at, 1), head * width : (head + 1) * width]
                    state[at, head] = decays[head] * state[at, head] + outer
            return carry

        lax.fori_loop(0, rows // block, update_step, 0)

    def reduce_start(h, lhs, weight, tag):
        start_reduce(lhs, s[weight], s["parts_" + tag].at[h], s["swapped_" + tag].at[h], tp, *pair_of("x", h))

    def reduce_spread(h, tag):
        swapped, staged = s["swapped_" + tag].at[h], s["staged_" + tag].at[h]
        send_sems, recv_sems = pair_of("x", h)
        spread_pairs(s["parts_" + tag].at[h], swapped, staged, s["landed_" + tag].at[h], tp, send_sems, recv_sems)
        closing.extend([(swapped, send_sems.at[0]), (staged, send_sems.at[1])])

    def reduce_total(h, tag):
        into = s["landed_" + tag].at[h]
        landed(into, pair_of("x", h)[1].at[1])
        return total_of(into[0], into.at[1:])

    gate_out, up_out, gate_in, up_in = s["gate_out"], s["up_out"], s["gate_in"], s["up_in"]
    copies_e, copies_f, copies_h, copies_u = [], [], [], []
    first_units = (units // LANES + 1) // 2 * LANES

    def project_second(h):
        for span in (slice(0, first_units), slice(first_units, units)):
            if span.start == 0:
                gate_out[h, :, :, span], s["squares_two"][h, n_kv - 1] = gathered_product(
                    second_gather[h], gathered_two.at[h], s["gain_two"], s["fg"].at[:, span]
                )
            else:
                gate_out[h, :, :, span] = project(s["fg"].at[:, span])
            send_all(
                crossed_all, lambda p: gate_out.at[h, p, :, span], lambda n: gate_in.at[h, n, :, span],
                sems["a"].at[h, 0], sems["a"].at[h, 1],
            )
            if span.start == 0:
                copies_u.append(send_squares("squares_two", h, crossed))
        closing.append((gate_in.at[h], sems["a"].at[h, 0]))
        copies_e.append(lambda: landed(gate_in.at[h], sems["a"].at[h, 1]))
        up_out[h] = project(s["fu"])
        copies_f.append(
            kv_send("f", h, crossed_all, lambda p: up_out.at[h, p], lambda n: up_in.at[h, n], up_in.at[h])
        )

    def activate(h):
        copies_e[h]()
        total = total_of(gate_in[h, 0], gate_in.at[h, 1:])
        scale = scale_of("squares_two", h, copies_u[h])
        activated = silu(total * scale)
        copies_f[h]()
        up = total_of(up_in[h, 0], up_in.at[h, 1:]) * scale
        s["hidden_out"][h] = (activated * up).astype(jnp.bfloat16)
        copies_h.append(
            kv_send("h", h, crossed_all, lambda p: s["hidden_out"].at[h], lambda n: hidden.at[h, kv], hidden.at[h])
        )

    second_gather = []
    ready("wp")
    project_first(0)
    ready("wo")
    remote_to(beside, s["wo"], s["wo_far"], sems["wo"].at[0], sems["wo"].at[1]).start()
    for h in range(1, halves):
        project_first(h)
    ready("state")
    for h in range(halves):
        attend(h)
    landed(s["wo_far"], sems["wo"].at[1])
    for h in range(halves):
        copies_m[h]()
        reduce_start(h, merged[h].reshape(batch, v_width), "wo_far", "x")
        reduce_spread(h, "x")
    for h in range(halves - 1):
        update(h)
    for gather in first_gather:
        gather[2]()
    for h in range(halves):
        total = reduce_total(h, "x")
        own = gathered[h, tp].reshape(batch, LANES).astype(jnp.float32)
        gathered_two[h, tp] = (own + total).astype(jnp.bfloat16).reshape(n_kv, rows, LANES)
        second_gather.append(start_gather(gathered_two.at[h], tp, n_tp, 1, *pair_of("g", h)))
        if h == 0:
            update(halves - 1)
    ready("gain_two", "fg", "fu")
    landed(s["wo_far"], sems["wo"].at[0])
    close_sends()
    for h in range(halves):
        project_second(h)
    for h in range(halves):
        activate(h)
    ready("fd")
    for h in range(halves):
        copies_h[h]()
        reduce_start(h, hidden[h].reshape(batch, units), "fd", "d")
        reduce_spread(h, "d")
    for h in range(halves):
        total = reduce_total(h, "d")
        own = gathered_two[h, tp].reshape(batch, LANES).astype(jnp.float32)
        out[:, h] = (own + total).astype(jnp.bfloat16).reshape(n_kv, rows, LANES)
    close_sends()
    for gather in second_gather:
        gather[2]()


def finish_kernel(chunks, state, out, state_to, out_to, sems):
    size = state.shape[0] // chunks
    for i in range(chunks):
        part = pl.ds(i * size, size)
        pltpu.make_async_copy(state.at[part], state_to.at[part], sems.at[0]).start()
    pltpu.make_async_copy(out, out_to, sems.at[1]).start()
    pltpu.make_async_copy(state, state_to, sems.at[0]).wait()
    pltpu.make_async_copy(out, out_to, sems.at[1]).wait()


HALVES = 2
FINISH_CHUNKS = 16
SHARED = {"f": "b", "h": "m", "squares_two": "squares"}


def fused_on_device(n_kv, n_tp, *arrays):
    (
        tokens, lengths, state, mixer_gain, wq, wk, wv, wg, wo, channel_gain, fg, fu, fd,
    ) = arrays
    columns = tokens.shape[1]
    rows = state.shape[0] // HALVES
    batch = n_kv * rows
    depth, q_width = wq.shape
    v_width, units = wv.shape[1], fg.shape[1]
    bf16, f32 = jnp.bfloat16, jnp.float32
    vmem = pl.BlockSpec(memory_space=pltpu.VMEM)
    hbm = pl.BlockSpec(memory_space=pltpu.HBM)
    chips = n_tp // CORES
    index = np.arange(QK) % (QK // 2)
    freq = jnp.asarray((10000.0 ** (-index / (QK // 2))).astype(np.float32))[None, :]
    a_width, b_width = 2 * q_width, 2 * v_width

    def buffer(*shape, dtype=bf16):
        return pltpu.VMEM((HALVES,) + shape, dtype)

    scratch = {
        "lengths": pltpu.VMEM((1, HALVES * rows), jnp.int32),
        "freq": pltpu.VMEM((1, QK), f32),
        "gain": pltpu.VMEM((1, depth), f32),
        "gain_two": pltpu.VMEM((1, depth), f32),
        "gathered": buffer(n_tp, n_kv, rows, columns),
        "gathered_two": buffer(n_tp, n_kv, rows, columns),
        "out_a": buffer(n_kv, rows, a_width),
        "out_b": buffer(n_kv, rows, b_width),
        "in_a": buffer(n_kv - 1, rows, a_width),
        "in_b": buffer(n_kv - 1, rows, b_width),
        "qk": buffer(QK, LANES, dtype=f32),
        "retained": pltpu.VMEM((HALVES * rows, v_width), f32),
        "value": pltpu.VMEM((HALVES * rows, v_width), f32),
        "merged": buffer(n_kv, rows, v_width),
        "merged_out": buffer(rows, v_width),
        "normed": pltpu.VMEM((batch, depth), bf16),
        "gate_out": buffer(n_kv, rows, units),
        "up_out": buffer(n_kv, rows, units),
        "gate_in": buffer(n_kv, rows, units),
        "up_in": buffer(n_kv, rows, units),
        "hidden_out": buffer(rows, units),
        "hidden": buffer(n_kv, rows, units),
        "squares": buffer(n_kv, 1, LANES, dtype=f32),
        "squares_two": buffer(n_kv, 1, LANES, dtype=f32),
    }
    shapes = {
        "wp": (depth, 2 * q_width + 2 * v_width), "fg": fg.shape, "fu": fu.shape,
        "wo": (CORES, wo.shape[0], chips * columns),
        "wo_far": (CORES, wo.shape[0], chips * columns),
        "fd": (CORES, fd.shape[0], chips * columns),
    }
    scratch.update({name: pltpu.VMEM(shape, bf16) for name, shape in shapes.items()})
    for tag in ("x", "d"):
        scratch["parts_" + tag] = buffer(CORES, chips, batch, columns)
        scratch["swapped_" + tag] = buffer(chips, batch, columns)
        scratch["staged_" + tag] = buffer(chips, batch, columns)
        scratch["landed_" + tag] = buffer(chips, batch, columns)
    dma = pltpu.SemaphoreType.DMA
    sems = {"load": dma((11,)), "wo": dma((2,))}
    sems["g_s"], sems["g_r"] = dma((HALVES, 2)), dma((HALVES, n_tp))
    for tag in ("x_s", "x_r", "a", "b", "m", "squares"):
        sems[tag] = dma((HALVES, 2))
    operands = (
        tokens.reshape(n_kv, HALVES, rows, columns), lengths[None, :], freq, mixer_gain[None, :],
        channel_gain[None, :], state, wq, wk, wv, wg, wo, fg, fu, fd,
    )
    out_shape = (n_kv, HALVES, rows, columns)
    out, new_state = pl.pallas_call(
        functools.partial(layer_kernel, n_kv, n_tp, depth * n_kv),
        out_shape=(pltpu.VMEM(out_shape, bf16), pltpu.VMEM(state.shape, f32)),
        in_specs=[hbm] * 14,
        out_specs=(vmem, vmem),
        scratch_shapes=[scratch, sems],
        compiler_params=pltpu.CompilerParams(
            collective_id=0, has_side_effects=True, vmem_limit_bytes=LAYER_VMEM
        ),
        name="layer",
    )(*[pltpu.with_memory_space_constraint(a, pltpu.HBM) for a in operands])
    new_state, out = pl.pallas_call(
        functools.partial(finish_kernel, FINISH_CHUNKS),
        out_shape=(
            jax.ShapeDtypeStruct(state.shape, f32),
            jax.ShapeDtypeStruct(out_shape, bf16),
        ),
        in_specs=[vmem, vmem],
        out_specs=(hbm, hbm),
        scratch_shapes=[dma((2,))],
        compiler_params=pltpu.CompilerParams(vmem_limit_bytes=FINISH_VMEM),
        name="finish",
    )(new_state, out)
    return out.reshape(tokens.shape), new_state


def fits(n_kv, n_tp, arrays):
    tokens, state, ffn_gate = arrays[0], arrays[2], arrays[10]
    rows, heads = state.shape[0], state.shape[1]
    return (
        tokens.shape[1] % LANES == 0
        and n_tp % CORES == 0
        and n_tp > CORES
        and n_kv == SIDE * SIDE
        and 4 * state.size < VMEM_TOTAL // 4
        and ffn_gate.shape[1] % LANES == 0
        and tokens.shape[1] == LANES
        and tokens.shape[0] == n_kv * rows
        and rows % (16 * HALVES) == 0
        and n_kv * rows // HALVES <= LANES
        and 2 * heads * rows == LANES
        and state.shape[2] == QK == LANES
        and state.shape[3] % LANES == 0
    )


def per_device(n_kv, n_tp, *arrays):
    if fits(n_kv, n_tp, arrays):
        return fused_on_device(n_kv, n_tp, *arrays)
    return on_device(*arrays)


def solution(mesh):
    in_specs = (
        P(None, ("kv", "tp")),
        P("kv"),
        P("kv", "tp", None, None),
        P("kv"),
        P("kv", "tp"),
        P("kv", "tp"),
        P("kv", "tp"),
        P("kv", "tp"),
        P("tp", "kv"),
        P("kv"),
        P("kv", "tp"),
        P("kv", "tp"),
        P("tp", "kv"),
    )
    out_specs = (P(None, ("kv", "tp")), P("kv", "tp", None, None))
    return jax.shard_map(
        functools.partial(per_device, mesh.shape["kv"], mesh.shape["tp"]),
        mesh=mesh, in_specs=in_specs, out_specs=out_specs, check_vma=False
    )
```

```python
import functools

import jax
import jax.numpy as jnp
import numpy as np
from jax import lax
from jax.experimental import pallas as pl
from jax.experimental.pallas import tpu as pltpu
from jax.sharding import PartitionSpec as P

D = 4096
HEADS = 16
QK = 128
LANES = 128


def rotate_heads(vectors, positions):
    half_dim = vectors.shape[-1] // 2
    frequency = 10000.0 ** (-jnp.arange(half_dim, dtype=jnp.float32) / half_dim)
    angles = positions.astype(jnp.float32)[:, None, None] * frequency
    cosine = jnp.cos(angles)
    sine_part = jnp.sin(angles)
    first_half = vectors[..., :half_dim]
    second = vectors[..., half_dim:]
    return jnp.concatenate(
        [first_half * cosine - second * sine_part, first_half * sine_part + second * cosine],
        axis=-1,
    )


def gathered_rows(columns):
    return lax.all_gather(columns, "tp", axis=1, tiled=True)


def owned_sums(partial_value, squares):
    raw_sums, totals = (
        lax.psum_scatter(
            partial_value.astype(jnp.bfloat16), "kv", scatter_dimension=0, tiled=True
        ).astype(jnp.float32),
        lax.psum_scatter(
            squares.astype(jnp.bfloat16), "kv", scatter_dimension=0, tiled=True
        ).astype(jnp.float32),
    )
    summed = raw_sums * lax.rsqrt(totals / D + 1e-06)[:, None]
    return summed


def every_sum(partial_value, squares):
    raw_sums, totals = (
        lax.psum(partial_value.astype(jnp.bfloat16), "kv").astype(jnp.float32),
        lax.psum(squares.astype(jnp.bfloat16), "kv").astype(jnp.float32),
    )
    summed = raw_sums * lax.rsqrt(totals / D + 1e-06)[:, None]
    return summed


def on_device(
    tokens,
    lengths,
    retention_state,
    mixer_gain,
    query_weight,
    key_weight,
    value_weight,
    gate_weight,
    output_weight,
    channel_gain,
    ffn_gate,
    ffn_up,
    ffn_down,
):
    feature_block = gathered_rows(tokens).astype(jnp.float32)
    squares = jnp.sum(feature_block * feature_block, axis=1)
    normed = (feature_block * mixer_gain).astype(jnp.bfloat16)
    partial_value = jnp.concatenate(
        [
            jnp.dot(normed, query_weight, preferred_element_type=jnp.float32),
            jnp.dot(normed, key_weight, preferred_element_type=jnp.float32),
            jnp.dot(normed, value_weight, preferred_element_type=jnp.float32),
            jnp.dot(normed, gate_weight, preferred_element_type=jnp.float32),
        ],
        axis=1,
    )
    owned_rows = owned_sums(partial_value, squares)
    local_heads = query_weight.shape[1] // QK
    q_width = query_weight.shape[1]
    v_width = value_weight.shape[1]
    head_width = v_width // local_heads
    seq_rows = owned_rows.shape[0]
    query_rows = rotate_heads(
        owned_rows[:, :q_width].reshape(seq_rows, local_heads, QK), lengths
    ).astype(jnp.bfloat16)
    key_rows = (
        rotate_heads(
            owned_rows[:, q_width : 2 * q_width].reshape(seq_rows, local_heads, QK), lengths
        )
        * QK ** (-0.5)
    ).astype(jnp.bfloat16)
    value_rows = (
        owned_rows[:, 2 * q_width : 2 * q_width + v_width]
        .astype(jnp.bfloat16)
        .reshape(seq_rows, local_heads, head_width)
    )
    gate_rows = owned_rows[:, 2 * q_width + v_width :]
    head_ids = (lax.axis_index("tp") * local_heads + jnp.arange(local_heads)).astype(jnp.float32)
    decay_rate = 1.0 - 2.0 ** (-5.0 - 10.0 * head_ids / (HEADS - 1))
    new_state = (
        decay_rate[None, :, None, None] * retention_state
        + key_rows.astype(jnp.float32)[..., :, None] * value_rows.astype(jnp.float32)[..., None, :]
    )
    retained = jnp.einsum(
        "bhk,bhkv->bhv", query_rows.astype(jnp.float32), new_state, precision=lax.Precision.HIGHEST
    )
    normalized = retained * lax.rsqrt(jnp.mean(retained * retained, axis=-1) + 1e-06)[..., None]
    merged = (normalized.reshape(seq_rows, v_width) * jax.nn.silu(gate_rows)).astype(jnp.bfloat16)
    mixed_part = jnp.dot(
        lax.all_gather(merged, "kv", axis=0, tiled=True),
        output_weight,
        preferred_element_type=jnp.float32,
    )
    mixed_cols = lax.psum_scatter(
        mixed_part.astype(jnp.bfloat16), "tp", scatter_dimension=1, tiled=True
    ).astype(jnp.float32)
    residual = (tokens.astype(jnp.float32) + mixed_cols).astype(jnp.bfloat16)
    block_two = gathered_rows(residual).astype(jnp.float32)
    squares_two = jnp.sum(block_two * block_two, axis=1)
    normed_two = (block_two * channel_gain).astype(jnp.bfloat16)
    partial_two = jnp.concatenate(
        [
            jnp.dot(normed_two, ffn_gate, preferred_element_type=jnp.float32),
            jnp.dot(normed_two, ffn_up, preferred_element_type=jnp.float32),
        ],
        axis=1,
    )
    hidden_units = ffn_gate.shape[1]
    summed = every_sum(partial_two, squares_two)
    hidden = (jax.nn.silu(summed[:, :hidden_units]) * summed[:, hidden_units:]).astype(jnp.bfloat16)
    down_part = jnp.dot(hidden, ffn_down, preferred_element_type=jnp.float32)
    down_sums = lax.psum_scatter(
        down_part.astype(jnp.bfloat16), "tp", scatter_dimension=1, tiled=True
    ).astype(jnp.float32)
    layer_output = (residual.astype(jnp.float32) + down_sums).astype(jnp.bfloat16)
    return (layer_output, new_state)


MESH_ID = pl.DeviceIdType.MESH
VMEM_TOTAL = 67043328
CORES = 2
SIDE = 2
LAYER_VMEM = 50000000
FINISH_VMEM = 20000000


def greet(devices):
    barrier = pltpu.get_barrier_semaphore()
    for device in devices:
        pl.semaphore_signal(barrier, inc=1, device_id=device, device_id_type=MESH_ID)
    pl.semaphore_wait(barrier, len(devices))


def kv_peers(kv, n_kv):
    return [n_kv - 1 - kv, kv + 1 - 2 * lax.rem(kv, SIDE), lax.rem(kv + SIDE, n_kv)]


def send_all(devices, source, target, send_sem, recv_sem):
    for k, device in enumerate(devices):
        remote_to(device, source(device["kv"]), target(k), send_sem, recv_sem).start()


def landed(ref, sem):
    pltpu.make_async_copy(ref, ref, sem).wait()


def load_all(pairs, sem):
    for source, target in pairs:
        pltpu.make_async_copy(source, target, sem).start()


def silu(value):
    return value / (1.0 + jnp.exp(-value))


def as_row(column):
    lane = lax.broadcasted_iota(jnp.int32, (column.shape[0], LANES), 1)
    row = lax.broadcasted_iota(jnp.int32, (column.shape[0], LANES), 0)
    return jnp.sum(jnp.where(row == lane, column, 0.0), axis=0, keepdims=True)


def as_column(row_values, first, rows):
    lane = lax.broadcasted_iota(jnp.int32, (rows, LANES), 1)
    row = lax.broadcasted_iota(jnp.int32, (rows, LANES), 0)
    return jnp.sum(jnp.where(row + first == lane, row_values, 0.0), axis=1, keepdims=True)


def remote(axis, peer, source, target, send_sem, recv_sem):
    return remote_to({axis: peer}, source, target, send_sem, recv_sem)


def remote_to(device, source, target, send_sem, recv_sem):
    return pltpu.make_async_remote_copy(
        src_ref=source, dst_ref=target, send_sem=send_sem, recv_sem=recv_sem,
        device_id=device, device_id_type=MESH_ID,
    )


def far_first(chip, chips):
    def ascending(at, k):
        return k + 1 - (at + chips - 1 - k) // chips

    low = 1 - chip // (chips // 2)
    mirrored = chips - 1 - chip
    return [
        low * (chips - 1 - ascending(mirrored, k)) + (1 - low) * ascending(chip, k)
        for k in range(chips - 1)
    ]


def start_gather(slots, tp, n_tp, hub, send_sems, recv_sems):
    chips = n_tp // CORES
    chip, core = tp // CORES, lax.rem(tp, CORES)
    partner = chip * CORES + 1 - core
    order = far_first(chip, chips)

    def block(peer, slot, send):
        return remote("tp", peer, slots.at[slot], slots.at[slot], send_sems.at[send], recv_sems.at[slot])

    for peer in order:
        block(peer * CORES + hub, tp, 0).start()
    block(partner, tp, 0).start()
    relayed = [
        block(partner, source * CORES + side, 1) for source in order[::-1] for side in range(CORES)
    ]

    def take(first, last):
        for copy in relayed[first * CORES : last * CORES]:
            copy.wait_recv()

            @pl.when(core == hub)
            def _():
                copy.start()

    def take_own():
        block(partner, partner, 0).wait_recv()

    def close():
        landed(slots.at[:chips], send_sems.at[0])

        @pl.when(core == hub)
        def _():
            landed(slots.at[: len(relayed)], send_sems.at[1])

    return take, take_own, close, order[::-1]


def start_reduce(lhs, weight, parts, swapped, tp, send_sems, recv_sems):
    chip, core = tp // CORES, lax.rem(tp, CORES)
    chips, columns = parts.shape[1], parts.shape[3]

    def multiply(side):
        full = jnp.dot(lhs, weight[side], preferred_element_type=jnp.float32).astype(jnp.bfloat16)
        for z in range(chips):
            parts[side, z] = full[:, z * columns : (z + 1) * columns]

    multiply(core)
    remote(
        "tp", chip * CORES + 1 - core, parts.at[core], swapped, send_sems.at[0], recv_sems.at[0]
    ).start()
    multiply(1 - core)


def spread_pairs(parts, swapped, staged, into, tp, send_sems, recv_sems):
    chips = parts.shape[1]
    chip, core = tp // CORES, lax.rem(tp, CORES)
    landed(swapped, recv_sems.at[0])
    for k, other in enumerate(far_first(chip, chips) + [chip]):
        pair = parts[1 - core, other].astype(jnp.float32) + swapped[other].astype(jnp.float32)
        staged[k] = pair.astype(jnp.bfloat16)
        remote(
            "tp", other * CORES + 1 - core, staged.at[k], into.at[chip], send_sems.at[1], recv_sems.at[1]
        ).start()


def total_of(own, others):
    total = own.astype(jnp.float32)
    for step in range(others.shape[0]):
        total += others[step].astype(jnp.float32)
    return total


def layer_kernel(
    n_kv, n_tp, features,
    tokens_hbm, lengths_hbm, freq_hbm, gain_hbm, gain_two_hbm, state_hbm,
    wq_hbm, wk_hbm, wv_hbm, wg_hbm, wo_hbm, fg_hbm, fu_hbm, fd_hbm,
    out, state, s, sems,
):
    kv, tp = lax.axis_index("kv"), lax.axis_index("tp")
    chips = n_tp // CORES
    chip, core = tp // CORES, lax.rem(tp, CORES)
    gathered, gathered_two, merged, hidden = s["gathered"], s["gathered_two"], s["merged"], s["hidden"]
    halves, rows = gathered.shape[0], gathered.shape[3]
    batch = n_kv * rows
    q_width, v_width = wq_hbm.shape[1], wv_hbm.shape[1]
    units, columns = fg_hbm.shape[1], tokens_hbm.shape[3]

    def sides(ref, target):
        return [
            (
                ref.at[:, (z * CORES + side) * columns : (z * CORES + side + 1) * columns],
                target.at[side, :, z * columns : (z + 1) * columns],
            )
            for side in range(CORES)
            for z in range(chips)
        ]

    groups = {
        "tokens": [(tokens_hbm.at[:, h], gathered.at[h, tp]) for h in range(halves)],
        "lengths": [(lengths_hbm, s["lengths"])],
        "freq": [(freq_hbm, s["freq"])],
        "gain": [(gain_hbm, s["gain"])],
        "wp": [
            (wq_hbm, s["wp"].at[:, :q_width]),
            (wk_hbm, s["wp"].at[:, q_width : 2 * q_width]),
            (wv_hbm, s["wp"].at[:, 2 * q_width : 2 * q_width + v_width]),
            (wg_hbm, s["wp"].at[:, 2 * q_width + v_width :]),
        ],
        "state": [(state_hbm, state)],
        "wo": sides(wo_hbm, s["wo"]),
        "gain_two": [(gain_two_hbm, s["gain_two"])],
        "fg": [(fg_hbm, s["fg"])],
        "fu": [(fu_hbm, s["fu"])],
        "fd": sides(fd_hbm, s["fd"]),
    }
    wholes = {
        "tokens": gathered.at[:, tp], "wp": s["wp"], "state": state, "wo": s["wo"], "fd": s["fd"],
        "lengths": s["lengths"], "freq": s["freq"], "gain": s["gain"],
        "gain_two": s["gain_two"], "fg": s["fg"], "fu": s["fu"],
    }
    pending = {}
    for i, (name, group) in enumerate(groups.items()):
        pending[name] = i
        load_all(group, sems["load"].at[i])

    def ready(*wanted):
        for name in wanted:
            if name in pending:
                landed(wholes[name], sems["load"].at[pending.pop(name)])

    partner = chip * CORES + 1 - core
    peers = [{"kv": peer, "tp": tp} for peer in kv_peers(kv, n_kv)]
    crossed = [{"kv": peer, "tp": partner} for peer in kv_peers(kv, n_kv)]
    along = [{"kv": kv, "tp": other * CORES + 1 - core} for other in far_first(chip, chips)]
    beside = {"kv": kv, "tp": partner}
    crossed_all = crossed + [beside]
    aside = [{"kv": kv, "tp": other * CORES + core} for other in far_first(chip, chips)]
    greet(along + aside + [beside] + peers + crossed)
    closing = []

    def close_sends():
        for extent, sem in closing:
            landed(extent, sem)
        closing.clear()

    def pair_of(name, h):
        return sems[name + "_s"].at[h], sems[name + "_r"].at[h]

    def kv_send(name, h, devices, source, target, extent):
        send_sem, recv_sem = sems[SHARED.get(name, name)].at[h, 0], sems[SHARED.get(name, name)].at[h, 1]
        send_all(devices, source, target, send_sem, recv_sem)
        closing.append((extent, send_sem))
        return lambda: landed(extent, recv_sem)

    def send_squares(name, h, devices):
        return kv_send(
            name, h, devices, lambda p: s[name].at[h, n_kv - 1], lambda n: s[name].at[h, n], s[name].at[h, : n_kv - 1]
        )

    def scale_of(name, h, wait):
        wait()
        total = s[name][h, 0]
        for n in range(1, n_kv):
            total += s[name][h, n]
        return lax.rsqrt(as_column(total, kv * rows, rows) / features + 1e-06)

    ready("tokens")
    first_gather = [start_gather(gathered.at[0], tp, n_tp, 0, *pair_of("g", 0))]
    ready("lengths", "freq", "gain")
    def gathered_product(gather, slots, gains, weight, between=None):
        take, take_own, _, near = gather
        span = CORES * columns

        def chunk(source):
            at = pl.multiple_of(source * span, span)
            x = jnp.concatenate(
                [slots[source * CORES + side].reshape(batch, columns) for side in range(CORES)], axis=1
            ).astype(jnp.float32)
            part = (x * gains[:, pl.ds(at, span)]).astype(jnp.bfloat16)
            s["normed"][:, pl.ds(at, span)] = part
            product = jnp.dot(part, weight[pl.ds(at, span), :], preferred_element_type=jnp.float32)
            return product, jnp.sum(x * x, axis=1, keepdims=True)

        take_own()
        product, squares = chunk(chip)
        if between is not None:
            between()
        for k, source in enumerate(near):
            take(k, k + 1)
            more, more_squares = chunk(source)
            product += more
            squares += more_squares
        return product.astype(jnp.bfloat16).reshape(n_kv, rows, product.shape[1]), as_row(squares)

    def project(weight):
        full = jnp.dot(s["normed"][...], weight[...], preferred_element_type=jnp.float32)
        return full.astype(jnp.bfloat16).reshape(n_kv, rows, full.shape[1])

    heads = q_width // QK
    width = v_width // heads
    out_a, out_b, in_a, in_b = s["out_a"], s["out_b"], s["in_a"], s["in_b"]
    first, second, copies_m, copies_q = [], [], [], []

    angles_of = []

    def find_angles():
        all_rows = halves * rows
        row = lax.broadcasted_iota(jnp.int32, (all_rows, all_rows), 0)
        col = lax.broadcasted_iota(jnp.int32, (all_rows, all_rows), 1)
        spread = jnp.where(row == col, s["lengths"][...].astype(jnp.float32), 0.0)
        angles = jnp.sum(spread, axis=1, keepdims=True) * s["freq"][...]
        cosine, sine = jnp.cos(angles), jnp.sin(angles)
        lane = lax.broadcasted_iota(jnp.int32, angles.shape, 1)
        sine = jnp.where(lane < QK // 2, -sine, sine)
        angles_of.extend([cosine, sine])

    def start_next_gather(h):
        if h == 1:
            find_angles()
        if h < halves:
            first_gather.append(start_gather(gathered.at[h], tp, n_tp, 0, *pair_of("g", h)))

    def project_first(h):
        product, s["squares"][h, n_kv - 1] = gathered_product(
            first_gather[h], gathered.at[h], s["gain"], s["wp"], lambda: start_next_gather(h + 1)
        )
        out_a[h] = product[:, :, : 2 * q_width]
        out_b[h] = product[:, :, 2 * q_width :]
        first.append(kv_send("a", h, peers, lambda p: out_a.at[h, p], lambda n: in_a.at[h, n], in_a.at[h]))
        copies_q.append(send_squares("squares", h, peers))
        second.append(kv_send("b", h, peers, lambda p: out_b.at[h, p], lambda n: in_b.at[h, n], in_b.at[h]))

    decays = []
    for head in range(heads):
        number = jnp.full((1, width), tp * heads + head, jnp.int32).astype(jnp.float32)
        decays.append(1.0 - jnp.exp2(-5.0 - 10.0 * number / (heads * n_tp - 1)))
    qk, value, retained = s["qk"], s["value"], s["retained"]

    def attend(h):
        base = h * rows
        first[h]()
        total = total_of(out_a[h, kv], in_a.at[h])
        scale = scale_of("squares", h, copies_q[h])
        total = total * scale
        cosines, sines = [table[base : base + rows] for table in angles_of]
        blocks = []
        for start, factor in ((0, 1.0), (q_width, QK ** (-0.5))):
            for head in range(heads):
                part = total[:, start + head * QK : start + (head + 1) * QK]
                turned = (part * cosines + pltpu.roll(part, QK // 2, 1) * sines) * factor
                blocks.append(turned.astype(jnp.bfloat16).astype(jnp.float32))
        columns = jnp.concatenate(blocks * (LANES // (len(blocks) * rows)), axis=0).T
        qk[h] = columns
        for i in range(rows):
            for head in range(heads):
                query = columns[:, head * rows + i : head * rows + i + 1]
                retained[base + i : base + i + 1, head * width : (head + 1) * width] = jnp.sum(
                    query * state[base + i, head], axis=0, keepdims=True
                )
        second[h]()
        total = total_of(out_b[h, kv], in_b.at[h]) * scale
        values = total[:, :v_width].astype(jnp.bfloat16).astype(jnp.float32)
        value[base : base + rows] = values
        pieces = []
        for head in range(heads):
            overlap = jnp.sum(blocks[head] * blocks[heads + head], axis=1, keepdims=True)
            span = slice(head * width, (head + 1) * width)
            piece = decays[head] * retained[base : base + rows, span] + overlap * values[:, span]
            pieces.append(piece * lax.rsqrt(jnp.mean(piece * piece, axis=1, keepdims=True) + 1e-06))
        s["merged_out"][h] = (jnp.concatenate(pieces, axis=1) * silu(total[:, v_width:])).astype(jnp.bfloat16)
        copies_m.append(
            kv_send("m", h, crossed_all, lambda p: s["merged_out"].at[h], lambda n: merged.at[h, kv], merged.at[h])
        )

    block = 8

    def update(h):
        base = h * rows

        def update_step(i, carry):
            start = i * block
            turned = pltpu.roll(qk[h], lax.rem(LANES - start, LANES), 1)
            for n in range(block):
                for head in range(heads):
                    lane = (heads + head) * rows + n
                    at = base + start + n
                    outer = turned[:, lane : lane + 1] * value[pl.ds(at, 1), head * width : (head + 1) * width]
                    state[at, head] = decays[head] * state[at, head] + outer
            return carry

        lax.fori_loop(0, rows // block, update_step, 0)

    def reduce_start(h, lhs, weight, tag):
        start_reduce(lhs, s[weight], s["parts_" + tag].at[h], s["swapped_" + tag].at[h], tp, *pair_of("x", h))

    def reduce_spread(h, tag):
        swapped, staged = s["swapped_" + tag].at[h], s["staged_" + tag].at[h]
        send_sems, recv_sems = pair_of("x", h)
        spread_pairs(s["parts_" + tag].at[h], swapped, staged, s["landed_" + tag].at[h], tp, send_sems, recv_sems)
        closing.extend([(swapped, send_sems.at[0]), (staged, send_sems.at[1])])

    def reduce_total(h, tag):
        into = s["landed_" + tag].at[h]
        landed(into, pair_of("x", h)[1].at[1])
        return total_of(into[0], into.at[1:])

    gate_out, up_out, gate_in, up_in = s["gate_out"], s["up_out"], s["gate_in"], s["up_in"]
    copies_e, copies_f, copies_h, copies_u = [], [], [], []
    first_units = units

    def project_second(h):
        for span in (slice(0, first_units),):
            if span.start == 0:
                gate_out[h, :, :, span], s["squares_two"][h, n_kv - 1] = gathered_product(
                    second_gather[h], gathered_two.at[h], s["gain_two"], s["fg"].at[:, span]
                )
            else:
                gate_out[h, :, :, span] = project(s["fg"].at[:, span])
            send_all(
                crossed_all, lambda p: gate_out.at[h, p, :, span], lambda n: gate_in.at[h, n, :, span],
                sems["a"].at[h, 0], sems["a"].at[h, 1],
            )
            if span.start == 0:
                copies_u.append(send_squares("squares_two", h, crossed))
        closing.append((gate_in.at[h], sems["a"].at[h, 0]))
        copies_e.append(lambda: landed(gate_in.at[h], sems["a"].at[h, 1]))
        up_out[h] = project(s["fu"])
        copies_f.append(
            kv_send("f", h, crossed_all, lambda p: up_out.at[h, p], lambda n: up_in.at[h, n], up_in.at[h])
        )

    def activate(h):
        copies_e[h]()
        total = total_of(gate_in[h, 0], gate_in.at[h, 1:])
        scale = scale_of("squares_two", h, copies_u[h])
        activated = silu(total * scale)
        copies_f[h]()
        up = total_of(up_in[h, 0], up_in.at[h, 1:]) * scale
        s["hidden_out"][h] = (activated * up).astype(jnp.bfloat16)
        copies_h.append(
            kv_send("h", h, crossed_all, lambda p: s["hidden_out"].at[h], lambda n: hidden.at[h, kv], hidden.at[h])
        )

    second_gather = []
    ready("wp")
    project_first(0)
    ready("wo")
    remote_to(beside, s["wo"], s["wo_far"], sems["wo"].at[0], sems["wo"].at[1]).start()
    for h in range(1, halves):
        project_first(h)
    ready("state")
    for h in range(halves):
        attend(h)
    landed(s["wo_far"], sems["wo"].at[1])
    for h in range(halves):
        copies_m[h]()
        reduce_start(h, merged[h].reshape(batch, v_width), "wo_far", "x")
        reduce_spread(h, "x")
    for h in range(halves - 1):
        update(h)
    for gather in first_gather:
        gather[2]()
    for h in range(halves):
        total = reduce_total(h, "x")
        own = gathered[h, tp].reshape(batch, LANES).astype(jnp.float32)
        gathered_two[h, tp] = (own + total).astype(jnp.bfloat16).reshape(n_kv, rows, LANES)
        second_gather.append(start_gather(gathered_two.at[h], tp, n_tp, 1, *pair_of("g", h)))
        if h == 0:
            update(halves - 1)
    ready("gain_two", "fg", "fu")
    landed(s["wo_far"], sems["wo"].at[0])
    close_sends()
    for h in range(halves):
        project_second(h)
    for h in range(halves):
        activate(h)
    ready("fd")
    for h in range(halves):
        copies_h[h]()
        reduce_start(h, hidden[h].reshape(batch, units), "fd", "d")
        reduce_spread(h, "d")
    for h in range(halves):
        total = reduce_total(h, "d")
        own = gathered_two[h, tp].reshape(batch, LANES).astype(jnp.float32)
        out[:, h] = (own + total).astype(jnp.bfloat16).reshape(n_kv, rows, LANES)
    close_sends()
    for gather in second_gather:
        gather[2]()


def finish_kernel(chunks, state, out, state_to, out_to, sems):
    size = state.shape[0] // chunks
    for i in range(chunks):
        part = pl.ds(i * size, size)
        pltpu.make_async_copy(state.at[part], state_to.at[part], sems.at[0]).start()
    pltpu.make_async_copy(out, out_to, sems.at[1]).start()
    pltpu.make_async_copy(state, state_to, sems.at[0]).wait()
    pltpu.make_async_copy(out, out_to, sems.at[1]).wait()


HALVES = 2
FINISH_CHUNKS = 16
SHARED = {"f": "b", "h": "m", "squares_two": "squares"}


def fused_on_device(n_kv, n_tp, *arrays):
    (
        tokens, lengths, state, mixer_gain, wq, wk, wv, wg, wo, channel_gain, fg, fu, fd,
    ) = arrays
    columns = tokens.shape[1]
    rows = state.shape[0] // HALVES
    batch = n_kv * rows
    depth, q_width = wq.shape
    v_width, units = wv.shape[1], fg.shape[1]
    bf16, f32 = jnp.bfloat16, jnp.float32
    vmem = pl.BlockSpec(memory_space=pltpu.VMEM)
    hbm = pl.BlockSpec(memory_space=pltpu.HBM)
    chips = n_tp // CORES
    index = np.arange(QK) % (QK // 2)
    freq = jnp.asarray((10000.0 ** (-index / (QK // 2))).astype(np.float32))[None, :]
    a_width, b_width = 2 * q_width, 2 * v_width

    def buffer(*shape, dtype=bf16):
        return pltpu.VMEM((HALVES,) + shape, dtype)

    scratch = {
        "lengths": pltpu.VMEM((1, HALVES * rows), jnp.int32),
        "freq": pltpu.VMEM((1, QK), f32),
        "gain": pltpu.VMEM((1, depth), f32),
        "gain_two": pltpu.VMEM((1, depth), f32),
        "gathered": buffer(n_tp, n_kv, rows, columns),
        "gathered_two": buffer(n_tp, n_kv, rows, columns),
        "out_a": buffer(n_kv, rows, a_width),
        "out_b": buffer(n_kv, rows, b_width),
        "in_a": buffer(n_kv - 1, rows, a_width),
        "in_b": buffer(n_kv - 1, rows, b_width),
        "qk": buffer(QK, LANES, dtype=f32),
        "retained": pltpu.VMEM((HALVES * rows, v_width), f32),
        "value": pltpu.VMEM((HALVES * rows, v_width), f32),
        "merged": buffer(n_kv, rows, v_width),
        "merged_out": buffer(rows, v_width),
        "normed": pltpu.VMEM((batch, depth), bf16),
        "gate_out": buffer(n_kv, rows, units),
        "up_out": buffer(n_kv, rows, units),
        "gate_in": buffer(n_kv, rows, units),
        "up_in": buffer(n_kv, rows, units),
        "hidden_out": buffer(rows, units),
        "hidden": buffer(n_kv, rows, units),
        "squares": buffer(n_kv, 1, LANES, dtype=f32),
        "squares_two": buffer(n_kv, 1, LANES, dtype=f32),
    }
    shapes = {
        "wp": (depth, 2 * q_width + 2 * v_width), "fg": fg.shape, "fu": fu.shape,
        "wo": (CORES, wo.shape[0], chips * columns),
        "wo_far": (CORES, wo.shape[0], chips * columns),
        "fd": (CORES, fd.shape[0], chips * columns),
    }
    scratch.update({name: pltpu.VMEM(shape, bf16) for name, shape in shapes.items()})
    for tag in ("x", "d"):
        scratch["parts_" + tag] = buffer(CORES, chips, batch, columns)
        scratch["swapped_" + tag] = buffer(chips, batch, columns)
        scratch["staged_" + tag] = buffer(chips, batch, columns)
        scratch["landed_" + tag] = buffer(chips, batch, columns)
    dma = pltpu.SemaphoreType.DMA
    sems = {"load": dma((11,)), "wo": dma((2,))}
    sems["g_s"], sems["g_r"] = dma((HALVES, 2)), dma((HALVES, n_tp))
    for tag in ("x_s", "x_r", "a", "b", "m", "squares"):
        sems[tag] = dma((HALVES, 2))
    operands = (
        tokens.reshape(n_kv, HALVES, rows, columns), lengths[None, :], freq, mixer_gain[None, :],
        channel_gain[None, :], state, wq, wk, wv, wg, wo, fg, fu, fd,
    )
    out_shape = (n_kv, HALVES, rows, columns)
    out, new_state = pl.pallas_call(
        functools.partial(layer_kernel, n_kv, n_tp, depth * n_kv),
        out_shape=(pltpu.VMEM(out_shape, bf16), pltpu.VMEM(state.shape, f32)),
        in_specs=[hbm] * 14,
        out_specs=(vmem, vmem),
        scratch_shapes=[scratch, sems],
        compiler_params=pltpu.CompilerParams(
            collective_id=0, has_side_effects=True, vmem_limit_bytes=LAYER_VMEM
        ),
        name="layer",
    )(*[pltpu.with_memory_space_constraint(a, pltpu.HBM) for a in operands])
    new_state, out = pl.pallas_call(
        functools.partial(finish_kernel, FINISH_CHUNKS),
        out_shape=(
            jax.ShapeDtypeStruct(state.shape, f32),
            jax.ShapeDtypeStruct(out_shape, bf16),
        ),
        in_specs=[vmem, vmem],
        out_specs=(hbm, hbm),
        scratch_shapes=[dma((2,))],
        compiler_params=pltpu.CompilerParams(vmem_limit_bytes=FINISH_VMEM),
        name="finish",
    )(new_state, out)
    return out.reshape(tokens.shape), new_state


def fits(n_kv, n_tp, arrays):
    tokens, state, ffn_gate = arrays[0], arrays[2], arrays[10]
    rows, heads = state.shape[0], state.shape[1]
    return (
        tokens.shape[1] % LANES == 0
        and n_tp % CORES == 0
        and n_tp > CORES
        and n_kv == SIDE * SIDE
        and 4 * state.size < VMEM_TOTAL // 4
        and ffn_gate.shape[1] % LANES == 0
        and tokens.shape[1] == LANES
        and tokens.shape[0] == n_kv * rows
        and rows % (16 * HALVES) == 0
        and n_kv * rows // HALVES <= LANES
        and 2 * heads * rows == LANES
        and state.shape[2] == QK == LANES
        and state.shape[3] % LANES == 0
    )


def per_device(n_kv, n_tp, *arrays):
    if fits(n_kv, n_tp, arrays):
        return fused_on_device(n_kv, n_tp, *arrays)
    return on_device(*arrays)


def solution(mesh):
    in_specs = (
        P(None, ("kv", "tp")),
        P("kv"),
        P("kv", "tp", None, None),
        P("kv"),
        P("kv", "tp"),
        P("kv", "tp"),
        P("kv", "tp"),
        P("kv", "tp"),
        P("tp", "kv"),
        P("kv"),
        P("kv", "tp"),
        P("kv", "tp"),
        P("tp", "kv"),
    )
    out_specs = (P(None, ("kv", "tp")), P("kv", "tp", None, None))
    return jax.shard_map(
        functools.partial(per_device, mesh.shape["kv"], mesh.shape["tp"]),
        mesh=mesh, in_specs=in_specs, out_specs=out_specs, check_vma=False
    )
```
